256 devices in a mesh: grp: 2 (over y), sp: 16 (over z), tp: 8 (over x, core).
Axes of the slice: x: 4, y: 2, z: 16, core: 2. Of those that a mesh axis runs over, the one named last changes fastest.
The devices are a block of a 4x16x16 slice.
Arguments:
- tokens: bfloat16 [65536, 2048], P(('grp', 'sp')), parts along dimension 0, may hold values from -6 to 6
- in_gain: float32 [2048], replicated, may hold values from 0.1 to 1.9
- w_input: bfloat16 [2048, 2048], P(None, 'tp'), may hold values from -0.125 to 0.125
- w_gate: bfloat16 [2048, 2048], P(None, 'tp'), may hold values from -4 to 4
- conv_taps: float32 [4, 2048], P(None, 'tp'), may hold values from -3 to 3
- w_rate: bfloat16 [8, 256, 256], P('tp'), may hold values from -0.375 to 0.375
- w_inlet: bfloat16 [8, 256, 256], P('tp'), may hold values from -0.375 to 0.375
- decay_param: float32 [2048], P('tp'), may hold values from 3 to 25
- decay_bias: float32 [8, 65536], P('tp', ('grp', 'sp')), parts along dimension 1, may hold values from -1.5 to 0
- out_gain: float32 [2048], P('tp'), may hold values from 0.1 to 1.9
- w_out: bfloat16 [2048, 2048], P('sp'), may hold values from -0.125 to 0.125
Outputs:
- mixer_out: bfloat16 [65536, 2048], P(('grp', 'sp', 'tp')), parts along dimension 0
The draws below stay inside these ranges and needn't reach their ends.
There are 2 independent parts, one for each index of `grp`. The reference program is written for one: setup_inputs(seed, part) draws one part's arguments, and reference() takes and returns one part's arrays. A program takes and returns all parts, laid end to end along the dimension named above; an argument that names none is the same for every part. Nothing has to cross between parts.
All inputs are finite; a program needn't handle non-finite values.
Results may differ from the reference program's by a relative error of at most 0.013.
Values may be sent and summed in bfloat16 or wider, within the bound.
A program may use at most 128 MiB of HBM per device.

```python
import math
import jax
import jax.numpy as jnp
from jax import lax

D = 2048
HEADS = 8
HEAD = 256
CONV = 4
SEQ_DEV = 2048
DR = 2048
SEQ = 32768


def draw_w_gate(key, part):
    base_key, jitter_key = jax.random.split(jax.random.fold_in(key, 11))
    columns = HEADS * HEAD
    base = jnp.clip(jax.random.normal(base_key, (D, columns), jnp.float32), -4.0, 4.0)
    position = jnp.arange(columns, dtype=jnp.float32) / columns
    jitter = jax.random.uniform(jitter_key, (columns,), jnp.float32) / HEADS
    column_scale = jnp.exp((position + jitter) * math.log(6.0))
    return (base * column_scale[None, :] / math.sqrt(D)).astype(jnp.bfloat16)


def draw_decay_param(key, part):
    pick_key, slow_key, fast_key = jax.random.split(jax.random.fold_in(key, 23), 3)
    channels = HEADS * HEAD
    slow = jax.random.bernoulli(pick_key, 0.5, (channels,))
    slow_rate = jax.random.uniform(slow_key, (channels,), jnp.float32, 0.2, 0.6) / (8.0 * SEQ)
    fast_rate = jnp.exp(jax.random.uniform(fast_key, (channels,), jnp.float32, math.log(1.0 / 400.0), math.log(1.0 / 120.0)))
    chosen = jnp.where(slow, slow_rate, fast_rate)
    return -jnp.log(jnp.expm1(chosen))


def draw_decay_bias(key, part):
    span_key, spot_key, depth_key = jax.random.split(jax.random.fold_in(key, 37), 3)
    span_count = SEQ // SEQ_DEV
    level = jnp.exp(jax.random.uniform(span_key, (HEADS, span_count), jnp.float32, math.log(0.2), math.log(1.2))) / SEQ
    dispersion = jnp.repeat(-level, SEQ_DEV, axis=1)
    spots = jax.random.randint(spot_key, (HEADS, 2), 0, SEQ)
    layer_count = jnp.log(jax.random.uniform(depth_key, (HEADS, 2), jnp.float32, 0.55, 0.8))
    match_count = (jnp.arange(SEQ, dtype=jnp.int32)[None, None, :] == spots[:, :, None]).astype(jnp.float32)
    pulse_train = jnp.sum(match_count * layer_count[:, :, None], axis=1)
    return dispersion + pulse_train


def level_of(key, dims, shards, least, top_value):
    factor_of = 1.0
    for dim, parts in shards:
        heights = jax.random.uniform(jax.random.fold_in(jax.random.fold_in(key, 6), dim), (parts,), jnp.float32, least / len(shards), top_value / len(shards))
        factor_of = factor_of * jnp.repeat(jnp.exp(heights), dims[dim] // parts).reshape((-1,) + (1,) * (len(dims) - 1 - dim))
    return factor_of


def scatter_about(key, dims, deviation, reach, shards=(), held_as=jnp.bfloat16):
    factor_of = level_of(key, dims, shards, -0.22, 0.18) if shards else 1.0
    drawn = jax.random.normal(key, dims, jnp.float32) * deviation * factor_of
    return jnp.minimum(jnp.maximum(drawn, -reach), reach).astype(held_as)


def setup_inputs(seed: int = 0, part: int = 0) -> dict:
    key_of = jax.random.split(jax.random.key(seed), 12)
    own_keys = jax.random.split(jax.random.fold_in(key_of[11], part), 12)
    return {
        "tokens": scatter_about(own_keys[0], (SEQ, D), 1.0, 6.0, ((0, 16),)),
        "in_gain": jnp.clip(1.0 + 0.18 * jax.random.normal(key_of[1], (D,), jnp.float32), 0.1, 1.9),
        "w_input": scatter_about(key_of[2], (D, DR), D ** -0.5, 0.125, ((1, 8),)),
        "w_gate": draw_w_gate(jax.random.fold_in(key_of[11], 71), part),
        "conv_taps": scatter_about(key_of[4], (CONV, DR), 0.5, 3.0, ((1, 8),), jnp.float32),
        "w_rate": scatter_about(key_of[5], (HEADS, HEAD, HEAD), HEAD ** -0.5, 0.375, ((0, 8),)),
        "w_inlet": scatter_about(key_of[6], (HEADS, HEAD, HEAD), HEAD ** -0.5, 0.375, ((0, 8),)),
        "decay_param": draw_decay_param(jax.random.fold_in(key_of[11], 71), part),
        "decay_bias": draw_decay_bias(jax.random.fold_in(jax.random.fold_in(key_of[11], part), 71), part),
        "out_gain": jnp.clip(1.0 + 0.18 * jax.random.normal(key_of[9], (DR,), jnp.float32), 0.1, 1.9),
        "w_out": scatter_about(key_of[10], (DR, D), DR ** -0.5, 0.125, ((0, 16),)),
    }


def combine_pairs(first_pair, second_pair):
    return (first_pair[0] * second_pair[0], second_pair[0] * first_pair[1] + second_pair[1])

def reference(tokens, in_gain, w_input, w_gate, conv_taps, w_rate, w_inlet, decay_param, decay_bias, out_gain, w_out):
    seq_len = tokens.shape[0]
    as_float = tokens.astype(jnp.float32)
    inv_norm = lax.rsqrt(lax.optimization_barrier(jnp.mean(as_float * as_float, axis=1, keepdims=True)) + 1e-06)
    normed = (as_float * inv_norm * in_gain).astype(jnp.bfloat16)
    projected = jnp.dot(normed, w_input, preferred_element_type=jnp.float32).astype(jnp.bfloat16)
    gate_raw = jnp.dot(normed, w_gate, preferred_element_type=jnp.float32).astype(jnp.bfloat16)
    padded = jnp.pad(projected.astype(jnp.float32), ((CONV - 1, 0), (0, 0)))
    tap_values = conv_taps.astype(jnp.float32)
    summed = padded[0:seq_len] * tap_values[0]
    for offset in range(1, CONV):
        summed = summed + padded[offset:offset + seq_len] * tap_values[offset]
    convolved = summed.astype(jnp.bfloat16)
    per_head = convolved.astype(jnp.float32).reshape(seq_len, HEADS, HEAD)
    rate_gate = jax.nn.sigmoid(jnp.einsum('shi,hij->shj', per_head, w_rate.astype(jnp.float32))).reshape(seq_len, HEADS * HEAD)
    input_gate = jax.nn.sigmoid(jnp.einsum('shi,hij->shj', per_head, w_inlet.astype(jnp.float32))).reshape(seq_len, HEADS * HEAD)
    head_bias = jnp.repeat(jnp.transpose(decay_bias), HEAD, axis=1)
    log_decay = -8.0 * rate_gate * jax.nn.softplus(-decay_param) + head_bias
    drive_term = jnp.sqrt(-jnp.expm1(2.0 * log_decay)) * input_gate * convolved.astype(jnp.float32)
    decay_prod, full_state = lax.associative_scan(combine_pairs, (jnp.exp(log_decay), drive_term), axis=0)
    gated_out = full_state * jax.nn.gelu(gate_raw.astype(jnp.float32))
    out_scale = lax.rsqrt(lax.optimization_barrier(jnp.mean(gated_out * gated_out, axis=1, keepdims=True)) + 1e-06)
    normed_out = (gated_out * out_scale * out_gain).astype(jnp.bfloat16)
    return jnp.dot(normed_out, w_out, preferred_element_type=jnp.float32).astype(jnp.bfloat16)
```

```python
import functools

import jax
import jax.numpy as jnp
from jax import lax
from jax.experimental import pallas as pl
from jax.experimental.pallas import tpu as pltpu
from jax.sharding import PartitionSpec as P

MESH = pl.DeviceIdType.MESH
F32 = jnp.float32
BF16 = jnp.bfloat16
LANES = 128
SEGS = 8
STEP = 32
PAD = 40


def log1p_small(u):
    series = u * (1.0 - u * (0.5 - u * (1.0 / 3.0 - u * (0.25 - u * (0.2 - u / 6.0)))))
    return jnp.where(u < 0.06, series, jnp.log(1.0 + u))


def softplus(x):
    return jnp.maximum(x, 0.0) + log1p_small(jnp.exp(-jnp.abs(x)))


def gelu(x):
    inner = 0.7978845608028654 * (x + 0.044715 * (x * x * x))
    return 0.5 * x * (1.0 + jnp.tanh(inner))


def kernel(
    tokens_in,
    gain_in,
    w_input_in,
    w_gate_in,
    taps_in,
    w_rate_in,
    w_inlet_in,
    dparam_in,
    bias_in,
    ogain_in,
    w_out_in,
    out,
    tok,
    wi,
    wg,
    wrn,
    gain,
    taps,
    dparam,
    bias,
    ogain,
    wv,
    proj,
    halo,
    biasc,
    invc,
    conv,
    gates,
    sa,
    sb,
    ht,
    pt,
    ge,
    segh,
    segp,
    carry_own,
    carry,
    gout,
    grecv,
    ss_own,
    ss_recv,
    obuf,
    tok_sem,
    in_sem,
    wv_sem,
    out_sem,
    zr,
    xr,
    yr,
    zs,
    xs,
    ys,
    ds_send,
    ds_recv,
    halo_send,
    halo_recv,
    carry_send,
    carry_recv,
    a2a_send,
    a2a_recv,
    ss_send,
    ss_recv_sem,
    know,
):
    grp, z, tp = lax.axis_index("grp"), lax.axis_index("sp"), lax.axis_index("tp")
    spans, peers = lax.axis_size("sp"), lax.axis_size("tp")
    half = spans // 2
    core = lax.rem(tp, 2)
    rows, width = tok.shape
    channels = wi.shape[1]
    block = width // spans
    share = block // 2
    tile = rows // 4
    mine = rows // peers
    first = lax.rem(2 * (tp // 2) + 4 * lax.rem(grp, 2), 8)
    partner = grp + 1 - 2 * lax.rem(grp, 2)
    sibling = tp + 1 - 2 * core

    def column(pos):
        offset = (0, 1, 2, 3, 4, 6, 5, 7)[pos]
        return pl.multiple_of(lax.rem(first + offset, 8) * channels, channels)

    def local(src, dst, sem):
        return pltpu.make_async_copy(src, dst, sem)

    def remote(src, dst, send, recv, where):
        return pltpu.make_async_remote_copy(
            src_ref=src, dst_ref=dst, send_sem=send, recv_sem=recv, device_id=where, device_id_type=MESH
        )

    def lines_of(owner):
        return pl.ds(pl.multiple_of(owner * block + core * share, share), share)

    own_lines = pl.ds(pl.multiple_of(z * block, block), block)
    wv_copies = [
        local(w_out_in.at[:, pl.ds(column(pos), channels)], wv.at[pos, own_lines, :], wv_sem.at[pos])
        for pos in range(8)
    ]
    for pos in range(4):
        wv_copies[pos].start()
    in_copies = [
        local(gain_in, gain, in_sem.at[0]),
        local(w_input_in, wi, in_sem.at[1]),
        local(bias_in, bias, in_sem.at[2]),
        local(taps_in, taps, in_sem.at[3]),
        local(dparam_in, dparam, in_sem.at[4]),
        local(ogain_in, ogain, in_sem.at[5]),
        local(w_rate_in, wrn.at[:, 0:channels], in_sem.at[6]),
        local(w_inlet_in, wrn.at[:, channels : 2 * channels], in_sem.at[7]),
        local(w_gate_in, wg, in_sem.at[8]),
    ]
    for k in (0, 1, 2):
        in_copies[k].start()

    def tok_copy(k):
        part = pl.ds(pl.multiple_of(k * tile, tile), tile)
        return local(tokens_in.at[part, :], tok.at[part, :], tok_sem.at[k])

    for k in (3, 2, 1, 0):
        tok_copy(k).start()
    for k in range(3, 9):
        in_copies[k].start()
    for pos in range(4, 8):
        wv_copies[pos].start()

    barrier = pltpu.get_barrier_semaphore()
    above, below = lax.rem(z + 1, spans), lax.rem(z + spans - 1, spans)
    for where in (
        [{"sp": above}, {"sp": below}, {"grp": partner}]
        + [{"tp": lax.rem(tp + k, peers)} for k in range(1, 8)]
    ):
        pl.semaphore_signal(barrier, inc=1, device_id=where, device_id_type=MESH)
    pl.semaphore_wait(barrier, 10)

    def knowledge(level, distance):
        for other in (lax.rem(z + distance, spans), lax.rem(z + spans - distance, spans)):
            pl.semaphore_signal(know.at[level], inc=1, device_id={"sp": other}, device_id_type=MESH)

    knowledge(0, 1)

    def z_copy(way, u, owner):
        side = lax.rem(u, 2)
        part = wv.at[pl.ds(2 * side, 2), lines_of(owner), :]
        where = {"sp": above if way == 0 else below}
        return remote(part, part, zs, zr.at[way, u], where)

    def owner_of(way, u):
        t = u // 2 + 1
        return lax.rem(z + spans - t, spans) if way == 0 else lax.rem(z + t, spans)

    def x_copy(way, u):
        side = lax.rem(u, 2)
        lines = lines_of(owner_of(way, u))
        where = {"tp": lax.rem(tp + 2 + 4 * side, peers)}
        return remote(wv.at[1 + side, lines, :], wv.at[7 - 3 * side, lines, :], xs, xr.at[way, u], where)

    def y_copy(way, u):
        side = lax.rem(u, 2)
        lines = lines_of(owner_of(way, u))
        return remote(
            wv.at[1 + side, lines, :], wv.at[6 - side, lines, :], ys, yr.at[way, u], {"grp": partner}
        )

    def d_copy(way, u, start):
        part = wv.at[pl.ds(start, 2), lines_of(owner_of(way, u)), :]
        return remote(part, part, ds_send, ds_recv, {"tp": sibling})

    def ring(u, ways=(0, 1), forward=(0, 1)):
        side = lax.rem(u, 2)
        for way in ways:
            z_copy(way, u, owner_of(way, u)).wait_recv()
            if way in forward:
                z_copy(way, u + 2, owner_of(way, u)).start()
            x_copy(way, u).start()
            y_copy(way, u).start()
            d_copy(way, u, 2 * side).start()

    def spread(u, ways=(0, 1)):
        side = lax.rem(u, 2)
        for way in ways:
            x_copy(way, u).wait_recv()
            y_copy(way, u).wait_recv()
            d_copy(way, u, 6 - 2 * side).start()

    for pos in range(4):
        wv_copies[pos].wait()
    for u in (0, 1):
        for way in (0, 1):
            z_copy(way, u, z).start()

    in_copies[0].wait()
    in_copies[1].wait()
    in_copies[2].wait()
    gain_cols = gain[...].T
    bias_cols = bias[...].T
    for j in range(width // LANES):
        part = pl.ds(j * LANES, LANES)
        wi[part, :] = (wi[part, :].astype(F32) * gain_cols[:, j : j + 1]).astype(BF16)
        biasc[part, :] = jnp.broadcast_to(bias_cols[:, j : j + 1], (LANES, LANES))

    pl.semaphore_wait(know.at[0], 2)
    knowledge(1, 2)

    def halo_copy():
        return remote(proj.at[pl.ds(rows, 8), :], halo, halo_send, halo_recv, {"sp": above})

    def project(i, _):
        k = 3 - i
        base = pl.multiple_of(k * tile, tile)
        tok_copy(k).wait()

        def norms(j, _):
            part = pl.ds(pl.multiple_of(base + j * 64, 64), 64)
            total = jnp.zeros((64, LANES), F32)
            for c in range(width // LANES):
                x = tok[part, c * LANES : (c + 1) * LANES].astype(F32)
                total = total + x * x
            mean = jnp.sum(total, axis=1, keepdims=True) * (1.0 / width)
            invc[part, :] = jnp.broadcast_to(lax.rsqrt(mean + 1e-06), (64, LANES))
            return 0

        lax.fori_loop(0, tile // 64, norms, 0)
        part = pl.ds(base, tile)
        acc = jnp.dot(tok[part, :], wi[...], preferred_element_type=F32)
        inv = invc[part, :]
        for c in range(channels // LANES):
            lane = slice(c * LANES, (c + 1) * LANES)
            proj[pl.ds(base + 8, tile), lane] = (acc[:, lane] * inv).astype(BF16).astype(F32)

        @pl.when(i == 0)
        def _():
            halo_copy().start()

        return 0

    lax.fori_loop(0, 2, project, 0)
    pl.semaphore_wait(know.at[1], 2)
    knowledge(2, 4)
    ring(0)
    lax.fori_loop(2, 4, project, 0)
    ring(1)

    for k in range(3, 8):
        in_copies[k].wait()
    halo_copy().wait_recv()
    proj[0:8, :] = jnp.where(z > 0, halo[...], 0.0)

    scale = -8.0 * softplus(-dparam[...])
    tap = [taps[k : k + 1, :] for k in range(4)]

    def gather_inputs(i):
        for s in range(SEGS):
            base = pl.multiple_of(s * mine + i * STEP, STEP)
            x = proj[pl.ds(base, STEP + 8), :]
            total = pltpu.roll(x, 3, axis=0)[8:] * tap[0]
            total = total + pltpu.roll(x, 2, axis=0)[8:] * tap[1]
            total = total + pltpu.roll(x, 1, axis=0)[8:] * tap[2]
            total = total + x[8:] * tap[3]
            conv[s * STEP : (s + 1) * STEP, :] = total.astype(BF16)

    def scan_tile(i, state):
        gather_inputs(i)
        gates[...] = jnp.dot(conv[...], wrn[...], preferred_element_type=F32)
        for s in range(SEGS):
            base = pl.multiple_of(s * mine + i * STEP, STEP)
            shift = biasc[pl.ds(base, STEP), :]
            part = slice(s * STEP, (s + 1) * STEP)
            for c in range(channels // LANES):
                lane = slice(c * LANES, (c + 1) * LANES)
                rate = jax.nn.sigmoid(gates[part, lane])
                inlet = jax.nn.sigmoid(gates[part, channels + c * LANES : channels + (c + 1) * LANES])
                log_decay = rate * scale[:, lane] + shift
                decay = jnp.exp(log_decay)
                y = -2.0 * log_decay
                series = y * (
                    1.0 - y * (0.5 - y * (1.0 / 6.0 - y * (1.0 / 24.0 - y * (1.0 / 120.0))))
                )
                grown = jnp.where(y < 0.2, series, 1.0 - decay * decay)
                root = grown * lax.rsqrt(jnp.maximum(grown, 1e-37))
                drive = root * inlet * conv[part, lane].astype(F32)
                sa[c, s * PAD : s * PAD + STEP, :] = decay
                sb[c, s * PAD : s * PAD + STEP, :] = drive
        state = list(state)
        for r in range(STEP):
            line = pl.ds(pl.multiple_of((i * STEP + r) * SEGS, SEGS), SEGS)
            for c in range(channels // LANES):
                a = sa[c, pl.ds(r, SEGS, stride=PAD), :]
                b = sb[c, pl.ds(r, SEGS, stride=PAD), :]
                h, p = state[2 * c], state[2 * c + 1]
                h, p = a * h + b, a * p
                ht[c, line, :] = h
                pt[c, line, :] = p
                state[2 * c], state[2 * c + 1] = h, p
        return tuple(state)

    lanes2 = channels // LANES
    state = (jnp.zeros((SEGS, LANES), F32), jnp.ones((SEGS, LANES), F32)) * lanes2
    state = lax.fori_loop(0, 3, scan_tile, state)
    ring(2)
    spread(0)
    pl.semaphore_wait(know.at[2], 2)
    state = lax.fori_loop(3, 6, scan_tile, state)
    ring(3)
    spread(1)
    state = lax.fori_loop(6, 8, scan_tile, state)

    for c in range(lanes2):
        h_end, p_end = state[2 * c], state[2 * c + 1]
        h, p = jnp.zeros((1, LANES), F32), jnp.ones((1, LANES), F32)
        for s in range(SEGS):
            segh[c, s : s + 1, :] = h
            segp[c, s : s + 1, :] = p
            h = p_end[s : s + 1] * h + h_end[s : s + 1]
            p = p_end[s : s + 1] * p
        carry_own[c : c + 1, :] = p
        carry_own[lanes2 + c : lanes2 + c + 1, :] = h

    carry[z] = carry_own[...]
    for k in range(1, 16):
        other = lax.rem(z + k, spans)
        remote(carry_own, carry.at[z], carry_send, carry_recv, {"sp": other}).start()

    in_copies[8].wait()
    for j in range(width // LANES):
        part = pl.ds(j * LANES, LANES)
        wg[part, :] = (wg[part, :].astype(F32) * gain_cols[:, j : j + 1]).astype(BF16)

    def gate(i, _):
        part = pl.ds(pl.multiple_of(i * tile, tile), tile)
        acc = jnp.dot(tok[part, :], wg[...], preferred_element_type=F32)
        inv = invc[part, :]
        for c in range(lanes2):
            lane = slice(c * LANES, (c + 1) * LANES)
            ge[part, lane] = gelu((acc[:, lane] * inv).astype(BF16).astype(F32))
        return 0

    lax.fori_loop(0, 2, gate, 0)
    ring(4)
    spread(2)
    lax.fori_loop(2, 4, gate, 0)
    ring(5)
    spread(3)

    everyone = carry.at[pl.ds(0, 15)]
    local(everyone, everyone, carry_recv).wait()
    incoming = [jnp.zeros((1, LANES), F32) for _ in range(lanes2)]
    for j in range(15):
        for c in range(lanes2):
            p = carry[j, c : c + 1, :]
            h = carry[j, lanes2 + c : lanes2 + c + 1, :]
            incoming[c] = jnp.where(j < z, p * incoming[c] + h, incoming[c])

    def a2a_copy(other):
        return remote(gout.at[other], grecv.at[tp], a2a_send, a2a_recv.at[tp], {"tp": other})

    def ss_copy(other):
        return remote(ss_own.at[other], ss_recv.at[tp], ss_send, ss_recv_sem, {"tp": other})

    ones = jnp.ones((8, LANES), F32)

    def read_out(i, _):
        s = lax.rem(tp + 4 + i, peers)
        total = jnp.zeros((mine, LANES), F32)
        for c in range(lanes2):
            lane = slice(c * LANES, (c + 1) * LANES)
            enter = segp[c, pl.ds(s, 1), :] * incoming[c] + segh[c, pl.ds(s, 1), :]
            lines = pl.ds(s, mine, stride=SEGS)
            state = ht[c, lines, :] + pt[c, lines, :] * enter
            gated = state * ge[pl.ds(pl.multiple_of(s * mine, mine), mine), lane]
            total = total + gated * gated
            gout[s, :, lane] = (gated * ogain[:, lane]).astype(BF16)
        sums = lax.dot_general(
            ones, total, (((1,), (1,)), ((), ())), precision=lax.Precision.HIGHEST,
            preferred_element_type=F32,
        )
        ss_own[s] = sums[0:1, :]

        @pl.when(i != 4)
        def _():
            a2a_copy(s).start()
            ss_copy(s).start()

        return 0

    lax.fori_loop(0, 8, read_out, 0)
    grecv[tp] = gout[tp]
    ss_recv[tp] = ss_own[tp]

    for u in range(6, 12):
        ring(u)
        spread(u - 2)
    ring(12, forward=(0,))
    spread(10)
    ring(13, forward=(1,))
    spread(11)
    ring(14, ways=(0,), forward=())
    spread(12)
    ring(15, ways=(1,), forward=())
    spread(13)
    spread(14, ways=(0,))
    spread(15, ways=(1,))

    for pos in range(4, 8):
        wv_copies[pos].wait()
    for k in range(1, 8):
        other = lax.rem(tp + k, peers)
        remote(gout.at[other], grecv.at[other], a2a_send, a2a_recv.at[other], {"tp": other}).wait_recv()
    seven = ss_recv.at[pl.ds(0, 7)]
    local(seven, seven, ss_recv_sem).wait()
    everything = wv.at[:, pl.ds(0, 15 * share), :]
    local(everything, everything, ds_recv).wait()

    total = ss_recv[0]
    for k in range(1, 8):
        total = total + ss_recv[k]
    scales = lax.rsqrt(total * (1.0 / width) + 1e-06)
    scales = jnp.broadcast_to(scales, (LANES, mine)).T

    def finish(pos, _):
        acc = jnp.zeros((mine, channels), F32)
        for k in range(8):
            acc = acc + jnp.dot(
                grecv[k], wv[pos, k * channels : (k + 1) * channels, :], preferred_element_type=F32
            )
        for c in range(lanes2):
            lane = slice(c * LANES, (c + 1) * LANES)
            obuf[pos, :, lane] = (acc[:, lane] * scales).astype(BF16)
        return 0

    def out_copy(pos):
        return local(obuf.at[pos], out.at[:, pl.ds(column(pos), channels)], out_sem.at[pos])

    for pos in range(8):
        finish(pos, 0)
        out_copy(pos).start()

    sent = wv.at[pl.ds(0, 2), pl.ds(0, 30 * share), :]
    local(sent, sent, zs).wait()
    sent = wv.at[0, pl.ds(0, 30 * share), :]
    local(sent, sent, xs).wait()
    local(sent, sent, ys).wait()
    local(everything, everything, ds_send).wait()
    halo_copy().wait_send()
    local(everyone, everyone, carry_send).wait()
    sent = gout.at[pl.ds(0, 7)]
    local(sent, sent, a2a_send).wait()
    sent = ss_own.at[pl.ds(0, 7)]
    local(sent, sent, ss_send).wait()
    for pos in range(8):
        out_copy(pos).wait()


def body(
    tokens, in_gain, w_input, w_gate, conv_taps, w_rate, w_inlet, decay_param, decay_bias, out_gain, w_out
):
    rows, width = tokens.shape
    channels = w_input.shape[1]
    lanes2 = channels // LANES
    spans, peers = lax.axis_size("sp"), lax.axis_size("tp")
    mine = rows // peers
    vmem = pltpu.VMEM
    dma = pltpu.SemaphoreType.DMA
    scratch = [
        vmem((rows, width), BF16),
        vmem((width, channels), BF16),
        vmem((width, channels), BF16),
        vmem((channels, 2 * channels), BF16),
        vmem((width // LANES, LANES), F32),
        vmem((4, channels), F32),
        vmem((1, channels), F32),
        vmem((rows // LANES, LANES), F32),
        vmem((1, channels), F32),
        vmem((8, width, channels), BF16),
        vmem((8 + rows, channels), F32),
        vmem((8, channels), F32),
        vmem((rows, LANES), F32),
        vmem((rows, LANES), F32),
        vmem((SEGS * STEP, channels), BF16),
        vmem((SEGS * STEP, 2 * channels), F32),
        vmem((lanes2, SEGS * PAD, LANES), F32),
        vmem((lanes2, SEGS * PAD, LANES), F32),
        vmem((lanes2, rows, LANES), F32),
        vmem((lanes2, rows, LANES), F32),
        vmem((rows, channels), F32),
        vmem((lanes2, SEGS, LANES), F32),
        vmem((lanes2, SEGS, LANES), F32),
        vmem((2 * lanes2, LANES), F32),
        vmem((spans, 2 * lanes2, LANES), F32),
        vmem((peers, mine, channels), BF16),
        vmem((peers, mine, channels), BF16),
        vmem((peers, 1, mine), F32),
        vmem((peers, 1, mine), F32),
        vmem((8, mine, channels), BF16),
        dma((4,)),
        dma((9,)),
        dma((8,)),
        dma((8,)),
        dma((2, 16)),
        dma((2, 16)),
        dma((2, 16)),
    ] + [dma(())] * 10 + [dma((8,)), dma(()), dma(()), pltpu.SemaphoreType.REGULAR((3,))]
    spec = pl.BlockSpec(memory_space=pl.ANY)
    return pl.pallas_call(
        kernel,
        out_shape=jax.ShapeDtypeStruct((mine, width), BF16),
        in_specs=[spec] * 11,
        out_specs=spec,
        scratch_shapes=scratch,
        compiler_params=pltpu.CompilerParams(
            collective_id=0, has_side_effects=True, vmem_limit_bytes=60 * 1024 * 1024
        ),
        name="gated_recurrence",
    )(
        tokens,
        in_gain.reshape(width // LANES, LANES),
        w_input,
        w_gate,
        conv_taps,
        w_rate.reshape(channels, channels),
        w_inlet.reshape(channels, channels),
        decay_param.reshape(1, channels),
        decay_bias.reshape(rows // LANES, LANES),
        out_gain.reshape(1, channels),
        w_out,
    )


def solution(mesh):
    return jax.shard_map(
        body,
        mesh=mesh,
        in_specs=(
            P(("grp", "sp"), None),
            P(),
            P(None, "tp"),
            P(None, "tp"),
            P(None, "tp"),
            P("tp", None, None),
            P("tp", None, None),
            P("tp"),
            P("tp", ("grp", "sp")),
            P("tp"),
            P("sp", None),
        ),
        out_specs=P(("grp", "sp", "tp"), None),
        check_vma=False,
    )
```

```python
import functools

import jax
import jax.numpy as jnp
from jax import lax
from jax.experimental import pallas as pl
from jax.experimental.pallas import tpu as pltpu
from jax.sharding import PartitionSpec as P

MESH = pl.DeviceIdType.MESH
F32 = jnp.float32
BF16 = jnp.bfloat16
LANES = 128
SEGS = 8
STEP = 32
PAD = 40


def log1p_small(u):
    series = u * (1.0 - u * (0.5 - u * (1.0 / 3.0 - u * (0.25 - u * (0.2 - u / 6.0)))))
    return jnp.where(u < 0.06, series, jnp.log(1.0 + u))


def softplus(x):
    return jnp.maximum(x, 0.0) + log1p_small(jnp.exp(-jnp.abs(x)))


def gelu(x):
    inner = 0.7978845608028654 * (x + 0.044715 * (x * x * x))
    return 0.5 * x * (1.0 + jnp.tanh(inner))


def kernel(
    tokens_in,
    gain_in,
    w_input_in,
    w_gate_in,
    taps_in,
    w_rate_in,
    w_inlet_in,
    dparam_in,
    bias_in,
    ogain_in,
    w_out_in,
    out,
    tok,
    wi,
    wg,
    wrn,
    gain,
    taps,
    dparam,
    bias,
    ogain,
    wv,
    proj,
    halo,
    biasc,
    invc,
    conv,
    gates,
    sa,
    sb,
    ht,
    pt,
    ge,
    segh,
    segp,
    carry_own,
    state_own,
    carry,
    gout,
    grecv,
    ss_own,
    ss_recv,
    obuf,
    tok_sem,
    in_sem,
    wv_sem,
    out_sem,
    zs,
    zr,
    xr,
    yr,
    xs,
    ys,
    ds_send,
    ds_recv,
    halo_send,
    halo_recv,
    carry_send,
    carry_recv,
    a2a_send,
    a2a_recv,
    ss_send,
    ss_recv_sem,
    know,
):
    grp, z, tp = lax.axis_index("grp"), lax.axis_index("sp"), lax.axis_index("tp")
    spans, peers = lax.axis_size("sp"), lax.axis_size("tp")
    core = lax.rem(tp, 2)
    rows, width = tok.shape
    channels = wi.shape[1]
    block = width // spans
    share = block // 2
    tile = rows // 4
    mine = rows // peers
    first = lax.rem(2 * (tp // 2) + 4 * lax.rem(grp, 2), 8)
    partner = grp + 1 - 2 * lax.rem(grp, 2)
    sibling = tp + 1 - 2 * core

    def column(pos):
        return pl.multiple_of(lax.rem(first + pos, 8) * channels, channels)

    def local(src, dst, sem):
        return pltpu.make_async_copy(src, dst, sem)

    def remote(src, dst, send, recv, where):
        return pltpu.make_async_remote_copy(
            src_ref=src, dst_ref=dst, send_sem=send, recv_sem=recv, device_id=where, device_id_type=MESH
        )

    def lines_of(owner):
        return pl.ds(pl.multiple_of(owner * block + core * share, share), share)

    own_lines = pl.ds(pl.multiple_of(z * block, block), block)
    wv_copies = [
        local(w_out_in.at[:, pl.ds(column(pos), channels)], wv.at[pos, own_lines, :], wv_sem.at[pos])
        for pos in range(8)
    ]
    for pos in range(2):
        wv_copies[pos].start()
    in_copies = [
        local(gain_in, gain, in_sem.at[0]),
        local(w_input_in, wi, in_sem.at[1]),
        local(bias_in, bias, in_sem.at[2]),
        local(taps_in, taps, in_sem.at[3]),
        local(dparam_in, dparam, in_sem.at[4]),
        local(ogain_in, ogain, in_sem.at[5]),
        local(w_rate_in, wrn.at[:, 0:channels], in_sem.at[6]),
        local(w_inlet_in, wrn.at[:, channels : 2 * channels], in_sem.at[7]),
        local(w_gate_in, wg, in_sem.at[8]),
    ]
    for k in (0, 1, 2):
        in_copies[k].start()

    def tok_copy(k):
        part = pl.ds(pl.multiple_of(k * tile, tile), tile)
        return local(tokens_in.at[part, :], tok.at[part, :], tok_sem.at[k])

    for k in (3, 2, 1, 0):
        tok_copy(k).start()
    for k in range(3, 9):
        in_copies[k].start()
    for pos in range(2, 8):
        wv_copies[pos].start()

    last = spans - 1
    barrier = pltpu.get_barrier_semaphore()
    above, below = lax.rem(z + 1, spans), lax.rem(z + last, spans)
    for where in [{"grp": partner}] + [{"tp": lax.rem(tp + k, peers)} for k in range(1, 8)]:
        pl.semaphore_signal(barrier, inc=1, device_id=where, device_id_type=MESH)

    def tell(sem, other):
        pl.semaphore_signal(sem, inc=1, device_id={"sp": other}, device_id_type=MESH)

    pl.when(z < last)(lambda: tell(barrier, above))
    pl.when(z > 0)(lambda: tell(barrier, below))
    ends = jnp.where(z > 0, 1, 0) + jnp.where(z < last, 1, 0)
    pl.semaphore_wait(barrier, 8 + ends)

    def learn(level):
        pl.when(z < last)(lambda: pl.semaphore_wait(know.at[level], 1))

    def teach(level):
        pl.when(z > 0)(lambda: tell(know.at[level], below))

    teach(0)
    pl.when(z > 0)(lambda: pl.semaphore_wait(know.at[3], 1))
    pl.when(z < last)(lambda: tell(know.at[3], above))
    pl.when(z == last)(lambda: tell(know.at[4], above))

    def from_below(span):
        return jnp.minimum(span, 2) + 6

    def from_above(span):
        return 9 - jnp.minimum(span, 2)

    def z_copy(way, t, side, owner):
        part = wv.at[side, lines_of(owner), :]
        where = {"sp": above if way == 0 else below}
        return remote(part, part, zs.at[way, t, side], zr.at[way, t, side], where)

    def owner_of(way, t):
        return lax.rem(z + spans - t, spans) if way == 0 else lax.rem(z + t, spans)

    def share_copy(k, way, t):
        lines = lines_of(owner_of(way, t))
        part = wv.at[0:2, lines, :]
        if k == 0:
            where = {"tp": lax.rem(tp + 2, peers)}
            return remote(part, wv.at[6:8, lines, :], xs, xr.at[0, way, t], where)
        if k == 1:
            where = {"tp": lax.rem(tp + 6, peers)}
            return remote(part, wv.at[2:4, lines, :], xs, xr.at[1, way, t], where)
        if k == 2:
            return remote(part, wv.at[4:6, lines, :], ys, yr.at[way, t], {"grp": partner})
        return remote(part, part, ds_send, ds_recv, {"tp": sibling})

    def ring(way, t):
        owner = owner_of(way, t)
        if way == 0:
            more = t + 1 <= from_below(above)
        else:
            more = jnp.logical_and(z > 0, t + 1 <= from_above(below))
        for side in (0, 1):
            z_copy(way, t, side, owner).wait_recv()

            @pl.when(more)
            def _():
                z_copy(way, t + 1, side, owner).start()

        for k in range(4):
            share_copy(k, way, t).start()

    def spread(way, t):
        for k in range(3):
            share_copy(k, way, t).wait_recv()
        part = wv.at[2:8, lines_of(owner_of(way, t)), :]
        remote(part, part, ds_send, ds_recv, {"tp": sibling}).start()

    def early(act, t):
        pl.when(z >= t)(lambda: act(0, t))

    for pos in range(2):
        wv_copies[pos].wait()

    def first_sends(way):
        for side in (0, 1):
            z_copy(way, 1, side, z).start()

    first_sends(0)
    pl.when(z > 0)(lambda: first_sends(1))

    in_copies[0].wait()
    in_copies[1].wait()
    in_copies[2].wait()
    gain_cols = gain[...].T
    bias_cols = bias[...].T
    for j in range(width // LANES):
        part = pl.ds(j * LANES, LANES)
        wi[part, :] = (wi[part, :].astype(F32) * gain_cols[:, j : j + 1]).astype(BF16)
        biasc[part, :] = jnp.broadcast_to(bias_cols[:, j : j + 1], (LANES, LANES))

    def halo_copy():
        return remote(proj.at[pl.ds(rows, 8), :], halo, halo_send, halo_recv, {"sp": above})

    def project(i, _):
        k = 3 - i
        base = pl.multiple_of(k * tile, tile)
        tok_copy(k).wait()

        def norms(j, _):
            part = pl.ds(pl.multiple_of(base + j * 64, 64), 64)
            total = jnp.zeros((64, LANES), F32)
            for c in range(width // LANES):
                x = tok[part, c * LANES : (c + 1) * LANES].astype(F32)
                total = total + x * x
            mean = jnp.sum(total, axis=1, keepdims=True) * (1.0 / width)
            invc[part, :] = jnp.broadcast_to(lax.rsqrt(mean + 1e-06), (64, LANES))
            return 0

        lax.fori_loop(0, tile // 64, norms, 0)
        part = pl.ds(base, tile)
        acc = jnp.dot(tok[part, :], wi[...], preferred_element_type=F32)
        inv = invc[part, :]
        for c in range(channels // LANES):
            lane = slice(c * LANES, (c + 1) * LANES)
            proj[pl.ds(base + 8, tile), lane] = (acc[:, lane] * inv).astype(BF16).astype(F32)

        @pl.when(jnp.logical_and(i == 0, z < last))
        def _():
            halo_copy().start()

        return 0

    lax.fori_loop(0, 2, project, 0)
    learn(0)
    teach(1)
    early(ring, 1)
    lax.fori_loop(2, 4, project, 0)
    learn(1)
    teach(2)
    ring(1, 1)
    early(ring, 2)
    early(spread, 1)

    for k in range(3, 8):
        in_copies[k].wait()
    pl.when(z > 0)(lambda: halo_copy().wait_recv())

    @pl.when(z > 0)
    def _():
        proj[0:8, :] = halo[...]

    @pl.when(z == 0)
    def _():
        proj[0:8, :] = jnp.zeros((8, channels), F32)

    scale = -8.0 * softplus(-dparam[...])
    tap = [taps[k : k + 1, :] for k in range(4)]

    def gather_inputs(i):
        for s in range(SEGS):
            base = pl.multiple_of(s * mine + i * STEP, STEP)
            x = proj[pl.ds(base, STEP + 8), :]
            total = pltpu.roll(x, 3, axis=0)[8:] * tap[0]
            total = total + pltpu.roll(x, 2, axis=0)[8:] * tap[1]
            total = total + pltpu.roll(x, 1, axis=0)[8:] * tap[2]
            total = total + x[8:] * tap[3]
            conv[s * STEP : (s + 1) * STEP, :] = total.astype(BF16)

    def scan_tile(i, state):
        gather_inputs(i)
        gates[...] = jnp.dot(conv[...], wrn[...], preferred_element_type=F32)
        for s in range(SEGS):
            base = pl.multiple_of(s * mine + i * STEP, STEP)
            shift = biasc[pl.ds(base, STEP), :]
            part = slice(s * STEP, (s + 1) * STEP)
            for c in range(channels // LANES):
                lane = slice(c * LANES, (c + 1) * LANES)
                rate = jax.nn.sigmoid(gates[part, lane])
                inlet = jax.nn.sigmoid(gates[part, channels + c * LANES : channels + (c + 1) * LANES])
                log_decay = rate * scale[:, lane] + shift
                decay = jnp.exp(log_decay)
                y = -2.0 * log_decay
                series = y * (
                    1.0 - y * (0.5 - y * (1.0 / 6.0 - y * (1.0 / 24.0 - y * (1.0 / 120.0))))
                )
                grown = jnp.where(y < 0.2, series, 1.0 - decay * decay)
                root = grown * lax.rsqrt(jnp.maximum(grown, 1e-37))
                drive = root * inlet * conv[part, lane].astype(F32)
                sa[c, s * PAD : s * PAD + STEP, :] = decay
                sb[c, s * PAD : s * PAD + STEP, :] = drive
        state = list(state)
        for r in range(STEP):
            line = pl.ds(pl.multiple_of((i * STEP + r) * SEGS, SEGS), SEGS)
            for c in range(channels // LANES):
                a = sa[c, pl.ds(r, SEGS, stride=PAD), :]
                b = sb[c, pl.ds(r, SEGS, stride=PAD), :]
                h, p = state[2 * c], state[2 * c + 1]
                h, p = a * h + b, a * p
                ht[c, line, :] = h
                pt[c, line, :] = p
                state[2 * c], state[2 * c + 1] = h, p
        return tuple(state)

    lanes2 = channels // LANES
    state = (jnp.zeros((SEGS, LANES), F32), jnp.ones((SEGS, LANES), F32)) * lanes2
    state = lax.fori_loop(0, 3, scan_tile, state)
    early(ring, 3)
    early(spread, 2)
    spread(1, 1)
    state = lax.fori_loop(3, 6, scan_tile, state)
    ring(1, 2)
    early(ring, 4)
    early(spread, 3)
    state = lax.fori_loop(6, 8, scan_tile, state)

    for c in range(lanes2):
        h_end, p_end = state[2 * c], state[2 * c + 1]
        h, p = jnp.zeros((1, LANES), F32), jnp.ones((1, LANES), F32)
        for s in range(SEGS):
            segh[c, s : s + 1, :] = h
            segp[c, s : s + 1, :] = p
            h = p_end[s : s + 1] * h + h_end[s : s + 1]
            p = p_end[s : s + 1] * p
        carry_own[c : c + 1, :] = p
        carry_own[lanes2 + c : lanes2 + c + 1, :] = h

    learn(2)

    def carry_copy(k):
        return remote(
            carry_own, carry.at[k - 1], carry_send.at[k - 1], carry_recv.at[k - 1],
            {"sp": lax.rem(z + k, spans)},
        )

    for k in (1, 2, 3):
        pl.when(z + k < spans)(lambda: carry_copy(k).start())

    in_copies[8].wait()
    for j in range(width // LANES):
        part = pl.ds(j * LANES, LANES)
        wg[part, :] = (wg[part, :].astype(F32) * gain_cols[:, j : j + 1]).astype(BF16)

    def gate(i, _):
        part = pl.ds(pl.multiple_of(i * tile, tile), tile)
        acc = jnp.dot(tok[part, :], wg[...], preferred_element_type=F32)
        inv = invc[part, :]
        for c in range(lanes2):
            lane = slice(c * LANES, (c + 1) * LANES)
            ge[part, lane] = gelu((acc[:, lane] * inv).astype(BF16).astype(F32))
        return 0

    lax.fori_loop(0, 2, gate, 0)
    early(ring, 5)
    early(spread, 4)
    spread(1, 2)
    lax.fori_loop(2, 4, gate, 0)
    ring(1, 3)
    early(ring, 6)
    early(spread, 5)

    def state_copy():
        return remote(
            state_own, carry.at[3], carry_send.at[3], carry_recv.at[3], {"sp": lax.rem(z + 4, spans)}
        )

    def received(copy, slot, k):
        pl.when(z >= k)(lambda: copy.wait_recv())

        @pl.when(z < k)
        def _():
            carry[slot] = jnp.zeros(carry.shape[1:], F32)

    received(state_copy(), 3, 4)
    for k in (1, 2, 3):
        received(carry_copy(k), k - 1, k)
    incoming = []
    for c in range(lanes2):
        h = carry[3, lanes2 + c : lanes2 + c + 1, :]
        for k in (3, 2, 1):
            h = carry[k - 1, c : c + 1, :] * h + carry[k - 1, lanes2 + c : lanes2 + c + 1, :]
        incoming.append(h)
        out_state = carry_own[c : c + 1, :] * h + carry_own[lanes2 + c : lanes2 + c + 1, :]
        state_own[c : c + 1, :] = jnp.zeros((1, LANES), F32)
        state_own[lanes2 + c : lanes2 + c + 1, :] = out_state
    pl.when(z + 4 < spans)(lambda: state_copy().start())

    def a2a_copy(other):
        return remote(gout.at[other], grecv.at[tp], a2a_send, a2a_recv.at[tp], {"tp": other})

    def ss_copy(other):
        return remote(ss_own.at[other], ss_recv.at[tp], ss_send, ss_recv_sem, {"tp": other})

    ones = jnp.ones((8, LANES), F32)

    def read_out(i, _):
        s = lax.rem(tp + 4 + i, peers)
        total = jnp.zeros((mine, LANES), F32)
        for c in range(lanes2):
            lane = slice(c * LANES, (c + 1) * LANES)
            enter = segp[c, pl.ds(s, 1), :] * incoming[c] + segh[c, pl.ds(s, 1), :]
            lines = pl.ds(s, mine, stride=SEGS)
            state = ht[c, lines, :] + pt[c, lines, :] * enter
            gated = state * ge[pl.ds(pl.multiple_of(s * mine, mine), mine), lane]
            total = total + gated * gated
            gout[s, :, lane] = (gated * ogain[:, lane]).astype(BF16)
        sums = lax.dot_general(
            ones, total, (((1,), (1,)), ((), ())), precision=lax.Precision.HIGHEST,
            preferred_element_type=F32,
        )
        ss_own[s] = sums[0:1, :]

        @pl.when(i != 4)
        def _():
            a2a_copy(s).start()
            ss_copy(s).start()

        return 0

    lax.fori_loop(0, 8, read_out, 0)
    grecv[tp] = gout[tp]
    ss_recv[tp] = ss_own[tp]

    done = jnp.minimum(z, 8)

    def late(act, k):
        pl.when(done + k <= from_below(z))(lambda: act(0, done + k))

    def upper(act, t):
        pl.when(t <= from_above(z))(lambda: act(1, t))

    early(ring, 7)
    early(ring, 8)
    ring(1, 4)
    early(spread, 6)
    spread(1, 3)
    early(spread, 7)
    ring(1, 5)
    early(spread, 8)
    spread(1, 4)

    def to_last(t, _):
        for side in (0, 1):
            z_copy(1, t + 1, side, t).start()
        return 0

    @pl.when(z == 0)
    def _():
        pl.semaphore_wait(know.at[4], 1)
        lax.fori_loop(0, 6, to_last, 0)

    ring(1, 6)
    pl.when(z == 0)(lambda: (to_last(6, 0), None)[1])
    spread(1, 5)
    late(ring, 1)
    late(ring, 2)
    spread(1, 6)
    ring(1, 7)
    late(spread, 1)
    late(ring, 3)
    late(spread, 2)
    late(ring, 4)
    spread(1, 7)
    upper(ring, 8)
    late(spread, 3)
    late(ring, 5)
    late(spread, 4)
    upper(ring, 9)
    upper(spread, 8)
    late(ring, 6)
    late(spread, 5)
    upper(spread, 9)
    late(spread, 6)

    for pos in range(2, 8):
        wv_copies[pos].wait()
    for k in range(1, 8):
        other = lax.rem(tp + k, peers)
        remote(gout.at[other], grecv.at[other], a2a_send, a2a_recv.at[other], {"tp": other}).wait_recv()
    seven = ss_recv.at[pl.ds(0, 7)]
    local(seven, seven, ss_recv_sem).wait()
    everything = wv.at[:, pl.ds(0, 15 * share), :]
    local(everything, everything, ds_recv).wait()

    total = ss_recv[0]
    for k in range(1, 8):
        total = total + ss_recv[k]
    scales = lax.rsqrt(total * (1.0 / width) + 1e-06)
    scales = jnp.broadcast_to(scales, (LANES, mine)).T

    def finish(pos, _):
        acc = jnp.zeros((mine, channels), F32)
        for k in range(8):
            acc = acc + jnp.dot(
                grecv[k], wv[pos, k * channels : (k + 1) * channels, :], preferred_element_type=F32
            )
        for c in range(lanes2):
            lane = slice(c * LANES, (c + 1) * LANES)
            obuf[pos, :, lane] = (acc[:, lane] * scales).astype(BF16)
        return 0

    def out_copy(pos):
        return local(obuf.at[pos], out.at[:, pl.ds(column(pos), channels)], out_sem.at[pos])

    for pos in range(8):
        finish(pos, 0)
        out_copy(pos).start()

    for way in (0, 1):
        count = from_below(above) if way == 0 else from_above(below)

        def sent(t, _):
            for side in (0, 1):
                z_copy(way, t + 1, side, z).wait_send()
            return 0

        lax.fori_loop(0, count, sent, 0)
    shared = wv.at[0:4, pl.ds(0, 15 * share), :]
    local(shared, shared, xs).wait()
    shared = wv.at[0:2, pl.ds(0, 15 * share), :]
    local(shared, shared, ys).wait()
    local(everything, everything, ds_send).wait()
    pl.when(z < last)(lambda: halo_copy().wait_send())
    for k in (1, 2, 3):
        pl.when(z + k < spans)(lambda: carry_copy(k).wait_send())
    pl.when(z + 4 < spans)(lambda: state_copy().wait_send())
    sent = gout.at[pl.ds(0, 7)]
    local(sent, sent, a2a_send).wait()
    sent = ss_own.at[pl.ds(0, 7)]
    local(sent, sent, ss_send).wait()
    for pos in range(8):
        out_copy(pos).wait()


def body(
    tokens, in_gain, w_input, w_gate, conv_taps, w_rate, w_inlet, decay_param, decay_bias, out_gain, w_out
):
    rows, width = tokens.shape
    channels = w_input.shape[1]
    lanes2 = channels // LANES
    spans, peers = lax.axis_size("sp"), lax.axis_size("tp")
    mine = rows // peers
    vmem = pltpu.VMEM
    dma = pltpu.SemaphoreType.DMA
    scratch = [
        vmem((rows, width), BF16),
        vmem((width, channels), BF16),
        vmem((width, channels), BF16),
        vmem((channels, 2 * channels), BF16),
        vmem((width // LANES, LANES), F32),
        vmem((4, channels), F32),
        vmem((1, channels), F32),
        vmem((rows // LANES, LANES), F32),
        vmem((1, channels), F32),
        vmem((8, width, channels), BF16),
        vmem((8 + rows, channels), F32),
        vmem((8, channels), F32),
        vmem((rows, LANES), F32),
        vmem((rows, LANES), F32),
        vmem((SEGS * STEP, channels), BF16),
        vmem((SEGS * STEP, 2 * channels), F32),
        vmem((lanes2, SEGS * PAD, LANES), F32),
        vmem((lanes2, SEGS * PAD, LANES), F32),
        vmem((lanes2, rows, LANES), F32),
        vmem((lanes2, rows, LANES), F32),
        vmem((rows, channels), F32),
        vmem((lanes2, SEGS, LANES), F32),
        vmem((lanes2, SEGS, LANES), F32),
        vmem((2 * lanes2, LANES), F32),
        vmem((2 * lanes2, LANES), F32),
        vmem((4, 2 * lanes2, LANES), F32),
        vmem((peers, mine, channels), BF16),
        vmem((peers, mine, channels), BF16),
        vmem((peers, 1, mine), F32),
        vmem((peers, 1, mine), F32),
        vmem((8, mine, channels), BF16),
        dma((4,)),
        dma((9,)),
        dma((8,)),
        dma((8,)),
        dma((2, 10, 2)),
        dma((2, 10, 2)),
        dma((2, 2, 10)),
        dma((2, 10)),
    ]
    scratch += [dma(())] * 6 + [dma((4,)), dma((4,)), dma(()), dma((8,)), dma(()), dma(())]
    scratch += [pltpu.SemaphoreType.REGULAR((5,))]
    spec = pl.BlockSpec(memory_space=pl.ANY)
    return pl.pallas_call(
        kernel,
        out_shape=jax.ShapeDtypeStruct((mine, width), BF16),
        in_specs=[spec] * 11,
        out_specs=spec,
        scratch_shapes=scratch,
        compiler_params=pltpu.CompilerParams(
            collective_id=0, has_side_effects=True, vmem_limit_bytes=60 * 1024 * 1024
        ),
        name="gated_recurrence",
    )(
        tokens,
        in_gain.reshape(width // LANES, LANES),
        w_input,
        w_gate,
        conv_taps,
        w_rate.reshape(channels, channels),
        w_inlet.reshape(channels, channels),
        decay_param.reshape(1, channels),
        decay_bias.reshape(rows // LANES, LANES),
        out_gain.reshape(1, channels),
        w_out,
    )


def solution(mesh):
    return jax.shard_map(
        body,
        mesh=mesh,
        in_specs=(
            P(("grp", "sp"), None),
            P(),
            P(None, "tp"),
            P(None, "tp"),
            P(None, "tp"),
            P("tp", None, None),
            P("tp", None, None),
            P("tp"),
            P("tp", ("grp", "sp")),
            P("tp"),
            P("sp", None),
        ),
        out_specs=P(("grp", "sp", "tp"), None),
        check_vma=False,
    )
```

```python
import functools

import jax
import jax.numpy as jnp
from jax import lax
from jax.experimental import pallas as pl
from jax.experimental.pallas import tpu as pltpu
from jax.sharding import PartitionSpec as P

MESH = pl.DeviceIdType.MESH
F32 = jnp.float32
BF16 = jnp.bfloat16
LANES = 128
SEGS = 8
STEP = 32
PAD = 40


def log1p_small(u):
    series = u * (1.0 - u * (0.5 - u * (1.0 / 3.0 - u * (0.25 - u * (0.2 - u / 6.0)))))
    return jnp.where(u < 0.06, series, jnp.log(1.0 + u))


def softplus(x):
    return jnp.maximum(x, 0.0) + log1p_small(jnp.exp(-jnp.abs(x)))


def gelu(x):
    inner = 0.7978845608028654 * (x + 0.044715 * (x * x * x))
    return 0.5 * x * (1.0 + jnp.tanh(inner))


def kernel(
    tokens_in,
    gain_in,
    w_input_in,
    w_gate_in,
    taps_in,
    w_rate_in,
    w_inlet_in,
    dparam_in,
    bias_in,
    ogain_in,
    w_out_in,
    out,
    tok,
    wi,
    wg,
    wrn,
    gain,
    taps,
    dparam,
    bias,
    ogain,
    wv,
    proj,
    halo,
    biasc,
    invc,
    conv,
    gates,
    sa,
    sb,
    ht,
    pt,
    ge,
    segh,
    segp,
    carry_own,
    state_own,
    carry,
    gout,
    grecv,
    ss_own,
    ss_recv,
    obuf,
    tok_sem,
    in_sem,
    wv_sem,
    out_sem,
    zs,
    zr,
    xr,
    yr,
    xs,
    ys,
    ds_send,
    ds_recv,
    halo_send,
    halo_recv,
    carry_send,
    carry_recv,
    a2a_send,
    a2a_recv,
    ss_send,
    ss_recv_sem,
    know,
):
    grp, z, tp = lax.axis_index("grp"), lax.axis_index("sp"), lax.axis_index("tp")
    spans, peers = lax.axis_size("sp"), lax.axis_size("tp")
    core = lax.rem(tp, 2)
    rows, width = tok.shape
    channels = wi.shape[1]
    lanes2 = channels // LANES
    block = width // spans
    share = block // 2
    tile = rows // 4
    mine = rows // peers
    first = lax.rem(2 * (tp // 2) + 4 * lax.rem(grp, 2), 8)
    partner = grp + 1 - 2 * lax.rem(grp, 2)
    sibling = tp + 1 - 2 * core

    def column(pos):
        return pl.multiple_of(lax.rem(first + pos, 8) * channels, channels)

    def local(src, dst, sem):
        return pltpu.make_async_copy(src, dst, sem)

    def remote(src, dst, send, recv, where):
        return pltpu.make_async_remote_copy(
            src_ref=src, dst_ref=dst, send_sem=send, recv_sem=recv, device_id=where, device_id_type=MESH
        )

    def lines_of(owner):
        return pl.ds(pl.multiple_of(owner * block + core * share, share), share)

    own_lines = pl.ds(pl.multiple_of(z * block, block), block)
    wv_copies = [
        local(w_out_in.at[:, pl.ds(column(pos), channels)], wv.at[pos, own_lines, :], wv_sem.at[pos])
        for pos in range(8)
    ]
    for pos in range(2):
        wv_copies[pos].start()
    in_copies = [
        local(gain_in, gain, in_sem.at[0]),
        local(w_input_in, wi, in_sem.at[1]),
        local(bias_in, bias, in_sem.at[2]),
        local(taps_in, taps, in_sem.at[3]),
        local(dparam_in, dparam, in_sem.at[4]),
        local(ogain_in, ogain, in_sem.at[5]),
        local(w_rate_in, wrn.at[:, 0:channels], in_sem.at[6]),
        local(w_inlet_in, wrn.at[:, channels : 2 * channels], in_sem.at[7]),
        local(w_gate_in, wg, in_sem.at[8]),
    ]
    for k in (0, 1, 2):
        in_copies[k].start()

    def tok_copy(k):
        part = pl.ds(pl.multiple_of(k * tile, tile), tile)
        return local(tokens_in.at[part, :], tok.at[part, :], tok_sem.at[k])

    for k in (3, 2, 1, 0):
        tok_copy(k).start()
    for k in range(3, 9):
        in_copies[k].start()
    for pos in range(2, 8):
        wv_copies[pos].start()

    last = spans - 1
    barrier = pltpu.get_barrier_semaphore()
    above, below = lax.rem(z + 1, spans), lax.rem(z + last, spans)
    for where in (
        [{"sp": above}, {"sp": below}, {"grp": partner}]
        + [{"tp": lax.rem(tp + k, peers)} for k in range(1, 8)]
    ):
        pl.semaphore_signal(barrier, inc=1, device_id=where, device_id_type=MESH)
    pl.semaphore_wait(barrier, 10)

    def learn(level):
        pl.when(z < last)(lambda: pl.semaphore_wait(know.at[level], 1))

    def teach(level):
        @pl.when(z > 0)
        def _():
            pl.semaphore_signal(know.at[level], inc=1, device_id={"sp": below}, device_id_type=MESH)

    teach(0)

    place = below

    def from_below(span):
        return jnp.minimum(lax.rem(span + last, spans), 2) + 6

    def from_above(span):
        return 9 - jnp.minimum(lax.rem(span + last, spans), 2)

    def z_copy(way, t, side, owner):
        part = wv.at[side, lines_of(owner), :]
        where = {"sp": above if way == 0 else below}
        return remote(part, part, zs.at[way, t, side], zr.at[way, t, side], where)

    def owner_of(way, t):
        return lax.rem(z + spans - t, spans) if way == 0 else lax.rem(z + t, spans)

    def share_copy(k, way, t):
        lines = lines_of(owner_of(way, t))
        part = wv.at[0:2, lines, :]
        if k == 0:
            where = {"tp": lax.rem(tp + 2, peers)}
            return remote(part, wv.at[6:8, lines, :], xs, xr.at[0, way, t], where)
        if k == 1:
            where = {"tp": lax.rem(tp + 6, peers)}
            return remote(part, wv.at[2:4, lines, :], xs, xr.at[1, way, t], where)
        if k == 2:
            return remote(part, wv.at[4:6, lines, :], ys, yr.at[way, t], {"grp": partner})
        return remote(part, part, ds_send, ds_recv, {"tp": sibling})

    def ring(way, t):
        owner = owner_of(way, t)
        more = t + 1 <= (from_below(above) if way == 0 else from_above(below))
        for side in (0, 1):
            z_copy(way, t, side, owner).wait_recv()

            @pl.when(more)
            def _():
                z_copy(way, t + 1, side, owner).start()

        for k in range(4):
            share_copy(k, way, t).start()

    def spread(way, t):
        for k in range(3):
            share_copy(k, way, t).wait_recv()
        part = wv.at[2:8, lines_of(owner_of(way, t)), :]
        remote(part, part, ds_send, ds_recv, {"tp": sibling}).start()

    def early(act, t):
        pl.when(place > t)(lambda: act(0, t))

    for pos in range(2):
        wv_copies[pos].wait()

    def first_sends(way):
        for side in (0, 1):
            z_copy(way, 1, side, z).start()

    first_sends(0)
    first_sends(1)

    in_copies[0].wait()
    in_copies[1].wait()
    in_copies[2].wait()
    gain_cols = gain[...].T
    bias_cols = bias[...].T
    for j in range(width // LANES):
        part = pl.ds(j * LANES, LANES)
        wi[part, :] = (wi[part, :].astype(F32) * gain_cols[:, j : j + 1]).astype(BF16)
        biasc[part, :] = jnp.broadcast_to(bias_cols[:, j : j + 1], (LANES, LANES))

    def halo_copy():
        return remote(proj.at[pl.ds(rows, 8), :], halo, halo_send, halo_recv, {"sp": above})

    def project(i, _):
        k = 3 - i
        base = pl.multiple_of(k * tile, tile)
        tok_copy(k).wait()

        part = pl.ds(base, tile)
        acc = jnp.dot(tok[part, :], wi[...], preferred_element_type=F32)
        for j in range(tile // 64):
            lines = pl.ds(pl.multiple_of(base + j * 64, 64), 64)
            total = jnp.zeros((64, LANES), F32)
            for c in range(width // LANES):
                x = tok[lines, c * LANES : (c + 1) * LANES].astype(F32)
                total = total + x * x
            mean = jnp.sum(total, axis=1, keepdims=True) * (1.0 / width)
            inv = jnp.broadcast_to(lax.rsqrt(mean + 1e-06), (64, LANES))
            invc[lines, :] = inv
            for c in range(lanes2):
                lane = slice(c * LANES, (c + 1) * LANES)
                scaled = acc[j * 64 : (j + 1) * 64, lane] * inv
                proj[pl.ds(base + 8 + j * 64, 64), lane] = scaled.astype(BF16).astype(F32)

        @pl.when(jnp.logical_and(i == 0, z < last))
        def _():
            halo_copy().start()

        return 0

    lax.fori_loop(0, 2, project, 0)
    learn(0)
    teach(1)
    early(ring, 1)
    lax.fori_loop(2, 4, project, 0)
    learn(1)
    teach(2)
    ring(1, 1)
    early(ring, 2)

    for k in range(3, 8):
        in_copies[k].wait()
    pl.when(z > 0)(lambda: halo_copy().wait_recv())

    @pl.when(z > 0)
    def _():
        proj[0:8, :] = halo[...]

    @pl.when(z == 0)
    def _():
        proj[0:8, :] = jnp.zeros((8, channels), F32)

    scale = -8.0 * softplus(-dparam[...])
    tap = [taps[k : k + 1, :] for k in range(4)]

    def gather_inputs(i):
        for s in range(SEGS):
            base = pl.multiple_of(s * mine + i * STEP, STEP)
            x = proj[pl.ds(base, STEP + 8), :]
            total = pltpu.roll(x, 3, axis=0)[8:] * tap[0]
            total = total + pltpu.roll(x, 2, axis=0)[8:] * tap[1]
            total = total + pltpu.roll(x, 1, axis=0)[8:] * tap[2]
            total = total + x[8:] * tap[3]
            conv[s * STEP : (s + 1) * STEP, :] = total.astype(BF16)

    def scan_tile(i, state):
        gather_inputs(i)
        gates[...] = jnp.dot(conv[...], wrn[...], preferred_element_type=F32)
        for s in range(SEGS):
            base = pl.multiple_of(s * mine + i * STEP, STEP)
            shift = biasc[pl.ds(base, STEP), :]
            part = slice(s * STEP, (s + 1) * STEP)
            for c in range(channels // LANES):
                lane = slice(c * LANES, (c + 1) * LANES)
                rate = jax.nn.sigmoid(gates[part, lane])
                inlet = jax.nn.sigmoid(gates[part, channels + c * LANES : channels + (c + 1) * LANES])
                log_decay = rate * scale[:, lane] + shift
                decay = jnp.exp(log_decay)
                y = -2.0 * log_decay
                series = y * (
                    1.0 - y * (0.5 - y * (1.0 / 6.0 - y * (1.0 / 24.0 - y * (1.0 / 120.0))))
                )
                grown = jnp.where(y < 0.2, series, 1.0 - decay * decay)
                root = grown * lax.rsqrt(jnp.maximum(grown, 1e-37))
                drive = root * inlet * conv[part, lane].astype(F32)
                sa[c, s * PAD : s * PAD + STEP, :] = decay
                sb[c, s * PAD : s * PAD + STEP, :] = drive
        state = list(state)
        for r in range(STEP):
            line = pl.ds(pl.multiple_of((i * STEP + r) * SEGS, SEGS), SEGS)
            for c in range(channels // LANES):
                a = sa[c, pl.ds(r, SEGS, stride=PAD), :]
                b = sb[c, pl.ds(r, SEGS, stride=PAD), :]
                h, p = state[2 * c], state[2 * c + 1]
                h, p = a * h + b, a * p
                ht[c, line, :] = h
                pt[c, line, :] = p
                state[2 * c], state[2 * c + 1] = h, p
        return tuple(state)

    state = (jnp.zeros((SEGS, LANES), F32), jnp.ones((SEGS, LANES), F32)) * lanes2
    state = lax.fori_loop(0, 3, scan_tile, state)
    early(ring, 3)
    state = lax.fori_loop(3, 6, scan_tile, state)
    ring(1, 2)
    early(ring, 4)
    early(spread, 1)
    spread(1, 1)
    state = lax.fori_loop(6, 8, scan_tile, state)

    for c in range(lanes2):
        h_end, p_end = state[2 * c], state[2 * c + 1]
        h, p = jnp.zeros((1, LANES), F32), jnp.ones((1, LANES), F32)
        for s in range(SEGS):
            segh[c, s : s + 1, :] = h
            segp[c, s : s + 1, :] = p
            h = p_end[s : s + 1] * h + h_end[s : s + 1]
            p = p_end[s : s + 1] * p
        carry_own[c : c + 1, :] = p
        carry_own[lanes2 + c : lanes2 + c + 1, :] = h

    learn(2)

    def carry_copy(k):
        return remote(
            carry_own, carry.at[k - 1], carry_send.at[k - 1], carry_recv.at[k - 1],
            {"sp": lax.rem(z + k, spans)},
        )

    for k in (1, 2, 3):
        pl.when(z + k < spans)(lambda: carry_copy(k).start())

    in_copies[8].wait()
    for j in range(width // LANES):
        part = pl.ds(j * LANES, LANES)
        wg[part, :] = (wg[part, :].astype(F32) * gain_cols[:, j : j + 1]).astype(BF16)

    def gate(i, _):
        part = pl.ds(pl.multiple_of(i * tile, tile), tile)
        acc = jnp.dot(tok[part, :], wg[...], preferred_element_type=F32)
        inv = invc[part, :]
        for c in range(lanes2):
            lane = slice(c * LANES, (c + 1) * LANES)
            ge[part, lane] = gelu((acc[:, lane] * inv).astype(BF16).astype(F32))
        return 0

    lax.fori_loop(0, 2, gate, 0)
    early(ring, 5)
    early(spread, 2)
    early(spread, 3)
    lax.fori_loop(2, 4, gate, 0)
    ring(1, 3)
    early(ring, 6)
    spread(1, 2)
    early(spread, 4)

    def state_copy():
        return remote(
            state_own, carry.at[3], carry_send.at[3], carry_recv.at[3], {"sp": lax.rem(z + 4, spans)}
        )

    def received(copy, slot, k):
        pl.when(z >= k)(lambda: copy.wait_recv())

        @pl.when(z < k)
        def _():
            carry[slot] = jnp.zeros(carry.shape[1:], F32)

    received(state_copy(), 3, 4)
    for k in (1, 2, 3):
        received(carry_copy(k), k - 1, k)
    incoming = []
    for c in range(lanes2):
        h = carry[3, lanes2 + c : lanes2 + c + 1, :]
        for k in (3, 2, 1):
            h = carry[k - 1, c : c + 1, :] * h + carry[k - 1, lanes2 + c : lanes2 + c + 1, :]
        incoming.append(h)
        out_state = carry_own[c : c + 1, :] * h + carry_own[lanes2 + c : lanes2 + c + 1, :]
        state_own[c : c + 1, :] = jnp.zeros((1, LANES), F32)
        state_own[lanes2 + c : lanes2 + c + 1, :] = out_state
    pl.when(z + 4 < spans)(lambda: state_copy().start())

    def a2a_copy(other):
        return remote(gout.at[other], grecv.at[tp], a2a_send, a2a_recv.at[tp], {"tp": other})

    def ss_copy(other):
        return remote(ss_own.at[other], ss_recv.at[tp], ss_send, ss_recv_sem, {"tp": other})

    ones = jnp.ones((8, LANES), F32)

    def read_out(i, _):
        s = lax.rem(tp + 4 + i, peers)
        total = jnp.zeros((mine, LANES), F32)
        for c in range(lanes2):
            lane = slice(c * LANES, (c + 1) * LANES)
            enter = segp[c, pl.ds(s, 1), :] * incoming[c] + segh[c, pl.ds(s, 1), :]
            lines = pl.ds(s, mine, stride=SEGS)
            state = ht[c, lines, :] + pt[c, lines, :] * enter
            gated = state * ge[pl.ds(pl.multiple_of(s * mine, mine), mine), lane]
            total = total + gated * gated
            gout[s, :, lane] = (gated * ogain[:, lane]).astype(BF16)
        sums = lax.dot_general(
            ones, total, (((1,), (1,)), ((), ())), precision=lax.Precision.HIGHEST,
            preferred_element_type=F32,
        )
        ss_own[s] = sums[0:1, :]

        @pl.when(i != 4)
        def _():
            a2a_copy(s).start()
            ss_copy(s).start()

        return 0

    lax.fori_loop(0, 8, read_out, 0)
    grecv[tp] = gout[tp]
    ss_recv[tp] = ss_own[tp]

    done = jnp.clip(place - 1, 0, 8)

    def late(act, k):
        pl.when(done + k <= from_below(z))(lambda: act(0, done + k))

    def upper(act, t):
        pl.when(t <= from_above(z))(lambda: act(1, t))

    early(ring, 7)
    early(ring, 8)
    ring(1, 4)
    late(ring, 1)
    ring(1, 5)
    early(spread, 5)
    spread(1, 3)
    late(ring, 2)
    ring(1, 6)
    early(spread, 6)
    late(ring, 3)
    ring(1, 7)
    late(ring, 4)
    late(ring, 5)
    upper(ring, 8)
    late(ring, 6)
    upper(ring, 9)
    late(ring, 7)
    early(spread, 7)
    early(spread, 8)
    spread(1, 4)
    late(spread, 1)
    spread(1, 5)
    late(spread, 2)
    spread(1, 6)
    late(spread, 3)
    spread(1, 7)
    late(spread, 4)
    late(spread, 5)
    upper(spread, 8)
    late(spread, 6)
    upper(spread, 9)
    late(spread, 7)

    for pos in range(2, 8):
        wv_copies[pos].wait()
    for k in range(1, 8):
        other = lax.rem(tp + k, peers)
        remote(gout.at[other], grecv.at[other], a2a_send, a2a_recv.at[other], {"tp": other}).wait_recv()
    seven = ss_recv.at[pl.ds(0, 7)]
    local(seven, seven, ss_recv_sem).wait()
    everything = wv.at[:, pl.ds(0, 15 * share), :]
    local(everything, everything, ds_recv).wait()

    total = ss_recv[0]
    for k in range(1, 8):
        total = total + ss_recv[k]
    scales = lax.rsqrt(total * (1.0 / width) + 1e-06)
    scales = jnp.broadcast_to(scales, (LANES, mine)).T

    def finish(pos, _):
        acc = jnp.zeros((mine, channels), F32)
        for k in range(8):
            acc = acc + jnp.dot(
                grecv[k], wv[pos, k * channels : (k + 1) * channels, :], preferred_element_type=F32
            )
        for c in range(lanes2):
            lane = slice(c * LANES, (c + 1) * LANES)
            obuf[pos, :, lane] = (acc[:, lane] * scales).astype(BF16)
        return 0

    def out_copy(pos):
        return local(obuf.at[pos], out.at[:, pl.ds(column(pos), channels)], out_sem.at[pos])

    for pos in range(8):
        finish(pos, 0)
        out_copy(pos).start()

    for way in (0, 1):
        count = from_below(above) if way == 0 else from_above(below)

        def sent(t, _):
            for side in (0, 1):
                z_copy(way, t + 1, side, z).wait_send()
            return 0

        lax.fori_loop(0, count, sent, 0)
    shared = wv.at[0:4, pl.ds(0, 15 * share), :]
    local(shared, shared, xs).wait()
    shared = wv.at[0:2, pl.ds(0, 15 * share), :]
    local(shared, shared, ys).wait()
    local(everything, everything, ds_send).wait()
    pl.when(z < last)(lambda: halo_copy().wait_send())
    for k in (1, 2, 3):
        pl.when(z + k < spans)(lambda: carry_copy(k).wait_send())
    pl.when(z + 4 < spans)(lambda: state_copy().wait_send())
    sent = gout.at[pl.ds(0, 7)]
    local(sent, sent, a2a_send).wait()
    sent = ss_own.at[pl.ds(0, 7)]
    local(sent, sent, ss_send).wait()
    for pos in range(8):
        out_copy(pos).wait()


def body(
    tokens, in_gain, w_input, w_gate, conv_taps, w_rate, w_inlet, decay_param, decay_bias, out_gain, w_out
):
    rows, width = tokens.shape
    channels = w_input.shape[1]
    lanes2 = channels // LANES
    spans, peers = lax.axis_size("sp"), lax.axis_size("tp")
    mine = rows // peers
    vmem = pltpu.VMEM
    dma = pltpu.SemaphoreType.DMA
    scratch = [
        vmem((rows, width), BF16),
        vmem((width, channels), BF16),
        vmem((width, channels), BF16),
        vmem((channels, 2 * channels), BF16),
        vmem((width // LANES, LANES), F32),
        vmem((4, channels), F32),
        vmem((1, channels), F32),
        vmem((rows // LANES, LANES), F32),
        vmem((1, channels), F32),
        vmem((8, width, channels), BF16),
        vmem((8 + rows, channels), F32),
        vmem((8, channels), F32),
        vmem((rows, LANES), F32),
        vmem((rows, LANES), F32),
        vmem((SEGS * STEP, channels), BF16),
        vmem((SEGS * STEP, 2 * channels), F32),
        vmem((lanes2, SEGS * PAD, LANES), F32),
        vmem((lanes2, SEGS * PAD, LANES), F32),
        vmem((lanes2, rows, LANES), F32),
        vmem((lanes2, rows, LANES), F32),
        vmem((rows, channels), F32),
        vmem((lanes2, SEGS, LANES), F32),
        vmem((lanes2, SEGS, LANES), F32),
        vmem((2 * lanes2, LANES), F32),
        vmem((2 * lanes2, LANES), F32),
        vmem((4, 2 * lanes2, LANES), F32),
        vmem((peers, mine, channels), BF16),
        vmem((peers, mine, channels), BF16),
        vmem((peers, 1, mine), F32),
        vmem((peers, 1, mine), F32),
        vmem((8, mine, channels), BF16),
        dma((4,)),
        dma((9,)),
        dma((8,)),
        dma((8,)),
        dma((2, 10, 2)),
        dma((2, 10, 2)),
        dma((2, 2, 10)),
        dma((2, 10)),
    ]
    scratch += [dma(())] * 6 + [dma((4,)), dma((4,)), dma(()), dma((8,)), dma(()), dma(())]
    scratch += [pltpu.SemaphoreType.REGULAR((3,))]
    spec = pl.BlockSpec(memory_space=pl.ANY)
    return pl.pallas_call(
        kernel,
        out_shape=jax.ShapeDtypeStruct((mine, width), BF16),
        in_specs=[spec] * 11,
        out_specs=spec,
        scratch_shapes=scratch,
        compiler_params=pltpu.CompilerParams(
            collective_id=0, has_side_effects=True, vmem_limit_bytes=60 * 1024 * 1024
        ),
        name="gated_recurrence",
    )(
        tokens,
        in_gain.reshape(width // LANES, LANES),
        w_input,
        w_gate,
        conv_taps,
        w_rate.reshape(channels, channels),
        w_inlet.reshape(channels, channels),
        decay_param.reshape(1, channels),
        decay_bias.reshape(rows // LANES, LANES),
        out_gain.reshape(1, channels),
        w_out,
    )


def solution(mesh):
    return jax.shard_map(
        body,
        mesh=mesh,
        in_specs=(
            P(("grp", "sp"), None),
            P(),
            P(None, "tp"),
            P(None, "tp"),
            P(None, "tp"),
            P("tp", None, None),
            P("tp", None, None),
            P("tp"),
            P("tp", ("grp", "sp")),
            P("tp"),
            P("sp", None),
        ),
        out_specs=P(("grp", "sp", "tp"), None),
        check_vma=False,
    )
```

```python
import functools

import jax
import jax.numpy as jnp
from jax import lax
from jax.experimental import pallas as pl
from jax.experimental.pallas import tpu as pltpu
from jax.sharding import PartitionSpec as P

MESH = pl.DeviceIdType.MESH
F32 = jnp.float32
BF16 = jnp.bfloat16
LANES = 128
SEGS = 8
STEP = 32
PAD = 40


def log1p_small(u):
    series = u * (1.0 - u * (0.5 - u * (1.0 / 3.0 - u * (0.25 - u * (0.2 - u / 6.0)))))
    return jnp.where(u < 0.06, series, jnp.log(1.0 + u))


def softplus(x):
    return jnp.maximum(x, 0.0) + log1p_small(jnp.exp(-jnp.abs(x)))


def gelu(x):
    inner = 0.7978845608028654 * (x + 0.044715 * (x * x * x))
    return 0.5 * x * (1.0 + jnp.tanh(inner))


def kernel(
    tokens_in,
    gain_in,
    w_input_in,
    w_gate_in,
    taps_in,
    w_rate_in,
    w_inlet_in,
    dparam_in,
    bias_in,
    ogain_in,
    w_out_in,
    out,
    tok,
    wi,
    wg,
    wrn,
    gain,
    taps,
    dparam,
    bias,
    ogain,
    wv,
    proj,
    halo,
    biasc,
    invc,
    conv,
    gates,
    sa,
    sb,
    ht,
    pt,
    ge,
    segh,
    segp,
    carry_own,
    state_own,
    carry,
    gout,
    grecv,
    ss_own,
    ss_recv,
    obuf,
    tok_sem,
    in_sem,
    wv_sem,
    out_sem,
    zs,
    zr,
    xr,
    yr,
    xs,
    ys,
    ds_send,
    ds_recv,
    halo_send,
    halo_recv,
    carry_send,
    carry_recv,
    a2a_send,
    a2a_recv,
    ss_send,
    ss_recv_sem,
    know,
):
    grp, z, tp = lax.axis_index("grp"), lax.axis_index("sp"), lax.axis_index("tp")
    spans, peers = lax.axis_size("sp"), lax.axis_size("tp")
    core = lax.rem(tp, 2)
    rows, width = tok.shape
    channels = wi.shape[1]
    lanes2 = channels // LANES
    block = width // spans
    share = block // 2
    tile = rows // 4
    mine = rows // peers
    first = lax.rem(2 * (tp // 2) + 4 * lax.rem(grp, 2), 8)
    partner = grp + 1 - 2 * lax.rem(grp, 2)
    sibling = tp + 1 - 2 * core

    def column(pos):
        return pl.multiple_of(lax.rem(first + pos, 8) * channels, channels)

    def local(src, dst, sem):
        return pltpu.make_async_copy(src, dst, sem)

    def remote(src, dst, send, recv, where):
        return pltpu.make_async_remote_copy(
            src_ref=src, dst_ref=dst, send_sem=send, recv_sem=recv, device_id=where, device_id_type=MESH
        )

    def lines_of(owner):
        return pl.ds(pl.multiple_of(owner * block + core * share, share), share)

    own_lines = pl.ds(pl.multiple_of(z * block, block), block)
    wv_copies = [
        local(w_out_in.at[:, pl.ds(column(pos), channels)], wv.at[pos, own_lines, :], wv_sem.at[pos])
        for pos in range(8)
    ]
    for pos in range(4):
        wv_copies[pos].start()
    in_copies = [
        local(gain_in, gain, in_sem.at[0]),
        local(w_input_in, wi, in_sem.at[1]),
        local(bias_in, bias, in_sem.at[2]),
        local(taps_in, taps, in_sem.at[3]),
        local(dparam_in, dparam, in_sem.at[4]),
        local(ogain_in, ogain, in_sem.at[5]),
        local(w_rate_in, wrn.at[:, 0:channels], in_sem.at[6]),
        local(w_inlet_in, wrn.at[:, channels : 2 * channels], in_sem.at[7]),
        local(w_gate_in, wg, in_sem.at[8]),
    ]
    for k in (0, 1, 2):
        in_copies[k].start()

    def tok_copy(k):
        part = pl.ds(pl.multiple_of(k * tile, tile), tile)
        return local(tokens_in.at[part, :], tok.at[part, :], tok_sem.at[k])

    for k in (3, 2, 1, 0):
        tok_copy(k).start()
    for k in range(3, 9):
        in_copies[k].start()
    for pos in range(4, 8):
        wv_copies[pos].start()

    last = spans - 1
    barrier = pltpu.get_barrier_semaphore()
    above, below = lax.rem(z + 1, spans), lax.rem(z + last, spans)
    for where in (
        [{"sp": above}, {"sp": below}, {"grp": partner}]
        + [{"tp": lax.rem(tp + k, peers)} for k in range(1, 8)]
    ):
        pl.semaphore_signal(barrier, inc=1, device_id=where, device_id_type=MESH)

    def learn(level):
        pl.when(z < last)(lambda: pl.semaphore_wait(know.at[level], 1))

    def teach(level):
        @pl.when(z > 0)
        def _():
            pl.semaphore_signal(know.at[level], inc=1, device_id={"sp": below}, device_id_type=MESH)

    place = below

    def from_below(span):
        return jnp.minimum(lax.rem(span + last, spans), 2) + 6

    def from_above(span):
        return 9 - jnp.minimum(lax.rem(span + last, spans), 2)

    def z_copy(way, t, side, owner):
        part = wv.at[2 * side : 2 * side + 2, lines_of(owner), :]
        where = {"sp": above if way == 0 else below}
        return remote(part, part, zs.at[way, t, side], zr.at[way, t, side], where)

    def owner_of(way, t):
        return lax.rem(z + spans - t, spans) if way == 0 else lax.rem(z + t, spans)

    def share_copy(k, way, t):
        lines = lines_of(owner_of(way, t))
        if k == 0:
            where = {"tp": lax.rem(tp + 2, peers)}
            return remote(wv.at[1, lines, :], wv.at[7, lines, :], xs, xr.at[0, way, t], where)
        if k == 1:
            where = {"tp": lax.rem(tp + 6, peers)}
            return remote(wv.at[2, lines, :], wv.at[4, lines, :], xs, xr.at[1, way, t], where)
        if k == 2:
            return remote(
                wv.at[1:3, lines, :], wv.at[5:7, lines, :], ys, yr.at[way, t], {"grp": partner}
            )
        part = wv.at[0:4, lines, :]
        return remote(part, part, ds_send, ds_recv, {"tp": sibling})

    def ring(way, t):
        owner = owner_of(way, t)
        more = t + 1 <= (from_below(above) if way == 0 else from_above(below))
        for side in (0, 1):
            z_copy(way, t, side, owner).wait_recv()

            @pl.when(more)
            def _():
                z_copy(way, t + 1, side, owner).start()

        for k in range(4):
            share_copy(k, way, t).start()

    def spread(way, t):
        for k in range(3):
            share_copy(k, way, t).wait_recv()
        part = wv.at[4:8, lines_of(owner_of(way, t)), :]
        remote(part, part, ds_send, ds_recv, {"tp": sibling}).start()

    def early(act, t):
        step = t - jnp.where(z > 0, 0, 1)
        pl.when(jnp.logical_and(place > t, step > 0))(lambda: act(0, step))

    def first_sends(way):
        for side in (0, 1):
            z_copy(way, 1, side, z).start()


    in_copies[0].wait()
    in_copies[1].wait()
    in_copies[2].wait()
    gain_cols = gain[...].T
    bias_cols = bias[...].T
    for j in range(width // LANES):
        part = pl.ds(j * LANES, LANES)
        wi[part, :] = (wi[part, :].astype(F32) * gain_cols[:, j : j + 1]).astype(BF16)
        biasc[part, :] = jnp.broadcast_to(bias_cols[:, j : j + 1], (LANES, LANES))

    def halo_copy():
        return remote(proj.at[pl.ds(rows, 8), :], halo, halo_send, halo_recv, {"sp": above})

    def project(i, _):
        k = 3 - i
        base = pl.multiple_of(k * tile, tile)
        tok_copy(k).wait()

        part = pl.ds(base, tile)
        acc = jnp.dot(tok[part, :], wi[...], preferred_element_type=F32)
        for j in range(tile // 64):
            lines = pl.ds(pl.multiple_of(base + j * 64, 64), 64)
            total = jnp.zeros((64, LANES), F32)
            for c in range(width // LANES):
                x = tok[lines, c * LANES : (c + 1) * LANES].astype(F32)
                total = total + x * x
            mean = jnp.sum(total, axis=1, keepdims=True) * (1.0 / width)
            inv = jnp.broadcast_to(lax.rsqrt(mean + 1e-06), (64, LANES))
            invc[lines, :] = inv
            for c in range(lanes2):
                lane = slice(c * LANES, (c + 1) * LANES)
                scaled = acc[j * 64 : (j + 1) * 64, lane] * inv
                proj[pl.ds(base + 8 + j * 64, 64), lane] = scaled.astype(BF16).astype(F32)

        return 0

    lax.fori_loop(0, 1, project, 0)
    pl.semaphore_wait(barrier, 10)
    pl.when(z < last)(lambda: halo_copy().start())
    teach(0)
    for pos in range(4):
        wv_copies[pos].wait()
    first_sends(0)
    first_sends(1)
    lax.fori_loop(1, 3, project, 0)
    learn(0)
    teach(1)
    early(ring, 1)
    lax.fori_loop(3, 4, project, 0)
    learn(1)
    teach(2)
    ring(1, 1)
    early(ring, 2)

    for k in range(3, 8):
        in_copies[k].wait()
    pl.when(z > 0)(lambda: halo_copy().wait_recv())

    @pl.when(z > 0)
    def _():
        proj[0:8, :] = halo[...]

    @pl.when(z == 0)
    def _():
        proj[0:8, :] = jnp.zeros((8, channels), F32)

    scale = -8.0 * softplus(-dparam[...])
    tap = [taps[k : k + 1, :] for k in range(4)]

    def gather_inputs(i):
        for s in range(SEGS):
            base = pl.multiple_of(s * mine + i * STEP, STEP)
            x = proj[pl.ds(base, STEP + 8), :]
            total = pltpu.roll(x, 3, axis=0)[8:] * tap[0]
            total = total + pltpu.roll(x, 2, axis=0)[8:] * tap[1]
            total = total + pltpu.roll(x, 1, axis=0)[8:] * tap[2]
            total = total + x[8:] * tap[3]
            conv[s * STEP : (s + 1) * STEP, :] = total.astype(BF16)

    def scan_tile(i, state):
        gather_inputs(i)
        gates[...] = jnp.dot(conv[...], wrn[...], preferred_element_type=F32)
        for s in range(SEGS):
            base = pl.multiple_of(s * mine + i * STEP, STEP)
            shift = biasc[pl.ds(base, STEP), :]
            part = slice(s * STEP, (s + 1) * STEP)
            for c in range(channels // LANES):
                lane = slice(c * LANES, (c + 1) * LANES)
                rate = jax.nn.sigmoid(gates[part, lane])
                inlet = jax.nn.sigmoid(gates[part, channels + c * LANES : channels + (c + 1) * LANES])
                log_decay = rate * scale[:, lane] + shift
                decay = jnp.exp(log_decay)
                y = -2.0 * log_decay
                series = y * (
                    1.0 - y * (0.5 - y * (1.0 / 6.0 - y * (1.0 / 24.0 - y * (1.0 / 120.0))))
                )
                grown = jnp.where(y < 0.2, series, 1.0 - decay * decay)
                root = grown * lax.rsqrt(jnp.maximum(grown, 1e-37))
                drive = root * inlet * conv[part, lane].astype(F32)
                sa[c, s * PAD : s * PAD + STEP, :] = decay
                sb[c, s * PAD : s * PAD + STEP, :] = drive
        state = list(state)
        for r in range(STEP):
            line = pl.ds(pl.multiple_of((i * STEP + r) * SEGS, SEGS), SEGS)
            for c in range(channels // LANES):
                a = sa[c, pl.ds(r, SEGS, stride=PAD), :]
                b = sb[c, pl.ds(r, SEGS, stride=PAD), :]
                h, p = state[2 * c], state[2 * c + 1]
                h, p = a * h + b, a * p
                ht[c, line, :] = h
                pt[c, line, :] = p
                state[2 * c], state[2 * c + 1] = h, p
        return tuple(state)

    state = (jnp.zeros((SEGS, LANES), F32), jnp.ones((SEGS, LANES), F32)) * lanes2
    state = lax.fori_loop(0, 3, scan_tile, state)
    early(ring, 3)
    state = lax.fori_loop(3, 6, scan_tile, state)
    ring(1, 2)
    early(ring, 4)
    early(spread, 1)
    spread(1, 1)
    state = lax.fori_loop(6, 8, scan_tile, state)

    for c in range(lanes2):
        h_end, p_end = state[2 * c], state[2 * c + 1]
        h, p = jnp.zeros((1, LANES), F32), jnp.ones((1, LANES), F32)
        for s in range(SEGS):
            segh[c, s : s + 1, :] = h
            segp[c, s : s + 1, :] = p
            h = p_end[s : s + 1] * h + h_end[s : s + 1]
            p = p_end[s : s + 1] * p
        carry_own[c : c + 1, :] = p
        carry_own[lanes2 + c : lanes2 + c + 1, :] = h

    learn(2)

    def carry_copy(k):
        return remote(
            carry_own, carry.at[k - 1], carry_send.at[k - 1], carry_recv.at[k - 1],
            {"sp": lax.rem(z + k, spans)},
        )

    for k in (1, 2, 3):
        pl.when(z + k < spans)(lambda: carry_copy(k).start())

    def state_copy():
        return remote(
            state_own, carry.at[3], carry_send.at[3], carry_recv.at[3], {"sp": lax.rem(z + 4, spans)}
        )

    @pl.when(z == 0)
    def _():
        state_own[...] = carry_own[...]
        state_copy().start()

    in_copies[8].wait()
    for j in range(width // LANES):
        part = pl.ds(j * LANES, LANES)
        wg[part, :] = (wg[part, :].astype(F32) * gain_cols[:, j : j + 1]).astype(BF16)

    def gate(i, _):
        part = pl.ds(pl.multiple_of(i * tile, tile), tile)
        acc = jnp.dot(tok[part, :], wg[...], preferred_element_type=F32)
        inv = invc[part, :]
        for c in range(lanes2):
            lane = slice(c * LANES, (c + 1) * LANES)
            ge[part, lane] = gelu((acc[:, lane] * inv).astype(BF16).astype(F32))
        return 0

    lax.fori_loop(0, 2, gate, 0)
    early(ring, 5)
    early(spread, 2)
    early(spread, 3)
    lax.fori_loop(2, 4, gate, 0)
    ring(1, 3)
    early(ring, 6)
    spread(1, 2)
    early(spread, 4)

    done = jnp.clip(place - 1, 0, jnp.where(z > 0, 8, 7))

    def late(act, k):
        pl.when(done + k <= from_below(z))(lambda: act(0, done + k))

    def upper(act, t):
        pl.when(t <= from_above(z))(lambda: act(1, t))

    def services():
        early(ring, 7)
        early(ring, 8)
        ring(1, 4)
        early(spread, 5)
        spread(1, 3)
        late(ring, 1)
        early(spread, 6)
        ring(1, 5)
        early(spread, 7)

    pl.when(z > 0)(services)

    def received(copy, slot, k):
        pl.when(z >= k)(lambda: copy.wait_recv())

        @pl.when(z < k)
        def _():
            carry[slot] = jnp.zeros(carry.shape[1:], F32)

    received(state_copy(), 3, 4)
    for k in (1, 2, 3):
        received(carry_copy(k), k - 1, k)
    incoming, out_states = [], []
    for c in range(lanes2):
        h = carry[3, lanes2 + c : lanes2 + c + 1, :]
        for k in (3, 2, 1):
            h = carry[k - 1, c : c + 1, :] * h + carry[k - 1, lanes2 + c : lanes2 + c + 1, :]
        incoming.append(h)
        out_state = carry_own[c : c + 1, :] * h + carry_own[lanes2 + c : lanes2 + c + 1, :]
        out_states.append(out_state)

    @pl.when(jnp.logical_and(z > 0, z + 4 < spans))
    def _():
        for c in range(lanes2):
            state_own[c : c + 1, :] = jnp.zeros((1, LANES), F32)
            state_own[lanes2 + c : lanes2 + c + 1, :] = out_states[c]
        state_copy().start()

    def a2a_copy(other):
        return remote(gout.at[other], grecv.at[tp], a2a_send, a2a_recv.at[tp], {"tp": other})

    def ss_copy(other):
        return remote(ss_own.at[other], ss_recv.at[tp], ss_send, ss_recv_sem, {"tp": other})

    ones = jnp.ones((8, LANES), F32)

    def read_out(i, _):
        s = lax.rem(tp + 4 + i, peers)
        total = jnp.zeros((mine, LANES), F32)
        for c in range(lanes2):
            lane = slice(c * LANES, (c + 1) * LANES)
            enter = segp[c, pl.ds(s, 1), :] * incoming[c] + segh[c, pl.ds(s, 1), :]
            lines = pl.ds(s, mine, stride=SEGS)
            state = ht[c, lines, :] + pt[c, lines, :] * enter
            gated = state * ge[pl.ds(pl.multiple_of(s * mine, mine), mine), lane]
            total = total + gated * gated
            gout[s, :, lane] = (gated * ogain[:, lane]).astype(BF16)
        sums = lax.dot_general(
            ones, total, (((1,), (1,)), ((), ())), precision=lax.Precision.HIGHEST,
            preferred_element_type=F32,
        )
        ss_own[s] = sums[0:1, :]

        @pl.when(i != 4)
        def _():
            a2a_copy(s).start()
            ss_copy(s).start()

        return 0

    lax.fori_loop(0, 8, read_out, 0)
    grecv[tp] = gout[tp]
    ss_recv[tp] = ss_own[tp]

    pl.when(z == 0)(services)
    late(ring, 2)
    ring(1, 6)
    late(ring, 3)
    ring(1, 7)
    late(ring, 4)
    late(ring, 5)
    upper(ring, 8)
    late(ring, 6)
    upper(ring, 9)
    late(ring, 7)
    early(spread, 8)
    spread(1, 4)
    late(spread, 1)
    spread(1, 5)
    late(spread, 2)
    spread(1, 6)
    late(spread, 3)
    spread(1, 7)
    late(spread, 4)
    late(spread, 5)
    upper(spread, 8)
    late(spread, 6)
    upper(spread, 9)
    late(spread, 7)

    for pos in range(4, 8):
        wv_copies[pos].wait()
    for k in range(1, 8):
        other = lax.rem(tp + k, peers)
        remote(gout.at[other], grecv.at[other], a2a_send, a2a_recv.at[other], {"tp": other}).wait_recv()
    seven = ss_recv.at[pl.ds(0, 7)]
    local(seven, seven, ss_recv_sem).wait()
    everything = wv.at[:, pl.ds(0, 15 * share), :]
    local(everything, everything, ds_recv).wait()

    total = ss_recv[0]
    for k in range(1, 8):
        total = total + ss_recv[k]
    scales = lax.rsqrt(total * (1.0 / width) + 1e-06)
    scales = jnp.broadcast_to(scales, (LANES, mine)).T

    def finish(pos, _):
        acc = jnp.zeros((mine, channels), F32)
        for k in range(8):
            acc = acc + jnp.dot(
                grecv[k], wv[pos, k * channels : (k + 1) * channels, :], preferred_element_type=F32
            )
        for c in range(lanes2):
            lane = slice(c * LANES, (c + 1) * LANES)
            obuf[pos, :, lane] = (acc[:, lane] * scales).astype(BF16)
        return 0

    def out_copy(pos):
        return local(obuf.at[pos], out.at[:, pl.ds(column(pos), channels)], out_sem.at[pos])

    for way in (0, 1):
        count = from_below(above) if way == 0 else from_above(below)

        def sent(t, _):
            for side in (0, 1):
                z_copy(way, t + 1, side, z).wait_send()
            return 0

        lax.fori_loop(0, count, sent, 0)
    shared = wv.at[0:2, pl.ds(0, 15 * share), :]
    local(shared, shared, xs).wait()
    local(shared, shared, ys).wait()
    local(everything, everything, ds_send).wait()
    pl.when(z < last)(lambda: halo_copy().wait_send())
    for k in (1, 2, 3):
        pl.when(z + k < spans)(lambda: carry_copy(k).wait_send())
    pl.when(z + 4 < spans)(lambda: state_copy().wait_send())
    sent = gout.at[pl.ds(0, 7)]
    local(sent, sent, a2a_send).wait()
    sent = ss_own.at[pl.ds(0, 7)]
    local(sent, sent, ss_send).wait()
    for pos in range(0, 8, 2):
        finish(pos, 0)
        finish(pos + 1, 0)
        out_copy(pos).start()
        out_copy(pos + 1).start()
    for pos in range(8):
        out_copy(pos).wait()


def body(
    tokens, in_gain, w_input, w_gate, conv_taps, w_rate, w_inlet, decay_param, decay_bias, out_gain, w_out
):
    rows, width = tokens.shape
    channels = w_input.shape[1]
    lanes2 = channels // LANES
    spans, peers = lax.axis_size("sp"), lax.axis_size("tp")
    mine = rows // peers
    vmem = pltpu.VMEM
    dma = pltpu.SemaphoreType.DMA
    scratch = [
        vmem((rows, width), BF16),
        vmem((width, channels), BF16),
        vmem((width, channels), BF16),
        vmem((channels, 2 * channels), BF16),
        vmem((width // LANES, LANES), F32),
        vmem((4, channels), F32),
        vmem((1, channels), F32),
        vmem((rows // LANES, LANES), F32),
        vmem((1, channels), F32),
        vmem((8, width, channels), BF16),
        vmem((8 + rows, channels), F32),
        vmem((8, channels), F32),
        vmem((rows, LANES), F32),
        vmem((rows, LANES), F32),
        vmem((SEGS * STEP, channels), BF16),
        vmem((SEGS * STEP, 2 * channels), F32),
        vmem((lanes2, SEGS * PAD, LANES), F32),
        vmem((lanes2, SEGS * PAD, LANES), F32),
        vmem((lanes2, rows, LANES), F32),
        vmem((lanes2, rows, LANES), F32),
        vmem((rows, channels), F32),
        vmem((lanes2, SEGS, LANES), F32),
        vmem((lanes2, SEGS, LANES), F32),
        vmem((2 * lanes2, LANES), F32),
        vmem((2 * lanes2, LANES), F32),
        vmem((4, 2 * lanes2, LANES), F32),
        vmem((peers, mine, channels), BF16),
        vmem((peers, mine, channels), BF16),
        vmem((peers, 1, mine), F32),
        vmem((peers, 1, mine), F32),
        vmem((8, mine, channels), BF16),
        dma((4,)),
        dma((9,)),
        dma((8,)),
        dma((8,)),
        dma((2, 10, 2)),
        dma((2, 10, 2)),
        dma((2, 2, 10)),
        dma((2, 10)),
    ]
    scratch += [dma(())] * 6 + [dma((4,)), dma((4,)), dma(()), dma((8,)), dma(()), dma(())]
    scratch += [pltpu.SemaphoreType.REGULAR((3,))]
    spec = pl.BlockSpec(memory_space=pl.ANY)
    return pl.pallas_call(
        kernel,
        out_shape=jax.ShapeDtypeStruct((mine, width), BF16),
        in_specs=[spec] * 11,
        out_specs=spec,
        scratch_shapes=scratch,
        compiler_params=pltpu.CompilerParams(
            collective_id=0, has_side_effects=True, vmem_limit_bytes=60 * 1024 * 1024
        ),
        name="gated_recurrence",
    )(
        tokens,
        in_gain.reshape(width // LANES, LANES),
        w_input,
        w_gate,
        conv_taps,
        w_rate.reshape(channels, channels),
        w_inlet.reshape(channels, channels),
        decay_param.reshape(1, channels),
        decay_bias.reshape(rows // LANES, LANES),
        out_gain.reshape(1, channels),
        w_out,
    )


def solution(mesh):
    return jax.shard_map(
        body,
        mesh=mesh,
        in_specs=(
            P(("grp", "sp"), None),
            P(),
            P(None, "tp"),
            P(None, "tp"),
            P(None, "tp"),
            P("tp", None, None),
            P("tp", None, None),
            P("tp"),
            P("tp", ("grp", "sp")),
            P("tp"),
            P("sp", None),
        ),
        out_specs=P(("grp", "sp", "tp"), None),
        check_vma=False,
    )
```

```python
import functools

import jax
import jax.numpy as jnp
from jax import lax
from jax.experimental import pallas as pl
from jax.experimental.pallas import tpu as pltpu
from jax.sharding import PartitionSpec as P

MESH = pl.DeviceIdType.MESH
F32 = jnp.float32
BF16 = jnp.bfloat16
LANES = 128
SEGS = 8
STEP = 32
PAD = 40


def log1p_small(u):
    series = u * (1.0 - u * (0.5 - u * (1.0 / 3.0 - u * (0.25 - u * (0.2 - u / 6.0)))))
    return jnp.where(u < 0.06, series, jnp.log(1.0 + u))


def softplus(x):
    return jnp.maximum(x, 0.0) + log1p_small(jnp.exp(-jnp.abs(x)))


def gelu(x):
    inner = 0.7978845608028654 * (x + 0.044715 * (x * x * x))
    return 0.5 * x * (1.0 + jnp.tanh(inner))


def kernel(
    tokens_in,
    gain_in,
    w_input_in,
    w_gate_in,
    taps_in,
    w_rate_in,
    w_inlet_in,
    dparam_in,
    bias_in,
    ogain_in,
    w_out_in,
    out,
    tok,
    wi,
    wg,
    wrn,
    gain,
    taps,
    dparam,
    bias,
    ogain,
    wv,
    proj,
    halo,
    biasc,
    invc,
    conv,
    gates,
    sa,
    sb,
    ht,
    pt,
    ge,
    segh,
    segp,
    carry_own,
    state_own,
    carry,
    gout,
    grecv,
    ss_own,
    ss_recv,
    obuf,
    tok_sem,
    in_sem,
    wv_sem,
    out_sem,
    zs,
    zr,
    xr,
    yr,
    xs,
    ys,
    ds_send,
    ds_recv,
    halo_send,
    halo_recv,
    carry_send,
    carry_recv,
    a2a_send,
    a2a_recv,
    ss_send,
    ss_recv_sem,
    know,
):
    grp, z, tp = lax.axis_index("grp"), lax.axis_index("sp"), lax.axis_index("tp")
    spans, peers = lax.axis_size("sp"), lax.axis_size("tp")
    core = lax.rem(tp, 2)
    rows, width = tok.shape
    channels = wi.shape[1]
    lanes2 = channels // LANES
    block = width // spans
    tile = rows // 4
    mine = rows // peers
    first = lax.rem(2 * (tp // 2) + 4 * lax.rem(grp, 2), 8)
    partner = grp + 1 - 2 * lax.rem(grp, 2)
    sibling = tp + 1 - 2 * core

    def column(pos):
        return pl.multiple_of(lax.rem(first + pos, 8) * channels, channels)

    def local(src, dst, sem):
        return pltpu.make_async_copy(src, dst, sem)

    def remote(src, dst, send, recv, where):
        return pltpu.make_async_remote_copy(
            src_ref=src, dst_ref=dst, send_sem=send, recv_sem=recv, device_id=where, device_id_type=MESH
        )

    own_lines = pl.ds(pl.multiple_of(z * block, block), block)
    wv_copies = [
        local(w_out_in.at[:, pl.ds(column(pos), channels)], wv.at[pos, own_lines, :], wv_sem.at[pos])
        for pos in range(8)
    ]
    for pos in range(4):
        wv_copies[pos].start()
    in_copies = [
        local(gain_in, gain, in_sem.at[0]),
        local(w_input_in, wi, in_sem.at[1]),
        local(bias_in, bias, in_sem.at[2]),
        local(taps_in, taps, in_sem.at[3]),
        local(dparam_in, dparam, in_sem.at[4]),
        local(ogain_in, ogain, in_sem.at[5]),
        local(w_rate_in, wrn.at[:, 0:channels], in_sem.at[6]),
        local(w_inlet_in, wrn.at[:, channels : 2 * channels], in_sem.at[7]),
        local(w_gate_in, wg, in_sem.at[8]),
    ]
    for k in (0, 1, 2):
        in_copies[k].start()

    def tok_copy(k):
        part = pl.ds(pl.multiple_of(k * tile, tile), tile)
        return local(tokens_in.at[part, :], tok.at[part, :], tok_sem.at[k])

    for k in (3, 2, 1, 0):
        tok_copy(k).start()
    for k in range(3, 9):
        in_copies[k].start()
    for pos in range(4, 8):
        wv_copies[pos].start()

    last = spans - 1
    barrier = pltpu.get_barrier_semaphore()
    above, below = lax.rem(z + 1, spans), lax.rem(z + last, spans)
    for where in (
        [{"sp": above}, {"sp": below}, {"grp": partner}]
        + [{"tp": lax.rem(tp + k, peers)} for k in range(1, 8)]
    ):
        pl.semaphore_signal(barrier, inc=1, device_id=where, device_id_type=MESH)

    def learn(level):
        pl.when(z < last)(lambda: pl.semaphore_wait(know.at[level], 1))

    def teach(level):
        @pl.when(z > 0)
        def _():
            pl.semaphore_signal(know.at[level], inc=1, device_id={"sp": below}, device_id_type=MESH)

    low = jnp.minimum(below, 2)
    count = (1 - core) * (low + 6) + core * (9 - low)
    onward = lax.rem(z + 1 + core * (spans - 2), spans)
    low = jnp.minimum(lax.rem(onward + last, spans), 2)
    count_out = (1 - core) * (low + 6) + core * (9 - low)
    count_other = spans - 1 - count

    def owner_of(way, t):
        return lax.rem(z + (1 - way) * (spans - t) + way * t, spans)

    def lines_of(owner):
        return pl.ds(pl.multiple_of(owner * block, block), block)

    def z_copy(t, pos, owner):
        part = wv.at[pos, lines_of(owner), :]
        return remote(part, part, zs.at[t, pos], zr.at[t, pos], {"sp": onward})

    def share_copy(k, t):
        lines = lines_of(owner_of(core, t))
        if k < 2:
            where = {"tp": lax.rem(tp + 2 + 4 * k, peers)}
            return remote(
                wv.at[1 + k, lines, :], wv.at[7 - 3 * k, lines, :], xs.at[k, t], xr.at[k, t], where
            )
        return remote(
            wv.at[1:3, lines, :], wv.at[5:7, lines, :], ys.at[t], yr.at[t], {"grp": partner}
        )

    def d_copy(level, way, t):
        part = wv.at[4 * level : 4 * level + 4, lines_of(owner_of(way, t)), :]
        return remote(part, part, ds_send.at[level, t], ds_recv.at[level, t], {"tp": sibling})

    def ring(t, _):
        owner = owner_of(core, t)
        for pos in (1, 2, 0, 3):
            z_copy(t, pos, owner).wait_recv()

            @pl.when(t < count_out)
            def _():
                z_copy(t + 1, pos, owner).start()

        for k in range(3):
            share_copy(k, t).start()
        d_copy(0, core, t).start()
        return 0

    def spread(t, _):
        for k in range(3):
            share_copy(k, t).wait_recv()
        d_copy(1, core, t).start()
        return 0

    def goal(up, down, at_first):
        up = jnp.minimum(up, jnp.maximum(below - 1, 0))
        up = jnp.where(z > 0, up, at_first)
        return (1 - core) * up + core * down

    def first_sends():
        for pos in (1, 2, 0, 3):
            z_copy(1, pos, z).start()

    in_copies[0].wait()
    in_copies[1].wait()
    in_copies[2].wait()
    gain_cols = gain[...].T
    bias_cols = bias[...].T
    for j in range(width // LANES):
        part = pl.ds(j * LANES, LANES)
        wi[part, :] = (wi[part, :].astype(F32) * gain_cols[:, j : j + 1]).astype(BF16)
        biasc[part, :] = jnp.broadcast_to(bias_cols[:, j : j + 1], (LANES, LANES))

    def halo_copy():
        return remote(proj.at[pl.ds(rows, 8), :], halo, halo_send, halo_recv, {"sp": above})

    def project(i, _):
        k = 3 - i
        base = pl.multiple_of(k * tile, tile)
        tok_copy(k).wait()

        part = pl.ds(base, tile)
        acc = jnp.dot(tok[part, :], wi[...], preferred_element_type=F32)
        for j in range(tile // 64):
            lines = pl.ds(pl.multiple_of(base + j * 64, 64), 64)
            total = jnp.zeros((64, LANES), F32)
            for c in range(width // LANES):
                x = tok[lines, c * LANES : (c + 1) * LANES].astype(F32)
                total = total + x * x
            mean = jnp.sum(total, axis=1, keepdims=True) * (1.0 / width)
            inv = jnp.broadcast_to(lax.rsqrt(mean + 1e-06), (64, LANES))
            invc[lines, :] = inv
            for c in range(lanes2):
                lane = slice(c * LANES, (c + 1) * LANES)
                scaled = acc[j * 64 : (j + 1) * 64, lane] * inv
                proj[pl.ds(base + 8 + j * 64, 64), lane] = scaled.astype(BF16).astype(F32)

        return 0

    lax.fori_loop(0, 1, project, 0)
    pl.semaphore_wait(barrier, 10)
    pl.when(z < last)(lambda: halo_copy().start())
    teach(0)
    for pos in range(4):
        wv_copies[pos].wait()
    first_sends()
    lax.fori_loop(1, 3, project, 0)
    r0 = goal(1, 0, 0)
    lax.fori_loop(1, r0 + 1, ring, 0)
    lax.fori_loop(3, 4, project, 0)
    learn(0)
    teach(1)
    r1 = goal(2, 0, 0)
    lax.fori_loop(r0 + 1, r1 + 1, ring, 0)

    for k in range(3, 8):
        in_copies[k].wait()
    pl.when(z > 0)(lambda: halo_copy().wait_recv())

    @pl.when(z > 0)
    def _():
        proj[0:8, :] = halo[...]

    @pl.when(z == 0)
    def _():
        proj[0:8, :] = jnp.zeros((8, channels), F32)

    scale = -8.0 * softplus(-dparam[...])
    tap = [taps[k : k + 1, :] for k in range(4)]

    def gather_inputs(i):
        for s in range(SEGS):
            base = pl.multiple_of(s * mine + i * STEP, STEP)
            x = proj[pl.ds(base, STEP + 8), :]
            total = pltpu.roll(x, 3, axis=0)[8:] * tap[0]
            total = total + pltpu.roll(x, 2, axis=0)[8:] * tap[1]
            total = total + pltpu.roll(x, 1, axis=0)[8:] * tap[2]
            total = total + x[8:] * tap[3]
            conv[s * STEP : (s + 1) * STEP, :] = total.astype(BF16)

    def scan_tile(i, state):
        gather_inputs(i)
        gates[...] = jnp.dot(conv[...], wrn[...], preferred_element_type=F32)
        for s in range(SEGS):
            base = pl.multiple_of(s * mine + i * STEP, STEP)
            shift = biasc[pl.ds(base, STEP), :]
            part = slice(s * STEP, (s + 1) * STEP)
            for c in range(channels // LANES):
                lane = slice(c * LANES, (c + 1) * LANES)
                rate = jax.nn.sigmoid(gates[part, lane])
                inlet = jax.nn.sigmoid(gates[part, channels + c * LANES : channels + (c + 1) * LANES])
                log_decay = rate * scale[:, lane] + shift
                decay = jnp.exp(log_decay)
                y = -2.0 * log_decay
                series = y * (
                    1.0 - y * (0.5 - y * (1.0 / 6.0 - y * (1.0 / 24.0 - y * (1.0 / 120.0))))
                )
                grown = jnp.where(y < 0.2, series, 1.0 - decay * decay)
                root = grown * lax.rsqrt(jnp.maximum(grown, 1e-37))
                drive = root * inlet * conv[part, lane].astype(F32)
                sa[c, s * PAD : s * PAD + STEP, :] = decay
                sb[c, s * PAD : s * PAD + STEP, :] = drive
        state = list(state)
        for r in range(STEP):
            line = pl.ds(pl.multiple_of((i * STEP + r) * SEGS, SEGS), SEGS)
            for c in range(channels // LANES):
                a = sa[c, pl.ds(r, SEGS, stride=PAD), :]
                b = sb[c, pl.ds(r, SEGS, stride=PAD), :]
                h, p = state[2 * c], state[2 * c + 1]
                h, p = a * h + b, a * p
                ht[c, line, :] = h
                pt[c, line, :] = p
                state[2 * c], state[2 * c + 1] = h, p
        return tuple(state)

    state = (jnp.zeros((SEGS, LANES), F32), jnp.ones((SEGS, LANES), F32)) * lanes2
    state = lax.fori_loop(0, 3, scan_tile, state)
    learn(1)
    teach(2)
    r2 = goal(3, 1, 0)
    lax.fori_loop(r1 + 1, r2 + 1, ring, 0)
    state = lax.fori_loop(3, 6, scan_tile, state)
    r3 = goal(4, 1, 0)
    lax.fori_loop(r2 + 1, r3 + 1, ring, 0)
    state = lax.fori_loop(6, 8, scan_tile, state)

    for c in range(lanes2):
        h_end, p_end = state[2 * c], state[2 * c + 1]
        h, p = jnp.zeros((1, LANES), F32), jnp.ones((1, LANES), F32)
        for s in range(SEGS):
            segh[c, s : s + 1, :] = h
            segp[c, s : s + 1, :] = p
            h = p_end[s : s + 1] * h + h_end[s : s + 1]
            p = p_end[s : s + 1] * p
        carry_own[c : c + 1, :] = p
        carry_own[lanes2 + c : lanes2 + c + 1, :] = h

    learn(2)

    def carry_copy(k):
        return remote(
            carry_own, carry.at[k - 1], carry_send.at[k - 1], carry_recv.at[k - 1],
            {"sp": lax.rem(z + k, spans)},
        )

    for k in (1, 2, 3):
        pl.when(z + k < spans)(lambda: carry_copy(k).start())

    def state_copy():
        return remote(
            state_own, carry.at[3], carry_send.at[3], carry_recv.at[3], {"sp": lax.rem(z + 4, spans)}
        )

    @pl.when(z == 0)
    def _():
        state_own[...] = carry_own[...]
        state_copy().start()

    r4 = goal(5, 2, 1)
    lax.fori_loop(r3 + 1, r4 + 1, ring, 0)
    s0 = goal(2, 0, 0)
    lax.fori_loop(1, s0 + 1, spread, 0)

    in_copies[8].wait()
    for j in range(width // LANES):
        part = pl.ds(j * LANES, LANES)
        wg[part, :] = (wg[part, :].astype(F32) * gain_cols[:, j : j + 1]).astype(BF16)

    def gate(i, _):
        part = pl.ds(pl.multiple_of(i * tile, tile), tile)
        acc = jnp.dot(tok[part, :], wg[...], preferred_element_type=F32)
        inv = invc[part, :]
        for c in range(lanes2):
            lane = slice(c * LANES, (c + 1) * LANES)
            ge[part, lane] = gelu((acc[:, lane] * inv).astype(BF16).astype(F32))
        return 0

    lax.fori_loop(0, 2, gate, 0)
    r5 = goal(6, 2, 1)
    lax.fori_loop(r4 + 1, r5 + 1, ring, 0)
    lax.fori_loop(2, 4, gate, 0)
    r6 = goal(7, 3, 3)
    lax.fori_loop(r5 + 1, r6 + 1, ring, 0)
    s1 = goal(4, 1, 0)
    lax.fori_loop(s0 + 1, s1 + 1, spread, 0)

    r7 = jnp.where(z > 0, (1 - core) * jnp.minimum(z, 8) + core * 6, r6)
    lax.fori_loop(r6 + 1, r7 + 1, ring, 0)
    s2 = jnp.where(z > 0, goal(7, 4, 0), s1)
    lax.fori_loop(s1 + 1, s2 + 1, spread, 0)

    def received(copy, slot, k):
        pl.when(z >= k)(lambda: copy.wait_recv())

        @pl.when(z < k)
        def _():
            carry[slot] = jnp.zeros(carry.shape[1:], F32)

    received(state_copy(), 3, 4)
    for k in (1, 2, 3):
        received(carry_copy(k), k - 1, k)
    incoming, out_states = [], []
    for c in range(lanes2):
        h = carry[3, lanes2 + c : lanes2 + c + 1, :]
        for k in (3, 2, 1):
            h = carry[k - 1, c : c + 1, :] * h + carry[k - 1, lanes2 + c : lanes2 + c + 1, :]
        incoming.append(h)
        out_state = carry_own[c : c + 1, :] * h + carry_own[lanes2 + c : lanes2 + c + 1, :]
        out_states.append(out_state)

    @pl.when(jnp.logical_and(z > 0, z + 4 < spans))
    def _():
        for c in range(lanes2):
            state_own[c : c + 1, :] = jnp.zeros((1, LANES), F32)
            state_own[lanes2 + c : lanes2 + c + 1, :] = out_states[c]
        state_copy().start()

    def a2a_copy(other):
        return remote(gout.at[other], grecv.at[tp], a2a_send, a2a_recv.at[tp], {"tp": other})

    def ss_copy(other):
        return remote(ss_own.at[other], ss_recv.at[tp], ss_send, ss_recv_sem, {"tp": other})

    ones = jnp.ones((8, LANES), F32)

    def read_out(i, _):
        s = lax.rem(tp + 4 + i, peers)
        total = jnp.zeros((mine, LANES), F32)
        for c in range(lanes2):
            lane = slice(c * LANES, (c + 1) * LANES)
            enter = segp[c, pl.ds(s, 1), :] * incoming[c] + segh[c, pl.ds(s, 1), :]
            lines = pl.ds(s, mine, stride=SEGS)
            state = ht[c, lines, :] + pt[c, lines, :] * enter
            gated = state * ge[pl.ds(pl.multiple_of(s * mine, mine), mine), lane]
            total = total + gated * gated
            gout[s, :, lane] = (gated * ogain[:, lane]).astype(BF16)
        sums = lax.dot_general(
            ones, total, (((1,), (1,)), ((), ())), precision=lax.Precision.HIGHEST,
            preferred_element_type=F32,
        )
        ss_own[s] = sums[0:1, :]

        @pl.when(i != 4)
        def _():
            a2a_copy(s).start()
            ss_copy(s).start()

        return 0

    lax.fori_loop(0, 8, read_out, 0)
    grecv[tp] = gout[tp]
    ss_recv[tp] = ss_own[tp]

    lax.fori_loop(r7 + 1, count + 1, ring, 0)
    lax.fori_loop(s2 + 1, count + 1, spread, 0)

    for pos in range(4, 8):
        wv_copies[pos].wait()
    for k in range(1, 8):
        other = lax.rem(tp + k, peers)
        remote(gout.at[other], grecv.at[other], a2a_send, a2a_recv.at[other], {"tp": other}).wait_recv()
    seven = ss_recv.at[pl.ds(0, 7)]
    local(seven, seven, ss_recv_sem).wait()

    def other_half(t, _):
        d_copy(0, 1 - core, t).wait_recv()
        d_copy(1, 1 - core, t).wait_recv()
        return 0

    lax.fori_loop(1, count_other + 1, other_half, 0)

    total = ss_recv[0]
    for k in range(1, 8):
        total = total + ss_recv[k]
    scales = lax.rsqrt(total * (1.0 / width) + 1e-06)
    scales = jnp.broadcast_to(scales, (LANES, mine)).T

    def finish(pos, _):
        acc = jnp.zeros((mine, channels), F32)
        for k in range(8):
            acc = acc + jnp.dot(
                grecv[k], wv[pos, k * channels : (k + 1) * channels, :], preferred_element_type=F32
            )
        for c in range(lanes2):
            lane = slice(c * LANES, (c + 1) * LANES)
            obuf[pos, :, lane] = (acc[:, lane] * scales).astype(BF16)
        return 0

    def out_copy(pos):
        return local(obuf.at[pos], out.at[:, pl.ds(column(pos), channels)], out_sem.at[pos])

    def passed(t, _):
        for pos in range(4):
            z_copy(t, pos, z).wait_send()
        return 0

    def shared(t, _):
        for k in range(3):
            share_copy(k, t).wait_send()
        d_copy(0, core, t).wait_send()
        d_copy(1, core, t).wait_send()
        return 0

    lax.fori_loop(1, count_out + 1, passed, 0)
    lax.fori_loop(1, count + 1, shared, 0)
    pl.when(z < last)(lambda: halo_copy().wait_send())
    for k in (1, 2, 3):
        pl.when(z + k < spans)(lambda: carry_copy(k).wait_send())
    pl.when(z + 4 < spans)(lambda: state_copy().wait_send())
    sent = gout.at[pl.ds(0, 7)]
    local(sent, sent, a2a_send).wait()
    sent = ss_own.at[pl.ds(0, 7)]
    local(sent, sent, ss_send).wait()
    for pos in range(0, 8, 2):
        finish(pos, 0)
        finish(pos + 1, 0)
        out_copy(pos).start()
        out_copy(pos + 1).start()
    for pos in range(8):
        out_copy(pos).wait()


def body(
    tokens, in_gain, w_input, w_gate, conv_taps, w_rate, w_inlet, decay_param, decay_bias, out_gain, w_out
):
    rows, width = tokens.shape
    channels = w_input.shape[1]
    lanes2 = channels // LANES
    spans, peers = lax.axis_size("sp"), lax.axis_size("tp")
    mine = rows // peers
    vmem = pltpu.VMEM
    dma = pltpu.SemaphoreType.DMA
    scratch = [
        vmem((rows, width), BF16),
        vmem((width, channels), BF16),
        vmem((width, channels), BF16),
        vmem((channels, 2 * channels), BF16),
        vmem((width // LANES, LANES), F32),
        vmem((4, channels), F32),
        vmem((1, channels), F32),
        vmem((rows // LANES, LANES), F32),
        vmem((1, channels), F32),
        vmem((8, width, channels), BF16),
        vmem((8 + rows, channels), F32),
        vmem((8, channels), F32),
        vmem((rows, LANES), F32),
        vmem((rows, LANES), F32),
        vmem((SEGS * STEP, channels), BF16),
        vmem((SEGS * STEP, 2 * channels), F32),
        vmem((lanes2, SEGS * PAD, LANES), F32),
        vmem((lanes2, SEGS * PAD, LANES), F32),
        vmem((lanes2, rows, LANES), F32),
        vmem((lanes2, rows, LANES), F32),
        vmem((rows, channels), F32),
        vmem((lanes2, SEGS, LANES), F32),
        vmem((lanes2, SEGS, LANES), F32),
        vmem((2 * lanes2, LANES), F32),
        vmem((2 * lanes2, LANES), F32),
        vmem((4, 2 * lanes2, LANES), F32),
        vmem((peers, mine, channels), BF16),
        vmem((peers, mine, channels), BF16),
        vmem((peers, 1, mine), F32),
        vmem((peers, 1, mine), F32),
        vmem((8, mine, channels), BF16),
        dma((4,)),
        dma((9,)),
        dma((8,)),
        dma((8,)),
        dma((10, 4)),
        dma((10, 4)),
        dma((2, 10)),
        dma((10,)),
        dma((2, 10)),
        dma((10,)),
        dma((2, 10)),
        dma((2, 10)),
        dma(()),
        dma(()),
        dma((4,)),
        dma((4,)),
        dma(()),
        dma((8,)),
        dma(()),
        dma(()),
    ]
    scratch += [pltpu.SemaphoreType.REGULAR((3,))]
    spec = pl.BlockSpec(memory_space=pl.ANY)
    return pl.pallas_call(
        kernel,
        out_shape=jax.ShapeDtypeStruct((mine, width), BF16),
        in_specs=[spec] * 11,
        out_specs=spec,
        scratch_shapes=scratch,
        compiler_params=pltpu.CompilerParams(
            collective_id=0, has_side_effects=True, vmem_limit_bytes=60 * 1024 * 1024
        ),
        name="gated_recurrence",
    )(
        tokens,
        in_gain.reshape(width // LANES, LANES),
        w_input,
        w_gate,
        conv_taps,
        w_rate.reshape(channels, channels),
        w_inlet.reshape(channels, channels),
        decay_param.reshape(1, channels),
        decay_bias.reshape(rows // LANES, LANES),
        out_gain.reshape(1, channels),
        w_out,
    )


def solution(mesh):
    return jax.shard_map(
        body,
        mesh=mesh,
        in_specs=(
            P(("grp", "sp"), None),
            P(),
            P(None, "tp"),
            P(None, "tp"),
            P(None, "tp"),
            P("tp", None, None),
            P("tp", None, None),
            P("tp"),
            P("tp", ("grp", "sp")),
            P("tp"),
            P("sp", None),
        ),
        out_specs=P(("grp", "sp", "tp"), None),
        check_vma=False,
    )
```

```python
import functools

import jax
import jax.numpy as jnp
from jax import lax
from jax.experimental import pallas as pl
from jax.experimental.pallas import tpu as pltpu
from jax.sharding import PartitionSpec as P

MESH = pl.DeviceIdType.MESH
F32 = jnp.float32
BF16 = jnp.bfloat16
LANES = 128
SEGS = 8
STEP = 32
PAD = 40


def log1p_small(u):
    series = u * (1.0 - u * (0.5 - u * (1.0 / 3.0 - u * (0.25 - u * (0.2 - u / 6.0)))))
    return jnp.where(u < 0.06, series, jnp.log(1.0 + u))


def softplus(x):
    return jnp.maximum(x, 0.0) + log1p_small(jnp.exp(-jnp.abs(x)))


def gelu(x):
    inner = 0.7978845608028654 * (x + 0.044715 * (x * x * x))
    return 0.5 * x * (1.0 + jnp.tanh(inner))


def kernel(
    tokens_in,
    gain_in,
    w_input_in,
    w_gate_in,
    taps_in,
    w_rate_in,
    w_inlet_in,
    dparam_in,
    bias_in,
    ogain_in,
    w_out_in,
    out,
    tok,
    wi,
    wg,
    wrn,
    gain,
    taps,
    dparam,
    bias,
    ogain,
    wv,
    proj,
    halo,
    biasc,
    invc,
    conv,
    gates,
    sa,
    sb,
    ht,
    pt,
    ge,
    segh,
    segp,
    carry_own,
    state_own,
    carry,
    gout,
    grecv,
    ss_own,
    ss_recv,
    obuf,
    tok_sem,
    in_sem,
    wv_sem,
    out_sem,
    zs,
    zr,
    xr,
    yr,
    xs,
    ys,
    ds_send,
    ds_recv,
    halo_send,
    halo_recv,
    carry_send,
    carry_recv,
    a2a_send,
    a2a_recv,
    ss_send,
    ss_recv_sem,
    know,
):
    grp, z, tp = lax.axis_index("grp"), lax.axis_index("sp"), lax.axis_index("tp")
    spans, peers = lax.axis_size("sp"), lax.axis_size("tp")
    core = lax.rem(tp, 2)
    rows, width = tok.shape
    channels = wi.shape[1]
    lanes2 = channels // LANES
    block = width // spans
    tile = rows // 4
    mine = rows // peers
    first = lax.rem(2 * (tp // 2) + 4 * lax.rem(grp, 2), 8)
    partner = grp + 1 - 2 * lax.rem(grp, 2)
    sibling = tp + 1 - 2 * core

    def column(pos):
        return pl.multiple_of(lax.rem(first + pos, 8) * channels, channels)

    def local(src, dst, sem):
        return pltpu.make_async_copy(src, dst, sem)

    def remote(src, dst, send, recv, where):
        return pltpu.make_async_remote_copy(
            src_ref=src, dst_ref=dst, send_sem=send, recv_sem=recv, device_id=where, device_id_type=MESH
        )

    own_lines = pl.ds(pl.multiple_of(z * block, block), block)
    wv_copies = [
        local(w_out_in.at[:, pl.ds(column(pos), channels)], wv.at[pos, own_lines, :], wv_sem.at[pos])
        for pos in range(8)
    ]
    for pos in range(4):
        wv_copies[pos].start()
    in_copies = [
        local(gain_in, gain, in_sem.at[0]),
        local(w_input_in, wi, in_sem.at[1]),
        local(bias_in, bias, in_sem.at[2]),
        local(taps_in, taps, in_sem.at[3]),
        local(dparam_in, dparam, in_sem.at[4]),
        local(ogain_in, ogain, in_sem.at[5]),
        local(w_rate_in, wrn.at[:, 0:channels], in_sem.at[6]),
        local(w_inlet_in, wrn.at[:, channels : 2 * channels], in_sem.at[7]),
        local(w_gate_in, wg, in_sem.at[8]),
    ]
    for k in (0, 1, 2):
        in_copies[k].start()

    def tok_copy(k):
        part = pl.ds(pl.multiple_of(k * tile, tile), tile)
        return local(tokens_in.at[part, :], tok.at[part, :], tok_sem.at[k])

    for k in (3, 2, 1, 0):
        tok_copy(k).start()
    for k in range(3, 9):
        in_copies[k].start()
    for pos in range(4, 8):
        wv_copies[pos].start()

    last = spans - 1
    barrier = pltpu.get_barrier_semaphore()
    above, below = lax.rem(z + 1, spans), lax.rem(z + last, spans)
    for where in (
        [{"sp": above}, {"sp": below}, {"grp": partner}]
        + [{"tp": lax.rem(tp + k, peers)} for k in range(1, 8)]
    ):
        pl.semaphore_signal(barrier, inc=1, device_id=where, device_id_type=MESH)

    def learn(level):
        pl.when(z < last)(lambda: pl.semaphore_wait(know.at[level], 1))

    def teach(level):
        @pl.when(z > 0)
        def _():
            pl.semaphore_signal(know.at[level], inc=1, device_id={"sp": below}, device_id_type=MESH)

    def blocks_at(span):
        low = jnp.minimum(lax.rem(span + last, spans), 3) + 5 - jnp.where(span > 0, 0, 1)
        return (1 - core) * low + core * (spans - 1 - low)

    count = blocks_at(z)
    onward = lax.rem(z + 1 + core * (spans - 2), spans)
    count_out = blocks_at(onward)
    count_other = spans - 1 - count

    def owner_of(way, t):
        return lax.rem(z + (1 - way) * (spans - t) + way * t, spans)

    def lines_of(owner):
        return pl.ds(pl.multiple_of(owner * block, block), block)

    def z_copy(t, pos, owner):
        part = wv.at[pos, lines_of(owner), :]
        return remote(part, part, zs.at[t, pos], zr.at[t, pos], {"sp": onward})

    def share_copy(k, t):
        lines = lines_of(owner_of(core, t))
        if k < 2:
            where = {"tp": lax.rem(tp + 2 + 4 * k, peers)}
            return remote(
                wv.at[1 + k, lines, :], wv.at[7 - 3 * k, lines, :], xs.at[k, t], xr.at[k, t], where
            )
        return remote(
            wv.at[1:3, lines, :], wv.at[5:7, lines, :], ys.at[t], yr.at[t], {"grp": partner}
        )

    def d_copy(level, way, t):
        part = wv.at[4 * level : 4 * level + 4, lines_of(owner_of(way, t)), :]
        return remote(part, part, ds_send.at[level, t], ds_recv.at[level, t], {"tp": sibling})

    def ring(t, _):
        owner = owner_of(core, t)
        for pos in (1, 2, 0, 3):
            z_copy(t, pos, owner).wait_recv()

            @pl.when(t < count_out)
            def _():
                z_copy(t + 1, pos, owner).start()

        for k in range(3):
            share_copy(k, t).start()
        d_copy(0, core, t).start()
        return 0

    def spread(t, _):
        for k in range(3):
            share_copy(k, t).wait_recv()
        d_copy(1, core, t).start()
        return 0

    def goal(up, down, first_up, first_down):
        up = jnp.where(z > 0, jnp.minimum(up, jnp.maximum(z - 2, 0)), first_up)
        return (1 - core) * up + core * jnp.where(z > 0, down, first_down)

    def first_sends():
        for pos in (1, 2, 0, 3):
            z_copy(1, pos, z).start()

    in_copies[0].wait()
    in_copies[1].wait()
    in_copies[2].wait()
    gain_cols = gain[...].T
    bias_cols = bias[...].T
    for j in range(width // LANES):
        part = pl.ds(j * LANES, LANES)
        wi[part, :] = (wi[part, :].astype(F32) * gain_cols[:, j : j + 1]).astype(BF16)
        biasc[part, :] = jnp.broadcast_to(bias_cols[:, j : j + 1], (LANES, LANES))

    def halo_copy():
        return remote(proj.at[pl.ds(rows, 8), :], halo, halo_send, halo_recv, {"sp": above})

    def project(i, _):
        k = 3 - i
        base = pl.multiple_of(k * tile, tile)
        tok_copy(k).wait()

        part = pl.ds(base, tile)
        acc = jnp.dot(tok[part, :], wi[...], preferred_element_type=F32)
        for j in range(tile // 64):
            lines = pl.ds(pl.multiple_of(base + j * 64, 64), 64)
            total = jnp.zeros((64, LANES), F32)
            for c in range(width // LANES):
                x = tok[lines, c * LANES : (c + 1) * LANES].astype(F32)
                total = total + x * x
            mean = jnp.sum(total, axis=1, keepdims=True) * (1.0 / width)
            inv = jnp.broadcast_to(lax.rsqrt(mean + 1e-06), (64, LANES))
            invc[lines, :] = inv
            for c in range(lanes2):
                lane = slice(c * LANES, (c + 1) * LANES)
                scaled = acc[j * 64 : (j + 1) * 64, lane] * inv
                proj[pl.ds(base + 8 + j * 64, 64), lane] = scaled.astype(BF16).astype(F32)

        return 0

    lax.fori_loop(0, 1, project, 0)
    pl.semaphore_wait(barrier, 10)
    pl.when(z < last)(lambda: halo_copy().start())
    teach(0)
    for pos in range(4):
        wv_copies[pos].wait()
    first_sends()
    lax.fori_loop(1, 4, project, 0)
    learn(0)
    teach(1)

    for k in range(3, 8):
        in_copies[k].wait()
    pl.when(z > 0)(lambda: halo_copy().wait_recv())

    @pl.when(z > 0)
    def _():
        proj[0:8, :] = halo[...]

    @pl.when(z == 0)
    def _():
        proj[0:8, :] = jnp.zeros((8, channels), F32)

    scale = -8.0 * softplus(-dparam[...])
    tap = [taps[k : k + 1, :] for k in range(4)]

    def gather_inputs(i):
        for s in range(SEGS):
            base = pl.multiple_of(s * mine + i * STEP, STEP)
            x = proj[pl.ds(base, STEP + 8), :]
            total = pltpu.roll(x, 3, axis=0)[8:] * tap[0]
            total = total + pltpu.roll(x, 2, axis=0)[8:] * tap[1]
            total = total + pltpu.roll(x, 1, axis=0)[8:] * tap[2]
            total = total + x[8:] * tap[3]
            conv[s * STEP : (s + 1) * STEP, :] = total.astype(BF16)

    def scan_tile(i, state):
        gather_inputs(i)
        gates[...] = jnp.dot(conv[...], wrn[...], preferred_element_type=F32)
        for s in range(SEGS):
            base = pl.multiple_of(s * mine + i * STEP, STEP)
            shift = biasc[pl.ds(base, STEP), :]
            part = slice(s * STEP, (s + 1) * STEP)
            for c in range(channels // LANES):
                lane = slice(c * LANES, (c + 1) * LANES)
                rate = jax.nn.sigmoid(gates[part, lane])
                inlet = jax.nn.sigmoid(gates[part, channels + c * LANES : channels + (c + 1) * LANES])
                log_decay = rate * scale[:, lane] + shift
                decay = jnp.exp(log_decay)
                y = -2.0 * log_decay
                series = y * (
                    1.0 - y * (0.5 - y * (1.0 / 6.0 - y * (1.0 / 24.0 - y * (1.0 / 120.0))))
                )
                grown = jnp.where(y < 0.2, series, 1.0 - decay * decay)
                root = grown * lax.rsqrt(jnp.maximum(grown, 1e-37))
                drive = root * inlet * conv[part, lane].astype(F32)
                sa[c, s * PAD : s * PAD + STEP, :] = decay
                sb[c, s * PAD : s * PAD + STEP, :] = drive
        state = list(state)
        for r in range(STEP):
            line = pl.ds(pl.multiple_of((i * STEP + r) * SEGS, SEGS), SEGS)
            for c in range(channels // LANES):
                a = sa[c, pl.ds(r, SEGS, stride=PAD), :]
                b = sb[c, pl.ds(r, SEGS, stride=PAD), :]
                h, p = state[2 * c], state[2 * c + 1]
                h, p = a * h + b, a * p
                ht[c, line, :] = h
                pt[c, line, :] = p
                state[2 * c], state[2 * c + 1] = h, p
        return tuple(state)

    state = (jnp.zeros((SEGS, LANES), F32), jnp.ones((SEGS, LANES), F32)) * lanes2
    state = lax.fori_loop(0, 3, scan_tile, state)
    learn(1)
    teach(2)
    r0 = goal(1, 0, 0, 0)
    lax.fori_loop(1, r0 + 1, ring, 0)
    state = lax.fori_loop(3, 6, scan_tile, state)
    r1 = goal(1, 1, 0, 1)
    lax.fori_loop(r0 + 1, r1 + 1, ring, 0)
    state = lax.fori_loop(6, 8, scan_tile, state)

    for c in range(lanes2):
        h_end, p_end = state[2 * c], state[2 * c + 1]
        h, p = jnp.zeros((1, LANES), F32), jnp.ones((1, LANES), F32)
        for s in range(SEGS):
            segh[c, s : s + 1, :] = h
            segp[c, s : s + 1, :] = p
            h = p_end[s : s + 1] * h + h_end[s : s + 1]
            p = p_end[s : s + 1] * p
        carry_own[c : c + 1, :] = p
        carry_own[lanes2 + c : lanes2 + c + 1, :] = h

    learn(2)

    def carry_copy(k):
        return remote(
            carry_own, carry.at[k - 1], carry_send.at[k - 1], carry_recv.at[k - 1],
            {"sp": lax.rem(z + k, spans)},
        )

    for k in (1, 2, 3):
        pl.when(z + k < spans)(lambda: carry_copy(k).start())

    def state_copy():
        return remote(
            state_own, carry.at[3], carry_send.at[3], carry_recv.at[3], {"sp": lax.rem(z + 4, spans)}
        )

    @pl.when(z == 0)
    def _():
        state_own[...] = carry_own[...]
        state_copy().start()

    r2 = goal(2, 1, 1, 2)
    lax.fori_loop(r1 + 1, r2 + 1, ring, 0)

    in_copies[8].wait()
    for j in range(width // LANES):
        part = pl.ds(j * LANES, LANES)
        wg[part, :] = (wg[part, :].astype(F32) * gain_cols[:, j : j + 1]).astype(BF16)

    def gate(i, _):
        part = pl.ds(pl.multiple_of(i * tile, tile), tile)
        acc = jnp.dot(tok[part, :], wg[...], preferred_element_type=F32)
        inv = invc[part, :]
        for c in range(lanes2):
            lane = slice(c * LANES, (c + 1) * LANES)
            ge[part, lane] = gelu((acc[:, lane] * inv).astype(BF16).astype(F32))
        return 0

    lax.fori_loop(0, 4, gate, 0)
    r3 = goal(3, 2, 1, 3)
    lax.fori_loop(r2 + 1, r3 + 1, ring, 0)
    s0 = goal(1, 1, 0, 0)
    lax.fori_loop(1, s0 + 1, spread, 0)

    r4 = goal(8, 5, 1, 3)
    lax.fori_loop(r3 + 1, r4 + 1, ring, 0)
    s1 = goal(7, 4, 0, 0)
    lax.fori_loop(s0 + 1, s1 + 1, spread, 0)

    def received(copy, slot, k):
        pl.when(z >= k)(lambda: copy.wait_recv())

        @pl.when(z < k)
        def _():
            carry[slot] = jnp.zeros(carry.shape[1:], F32)

    received(state_copy(), 3, 4)
    for k in (1, 2, 3):
        received(carry_copy(k), k - 1, k)
    incoming, out_states = [], []
    for c in range(lanes2):
        h = carry[3, lanes2 + c : lanes2 + c + 1, :]
        for k in (3, 2, 1):
            h = carry[k - 1, c : c + 1, :] * h + carry[k - 1, lanes2 + c : lanes2 + c + 1, :]
        incoming.append(h)
        out_state = carry_own[c : c + 1, :] * h + carry_own[lanes2 + c : lanes2 + c + 1, :]
        out_states.append(out_state)

    @pl.when(jnp.logical_and(z > 0, z + 4 < spans))
    def _():
        for c in range(lanes2):
            state_own[c : c + 1, :] = jnp.zeros((1, LANES), F32)
            state_own[lanes2 + c : lanes2 + c + 1, :] = out_states[c]
        state_copy().start()

    def a2a_copy(other):
        return remote(gout.at[other], grecv.at[tp], a2a_send, a2a_recv.at[tp], {"tp": other})

    def ss_copy(other):
        return remote(ss_own.at[other], ss_recv.at[tp], ss_send, ss_recv_sem, {"tp": other})

    ones = jnp.ones((8, LANES), F32)

    def read_out(i, _):
        s = lax.rem(tp + 4 + i, peers)
        total = jnp.zeros((mine, LANES), F32)
        for c in range(lanes2):
            lane = slice(c * LANES, (c + 1) * LANES)
            enter = segp[c, pl.ds(s, 1), :] * incoming[c] + segh[c, pl.ds(s, 1), :]
            lines = pl.ds(s, mine, stride=SEGS)
            state = ht[c, lines, :] + pt[c, lines, :] * enter
            gated = state * ge[pl.ds(pl.multiple_of(s * mine, mine), mine), lane]
            total = total + gated * gated
            gout[s, :, lane] = (gated * ogain[:, lane]).astype(BF16)
        sums = lax.dot_general(
            ones, total, (((1,), (1,)), ((), ())), preferred_element_type=F32
        )
        ss_own[s] = sums[0:1, :]

        @pl.when(i != 4)
        def _():
            a2a_copy(s).start()
            ss_copy(s).start()

        return 0

    lax.fori_loop(0, 8, read_out, 0)
    grecv[tp] = gout[tp]
    ss_recv[tp] = ss_own[tp]

    lax.fori_loop(r4 + 1, count + 1, ring, 0)
    lax.fori_loop(s1 + 1, count + 1, spread, 0)

    for pos in range(4, 8):
        wv_copies[pos].wait()
    for k in range(1, 8):
        other = lax.rem(tp + k, peers)
        remote(gout.at[other], grecv.at[other], a2a_send, a2a_recv.at[other], {"tp": other}).wait_recv()
    seven = ss_recv.at[pl.ds(0, 7)]
    local(seven, seven, ss_recv_sem).wait()

    def other_half(t, _):
        d_copy(0, 1 - core, t).wait_recv()
        d_copy(1, 1 - core, t).wait_recv()
        return 0

    lax.fori_loop(1, count_other + 1, other_half, 0)

    total = ss_recv[0]
    for k in range(1, 8):
        total = total + ss_recv[k]
    scales = lax.rsqrt(total * (1.0 / width) + 1e-06)
    scales = jnp.broadcast_to(scales, (LANES, mine)).T

    def finish(pos, _):
        acc = jnp.zeros((mine, channels), F32)
        for k in range(8):
            acc = acc + jnp.dot(
                grecv[k], wv[pos, k * channels : (k + 1) * channels, :], preferred_element_type=F32
            )
        for c in range(lanes2):
            lane = slice(c * LANES, (c + 1) * LANES)
            obuf[pos, :, lane] = (acc[:, lane] * scales).astype(BF16)
        return 0

    def out_copy(pos):
        return local(obuf.at[pos], out.at[:, pl.ds(column(pos), channels)], out_sem.at[pos])

    def passed(t, _):
        for pos in range(4):
            z_copy(t, pos, z).wait_send()
        return 0

    def shared(t, _):
        for k in range(3):
            share_copy(k, t).wait_send()
        d_copy(0, core, t).wait_send()
        d_copy(1, core, t).wait_send()
        return 0

    lax.fori_loop(1, count_out + 1, passed, 0)
    lax.fori_loop(1, count + 1, shared, 0)
    pl.when(z < last)(lambda: halo_copy().wait_send())
    for k in (1, 2, 3):
        pl.when(z + k < spans)(lambda: carry_copy(k).wait_send())
    pl.when(z + 4 < spans)(lambda: state_copy().wait_send())
    sent = gout.at[pl.ds(0, 7)]
    local(sent, sent, a2a_send).wait()
    sent = ss_own.at[pl.ds(0, 7)]
    local(sent, sent, ss_send).wait()
    for pos in range(8):
        finish(pos, 0)
    for pos in range(8):
        out_copy(pos).start()
    for pos in range(8):
        out_copy(pos).wait()


def body(
    tokens, in_gain, w_input, w_gate, conv_taps, w_rate, w_inlet, decay_param, decay_bias, out_gain, w_out
):
    rows, width = tokens.shape
    channels = w_input.shape[1]
    lanes2 = channels // LANES
    spans, peers = lax.axis_size("sp"), lax.axis_size("tp")
    mine = rows // peers
    vmem = pltpu.VMEM
    dma = pltpu.SemaphoreType.DMA
    scratch = [
        vmem((rows, width), BF16),
        vmem((width, channels), BF16),
        vmem((width, channels), BF16),
        vmem((channels, 2 * channels), BF16),
        vmem((width // LANES, LANES), F32),
        vmem((4, channels), F32),
        vmem((1, channels), F32),
        vmem((rows // LANES, LANES), F32),
        vmem((1, channels), F32),
        vmem((8, width, channels), BF16),
        vmem((8 + rows, channels), F32),
        vmem((8, channels), F32),
        vmem((rows, LANES), F32),
        vmem((rows, LANES), F32),
        vmem((SEGS * STEP, channels), BF16),
        vmem((SEGS * STEP, 2 * channels), F32),
        vmem((lanes2, SEGS * PAD, LANES), F32),
        vmem((lanes2, SEGS * PAD, LANES), F32),
        vmem((lanes2, rows, LANES), F32),
        vmem((lanes2, rows, LANES), F32),
        vmem((rows, channels), F32),
        vmem((lanes2, SEGS, LANES), F32),
        vmem((lanes2, SEGS, LANES), F32),
        vmem((2 * lanes2, LANES), F32),
        vmem((2 * lanes2, LANES), F32),
        vmem((4, 2 * lanes2, LANES), F32),
        vmem((peers, mine, channels), BF16),
        vmem((peers, mine, channels), BF16),
        vmem((peers, 1, mine), F32),
        vmem((peers, 1, mine), F32),
        vmem((8, mine, channels), BF16),
        dma((4,)),
        dma((9,)),
        dma((8,)),
        dma((8,)),
        dma((11, 4)),
        dma((11, 4)),
        dma((2, 11)),
        dma((11,)),
        dma((2, 11)),
        dma((11,)),
        dma((2, 11)),
        dma((2, 11)),
        dma(()),
        dma(()),
        dma((4,)),
        dma((4,)),
        dma(()),
        dma((8,)),
        dma(()),
        dma(()),
    ]
    scratch += [pltpu.SemaphoreType.REGULAR((3,))]
    spec = pl.BlockSpec(memory_space=pl.ANY)
    return pl.pallas_call(
        kernel,
        out_shape=jax.ShapeDtypeStruct((mine, width), BF16),
        in_specs=[spec] * 11,
        out_specs=spec,
        scratch_shapes=scratch,
        compiler_params=pltpu.CompilerParams(
            collective_id=0, has_side_effects=True, vmem_limit_bytes=60 * 1024 * 1024
        ),
        name="gated_recurrence",
    )(
        tokens,
        in_gain.reshape(width // LANES, LANES),
        w_input,
        w_gate,
        conv_taps,
        w_rate.reshape(channels, channels),
        w_inlet.reshape(channels, channels),
        decay_param.reshape(1, channels),
        decay_bias.reshape(rows // LANES, LANES),
        out_gain.reshape(1, channels),
        w_out,
    )


def solution(mesh):
    return jax.shard_map(
        body,
        mesh=mesh,
        in_specs=(
            P(("grp", "sp"), None),
            P(),
            P(None, "tp"),
            P(None, "tp"),
            P(None, "tp"),
            P("tp", None, None),
            P("tp", None, None),
            P("tp"),
            P("tp", ("grp", "sp")),
            P("tp"),
            P("sp", None),
        ),
        out_specs=P(("grp", "sp", "tp"), None),
        check_vma=False,
    )
```

```python
import functools

import jax
import jax.numpy as jnp
from jax import lax
from jax.experimental import pallas as pl
from jax.experimental.pallas import tpu as pltpu
from jax.sharding import PartitionSpec as P

MESH = pl.DeviceIdType.MESH
F32 = jnp.float32
BF16 = jnp.bfloat16
LANES = 128
SEGS = 8
STEP = 32
PAD = 40


def log1p_small(u):
    series = u * (1.0 - u * (0.5 - u * (1.0 / 3.0 - u * (0.25 - u * (0.2 - u / 6.0)))))
    return jnp.where(u < 0.06, series, jnp.log(1.0 + u))


def softplus(x):
    return jnp.maximum(x, 0.0) + log1p_small(jnp.exp(-jnp.abs(x)))


def gelu(x):
    inner = 0.7978845608028654 * (x + 0.044715 * (x * x * x))
    return 0.5 * x * (1.0 + jnp.tanh(inner))


def kernel(
    tokens_in,
    gain_in,
    w_input_in,
    w_gate_in,
    taps_in,
    w_rate_in,
    w_inlet_in,
    dparam_in,
    bias_in,
    ogain_in,
    w_out_in,
    out,
    tok,
    wi,
    wg,
    wrn,
    gain,
    taps,
    dparam,
    bias,
    ogain,
    wv,
    proj,
    halo,
    biasc,
    invc,
    conv,
    gates,
    sa,
    sb,
    ht,
    pt,
    ge,
    segh,
    segp,
    carry_own,
    state_own,
    carry,
    gout,
    grecv,
    ss_own,
    ss_recv,
    obuf,
    tok_sem,
    in_sem,
    wv_sem,
    out_sem,
    zs,
    zr,
    xr,
    yr,
    xs,
    ys,
    ds_send,
    ds_recv,
    halo_send,
    halo_recv,
    carry_send,
    carry_recv,
    a2a_send,
    a2a_recv,
    ss_send,
    ss_recv_sem,
    know,
):
    grp, z, tp = lax.axis_index("grp"), lax.axis_index("sp"), lax.axis_index("tp")
    spans, peers = lax.axis_size("sp"), lax.axis_size("tp")
    core = lax.rem(tp, 2)
    rows, width = tok.shape
    channels = wi.shape[1]
    lanes2 = channels // LANES
    block = width // spans
    tile = rows // 4
    mine = rows // peers
    first = lax.rem(2 * (tp // 2) + 4 * lax.rem(grp, 2), 8)
    partner = grp + 1 - 2 * lax.rem(grp, 2)
    sibling = tp + 1 - 2 * core

    def column(pos):
        return pl.multiple_of(lax.rem(first + pos, 8) * channels, channels)

    def local(src, dst, sem):
        return pltpu.make_async_copy(src, dst, sem)

    def remote(src, dst, send, recv, where):
        return pltpu.make_async_remote_copy(
            src_ref=src, dst_ref=dst, send_sem=send, recv_sem=recv, device_id=where, device_id_type=MESH
        )

    own_lines = pl.ds(pl.multiple_of(z * block, block), block)
    wv_copies = [
        local(w_out_in.at[:, pl.ds(column(pos), channels)], wv.at[pos, own_lines, :], wv_sem.at[pos])
        for pos in range(8)
    ]
    for pos in range(4):
        wv_copies[pos].start()
    in_copies = [
        local(gain_in, gain, in_sem.at[0]),
        local(w_input_in, wi, in_sem.at[1]),
        local(bias_in, bias, in_sem.at[2]),
        local(taps_in, taps, in_sem.at[3]),
        local(dparam_in, dparam, in_sem.at[4]),
        local(ogain_in, ogain, in_sem.at[5]),
        local(w_rate_in, wrn.at[:, 0:channels], in_sem.at[6]),
        local(w_inlet_in, wrn.at[:, channels : 2 * channels], in_sem.at[7]),
        local(w_gate_in, wg, in_sem.at[8]),
    ]
    for k in (0, 1, 2):
        in_copies[k].start()

    def tok_copy(k):
        part = pl.ds(pl.multiple_of(k * tile, tile), tile)
        return local(tokens_in.at[part, :], tok.at[part, :], tok_sem.at[k])

    for k in (3, 2, 1, 0):
        tok_copy(k).start()
    for k in range(3, 9):
        in_copies[k].start()
    for pos in range(4, 8):
        wv_copies[pos].start()

    last = spans - 1
    barrier = pltpu.get_barrier_semaphore()
    above, below = lax.rem(z + 1, spans), lax.rem(z + last, spans)
    for where in (
        [{"sp": above}, {"sp": below}, {"grp": partner}]
        + [{"tp": lax.rem(tp + k, peers)} for k in range(1, 8)]
    ):
        pl.semaphore_signal(barrier, inc=1, device_id=where, device_id_type=MESH)

    def learn(level):
        pl.when(z < last)(lambda: pl.semaphore_wait(know.at[level], 1))

    def teach(level):
        @pl.when(z > 0)
        def _():
            pl.semaphore_signal(know.at[level], inc=1, device_id={"sp": below}, device_id_type=MESH)

    def blocks_at(span):
        low = jnp.minimum(lax.rem(span + last, spans), 2) + 6 - jnp.where(span > 0, 0, 2)
        return (1 - core) * low + core * (spans - 1 - low)

    count = blocks_at(z)
    onward = lax.rem(z + 1 + core * (spans - 2), spans)
    count_out = blocks_at(onward)
    count_other = spans - 1 - count

    def owner_of(way, t):
        return lax.rem(z + (1 - way) * (spans - t) + way * t, spans)

    def lines_of(owner):
        return pl.ds(pl.multiple_of(owner * block, block), block)

    def z_copy(t, pos, owner):
        part = wv.at[pos, lines_of(owner), :]
        return remote(part, part, zs.at[t, pos], zr.at[t, pos], {"sp": onward})

    def share_copy(k, t):
        lines = lines_of(owner_of(core, t))
        if k < 2:
            where = {"tp": lax.rem(tp + 2 + 4 * k, peers)}
            return remote(
                wv.at[1 + k, lines, :], wv.at[7 - 3 * k, lines, :], xs.at[k, t], xr.at[k, t], where
            )
        return remote(
            wv.at[1:3, lines, :], wv.at[5:7, lines, :], ys.at[t], yr.at[t], {"grp": partner}
        )

    def d_copy(level, way, t):
        part = wv.at[4 * level : 4 * level + 4, lines_of(owner_of(way, t)), :]
        return remote(part, part, ds_send.at[level, t], ds_recv.at[level, t], {"tp": sibling})

    def ring(t, _):
        owner = owner_of(core, t)
        for pos in (1, 2, 0, 3):
            z_copy(t, pos, owner).wait_recv()

            @pl.when(t < count_out)
            def _():
                z_copy(t + 1, pos, owner).start()

        for k in range(3):
            share_copy(k, t).start()
        d_copy(0, core, t).start()
        return 0

    def spread(t, _):
        for k in range(3):
            share_copy(k, t).wait_recv()
        d_copy(1, core, t).start()
        return 0

    def goal(up, down, first_up, first_down):
        up = jnp.where(z > 0, jnp.minimum(up, jnp.maximum(z - 2, 0)), first_up)
        down = jnp.where(z > 0, jnp.where(z == 1, jnp.maximum(down, 4), down), first_down)
        return (1 - core) * up + core * down

    def first_sends():
        for pos in (1, 2, 0, 3):
            z_copy(1, pos, z).start()

    in_copies[0].wait()
    in_copies[1].wait()
    in_copies[2].wait()
    gain_cols = gain[...].T
    bias_cols = bias[...].T
    for j in range(width // LANES):
        part = pl.ds(j * LANES, LANES)
        wi[part, :] = (wi[part, :].astype(F32) * gain_cols[:, j : j + 1]).astype(BF16)
        biasc[part, :] = jnp.broadcast_to(bias_cols[:, j : j + 1], (LANES, LANES))

    def halo_copy():
        return remote(proj.at[pl.ds(rows, 8), :], halo, halo_send, halo_recv, {"sp": above})

    def project(i, _):
        k = 3 - i
        base = pl.multiple_of(k * tile, tile)
        tok_copy(k).wait()

        part = pl.ds(base, tile)
        acc = jnp.dot(tok[part, :], wi[...], preferred_element_type=F32)
        for j in range(tile // 64):
            lines = pl.ds(pl.multiple_of(base + j * 64, 64), 64)
            total = jnp.zeros((64, LANES), F32)
            for c in range(width // LANES):
                x = tok[lines, c * LANES : (c + 1) * LANES].astype(F32)
                total = total + x * x
            mean = jnp.sum(total, axis=1, keepdims=True) * (1.0 / width)
            inv = jnp.broadcast_to(lax.rsqrt(mean + 1e-06), (64, LANES))
            invc[lines, :] = inv
            for c in range(lanes2):
                lane = slice(c * LANES, (c + 1) * LANES)
                scaled = acc[j * 64 : (j + 1) * 64, lane] * inv
                proj[pl.ds(base + 8 + j * 64, 64), lane] = scaled.astype(BF16).astype(F32)

        return 0

    lax.fori_loop(0, 1, project, 0)
    pl.semaphore_wait(barrier, 10)
    pl.when(z < last)(lambda: halo_copy().start())
    teach(0)
    for pos in range(4):
        wv_copies[pos].wait()
    first_sends()
    lax.fori_loop(1, 4, project, 0)
    learn(0)
    teach(1)

    for k in range(3, 8):
        in_copies[k].wait()
    ahead = jnp.where(z == 1, 4 * core, 0)
    lax.fori_loop(1, ahead + 1, ring, 0)
    pl.when(z > 0)(lambda: halo_copy().wait_recv())

    @pl.when(z > 0)
    def _():
        proj[0:8, :] = halo[...]

    @pl.when(z == 0)
    def _():
        proj[0:8, :] = jnp.zeros((8, channels), F32)

    scale = -8.0 * softplus(-dparam[...])
    tap = [taps[k : k + 1, :] for k in range(4)]

    def gather_inputs(i):
        for s in range(SEGS):
            base = pl.multiple_of(s * mine + i * STEP, STEP)
            x = proj[pl.ds(base, STEP + 8), :]
            total = pltpu.roll(x, 3, axis=0)[8:] * tap[0]
            total = total + pltpu.roll(x, 2, axis=0)[8:] * tap[1]
            total = total + pltpu.roll(x, 1, axis=0)[8:] * tap[2]
            total = total + x[8:] * tap[3]
            conv[s * STEP : (s + 1) * STEP, :] = total.astype(BF16)

    def scan_tile(i, state):
        gather_inputs(i)
        gates[...] = jnp.dot(conv[...], wrn[...], preferred_element_type=F32)
        for s in range(SEGS):
            base = pl.multiple_of(s * mine + i * STEP, STEP)
            shift = biasc[pl.ds(base, STEP), :]
            part = slice(s * STEP, (s + 1) * STEP)
            for c in range(channels // LANES):
                lane = slice(c * LANES, (c + 1) * LANES)
                rate = jax.nn.sigmoid(gates[part, lane])
                inlet = jax.nn.sigmoid(gates[part, channels + c * LANES : channels + (c + 1) * LANES])
                log_decay = rate * scale[:, lane] + shift
                decay = jnp.exp(log_decay)
                y = -2.0 * log_decay
                series = y * (
                    1.0 - y * (0.5 - y * (1.0 / 6.0 - y * (1.0 / 24.0 - y * (1.0 / 120.0))))
                )
                grown = jnp.where(y < 0.2, series, 1.0 - decay * decay)
                root = grown * lax.rsqrt(jnp.maximum(grown, 1e-37))
                drive = root * inlet * conv[part, lane].astype(F32)
                sa[c, s * PAD : s * PAD + STEP, :] = decay
                sb[c, s * PAD : s * PAD + STEP, :] = drive
        state = list(state)
        for r in range(STEP):
            line = pl.ds(pl.multiple_of((i * STEP + r) * SEGS, SEGS), SEGS)
            for c in range(channels // LANES):
                a = sa[c, pl.ds(r, SEGS, stride=PAD), :]
                b = sb[c, pl.ds(r, SEGS, stride=PAD), :]
                h, p = state[2 * c], state[2 * c + 1]
                h, p = a * h + b, a * p
                ht[c, line, :] = h
                pt[c, line, :] = p
                state[2 * c], state[2 * c + 1] = h, p
        return tuple(state)

    state = (jnp.zeros((SEGS, LANES), F32), jnp.ones((SEGS, LANES), F32)) * lanes2
    state = lax.fori_loop(0, 3, scan_tile, state)
    learn(1)
    teach(2)
    r0 = goal(1, 0, 0, 1)
    lax.fori_loop(ahead + 1, r0 + 1, ring, 0)
    state = lax.fori_loop(3, 6, scan_tile, state)
    r1 = goal(1, 1, 0, 2)
    lax.fori_loop(r0 + 1, r1 + 1, ring, 0)
    state = lax.fori_loop(6, 8, scan_tile, state)

    for c in range(lanes2):
        h_end, p_end = state[2 * c], state[2 * c + 1]
        h, p = jnp.zeros((1, LANES), F32), jnp.ones((1, LANES), F32)
        for s in range(SEGS):
            segh[c, s : s + 1, :] = h
            segp[c, s : s + 1, :] = p
            h = p_end[s : s + 1] * h + h_end[s : s + 1]
            p = p_end[s : s + 1] * p
        carry_own[c : c + 1, :] = p
        carry_own[lanes2 + c : lanes2 + c + 1, :] = h

    learn(2)

    def carry_copy(k):
        return remote(
            carry_own, carry.at[k - 1], carry_send.at[k - 1], carry_recv.at[k - 1],
            {"sp": lax.rem(z + k, spans)},
        )

    for k in (1, 2, 3):
        pl.when(z + k < spans)(lambda: carry_copy(k).start())

    def state_copy():
        return remote(
            state_own, carry.at[3], carry_send.at[3], carry_recv.at[3], {"sp": lax.rem(z + 4, spans)}
        )

    @pl.when(z == 0)
    def _():
        state_own[...] = carry_own[...]
        state_copy().start()

    r2 = goal(1, 1, 1, 3)
    lax.fori_loop(r1 + 1, r2 + 1, ring, 0)

    in_copies[8].wait()
    for j in range(width // LANES):
        part = pl.ds(j * LANES, LANES)
        wg[part, :] = (wg[part, :].astype(F32) * gain_cols[:, j : j + 1]).astype(BF16)

    def gate(i, _):
        part = pl.ds(pl.multiple_of(i * tile, tile), tile)
        acc = jnp.dot(tok[part, :], wg[...], preferred_element_type=F32)
        inv = invc[part, :]
        for c in range(lanes2):
            lane = slice(c * LANES, (c + 1) * LANES)
            ge[part, lane] = gelu((acc[:, lane] * inv).astype(BF16).astype(F32))
        return 0

    lax.fori_loop(0, 2, gate, 0)
    rg = goal(2, 1, 1, 4)
    lax.fori_loop(r2 + 1, rg + 1, ring, 0)
    lax.fori_loop(2, 4, gate, 0)
    r3 = goal(3, 2, 1, 5)
    lax.fori_loop(rg + 1, r3 + 1, ring, 0)
    s0 = goal(1, 1, 0, 2)
    lax.fori_loop(1, s0 + 1, spread, 0)

    r4 = goal(8, 5, 1, 5)
    lax.fori_loop(r3 + 1, r4 + 1, ring, 0)
    s1 = goal(7, 4, 0, 2)
    lax.fori_loop(s0 + 1, s1 + 1, spread, 0)

    def received(copy, slot, k):
        pl.when(z >= k)(lambda: copy.wait_recv())

        @pl.when(z < k)
        def _():
            carry[slot] = jnp.zeros(carry.shape[1:], F32)

    received(state_copy(), 3, 4)
    for k in (1, 2, 3):
        received(carry_copy(k), k - 1, k)
    incoming, out_states = [], []
    for c in range(lanes2):
        h = carry[3, lanes2 + c : lanes2 + c + 1, :]
        for k in (3, 2, 1):
            h = carry[k - 1, c : c + 1, :] * h + carry[k - 1, lanes2 + c : lanes2 + c + 1, :]
        incoming.append(h)
        out_state = carry_own[c : c + 1, :] * h + carry_own[lanes2 + c : lanes2 + c + 1, :]
        out_states.append(out_state)

    @pl.when(jnp.logical_and(z > 0, z + 4 < spans))
    def _():
        for c in range(lanes2):
            state_own[c : c + 1, :] = jnp.zeros((1, LANES), F32)
            state_own[lanes2 + c : lanes2 + c + 1, :] = out_states[c]
        state_copy().start()

    def a2a_copy(other):
        return remote(gout.at[other], grecv.at[tp], a2a_send, a2a_recv.at[tp], {"tp": other})

    def ss_copy(other):
        return remote(ss_own.at[other], ss_recv.at[tp], ss_send, ss_recv_sem, {"tp": other})

    ones = jnp.ones((8, LANES), F32)

    def read_out(i, _):
        s = lax.rem(tp + 4 + i, peers)
        total = jnp.zeros((mine, LANES), F32)
        for c in range(lanes2):
            lane = slice(c * LANES, (c + 1) * LANES)
            enter = segp[c, pl.ds(s, 1), :] * incoming[c] + segh[c, pl.ds(s, 1), :]
            lines = pl.ds(s, mine, stride=SEGS)
            state = ht[c, lines, :] + pt[c, lines, :] * enter
            gated = state * ge[pl.ds(pl.multiple_of(s * mine, mine), mine), lane]
            total = total + gated * gated
            gout[s, :, lane] = (gated * ogain[:, lane]).astype(BF16)
        sums = lax.dot_general(
            ones, total, (((1,), (1,)), ((), ())), preferred_element_type=F32
        )
        ss_own[s] = sums[0:1, :]

        @pl.when(i != 4)
        def _():
            a2a_copy(s).start()
            ss_copy(s).start()

        return 0

    lax.fori_loop(0, 8, read_out, 0)
    grecv[tp] = gout[tp]
    ss_recv[tp] = ss_own[tp]

    def both(t, _):
        ring(t, 0)
        pl.when(t - 3 > s1)(lambda: (spread(t - 3, 0), None)[1])
        return 0

    lax.fori_loop(r4 + 1, count + 1, both, 0)
    lax.fori_loop(jnp.maximum(s1, jnp.where(count > r4, count - 3, s1)) + 1, count + 1, spread, 0)

    for pos in range(4, 8):
        wv_copies[pos].wait()
    for k in range(1, 8):
        other = lax.rem(tp + k, peers)
        remote(gout.at[other], grecv.at[other], a2a_send, a2a_recv.at[other], {"tp": other}).wait_recv()
    seven = ss_recv.at[pl.ds(0, 7)]
    local(seven, seven, ss_recv_sem).wait()

    def other_half(t, _):
        d_copy(0, 1 - core, t).wait_recv()
        d_copy(1, 1 - core, t).wait_recv()
        return 0

    lax.fori_loop(1, count_other + 1, other_half, 0)

    total = ss_recv[0]
    for k in range(1, 8):
        total = total + ss_recv[k]
    scales = lax.rsqrt(total * (1.0 / width) + 1e-06)
    scales = jnp.broadcast_to(scales, (LANES, mine)).T

    def finish(pos, _):
        acc = jnp.zeros((mine, channels), F32)
        for k in range(8):
            acc = acc + jnp.dot(
                grecv[k], wv[pos, k * channels : (k + 1) * channels, :], preferred_element_type=F32
            )
        for c in range(lanes2):
            lane = slice(c * LANES, (c + 1) * LANES)
            where = pl.ds(pl.multiple_of(column(pos) + c * LANES, LANES), LANES)
            obuf[:, where] = (acc[:, lane] * scales).astype(BF16)
        return 0

    def out_copy(k):
        part = pl.ds(k * (mine // 4), mine // 4)
        return local(obuf.at[part, :], out.at[part, :], out_sem.at[k])

    def passed(t, _):
        for pos in range(4):
            z_copy(t, pos, z).wait_send()
        return 0

    def shared(t, _):
        for k in range(3):
            share_copy(k, t).wait_send()
        d_copy(0, core, t).wait_send()
        d_copy(1, core, t).wait_send()
        return 0

    lax.fori_loop(1, count_out + 1, passed, 0)
    lax.fori_loop(1, count + 1, shared, 0)
    pl.when(z < last)(lambda: halo_copy().wait_send())
    for k in (1, 2, 3):
        pl.when(z + k < spans)(lambda: carry_copy(k).wait_send())
    pl.when(z + 4 < spans)(lambda: state_copy().wait_send())
    sent = gout.at[pl.ds(0, 7)]
    local(sent, sent, a2a_send).wait()
    sent = ss_own.at[pl.ds(0, 7)]
    local(sent, sent, ss_send).wait()
    for pos in range(8):
        finish(pos, 0)
    for k in range(4):
        out_copy(k).start()
    for k in range(4):
        out_copy(k).wait()


def body(
    tokens, in_gain, w_input, w_gate, conv_taps, w_rate, w_inlet, decay_param, decay_bias, out_gain, w_out
):
    rows, width = tokens.shape
    channels = w_input.shape[1]
    lanes2 = channels // LANES
    spans, peers = lax.axis_size("sp"), lax.axis_size("tp")
    mine = rows // peers
    vmem = pltpu.VMEM
    dma = pltpu.SemaphoreType.DMA
    scratch = [
        vmem((rows, width), BF16),
        vmem((width, channels), BF16),
        vmem((width, channels), BF16),
        vmem((channels, 2 * channels), BF16),
        vmem((width // LANES, LANES), F32),
        vmem((4, channels), F32),
        vmem((1, channels), F32),
        vmem((rows // LANES, LANES), F32),
        vmem((1, channels), F32),
        vmem((8, width, channels), BF16),
        vmem((8 + rows, channels), F32),
        vmem((8, channels), F32),
        vmem((rows, LANES), F32),
        vmem((rows, LANES), F32),
        vmem((SEGS * STEP, channels), BF16),
        vmem((SEGS * STEP, 2 * channels), F32),
        vmem((lanes2, SEGS * PAD, LANES), F32),
        vmem((lanes2, SEGS * PAD, LANES), F32),
        vmem((lanes2, rows, LANES), F32),
        vmem((lanes2, rows, LANES), F32),
        vmem((rows, channels), F32),
        vmem((lanes2, SEGS, LANES), F32),
        vmem((lanes2, SEGS, LANES), F32),
        vmem((2 * lanes2, LANES), F32),
        vmem((2 * lanes2, LANES), F32),
        vmem((4, 2 * lanes2, LANES), F32),
        vmem((peers, mine, channels), BF16),
        vmem((peers, mine, channels), BF16),
        vmem((peers, 1, mine), F32),
        vmem((peers, 1, mine), F32),
        vmem((mine, width), BF16),
        dma((4,)),
        dma((9,)),
        dma((8,)),
        dma((8,)),
        dma((11, 4)),
        dma((11, 4)),
        dma((2, 11)),
        dma((11,)),
        dma((2, 11)),
        dma((11,)),
        dma((2, 11)),
        dma((2, 11)),
        dma(()),
        dma(()),
        dma((4,)),
        dma((4,)),
        dma(()),
        dma((8,)),
        dma(()),
        dma(()),
    ]
    scratch += [pltpu.SemaphoreType.REGULAR((3,))]
    spec = pl.BlockSpec(memory_space=pl.ANY)
    return pl.pallas_call(
        kernel,
        out_shape=jax.ShapeDtypeStruct((mine, width), BF16),
        in_specs=[spec] * 11,
        out_specs=spec,
        scratch_shapes=scratch,
        compiler_params=pltpu.CompilerParams(
            collective_id=0, has_side_effects=True, vmem_limit_bytes=60 * 1024 * 1024
        ),
        name="gated_recurrence",
    )(
        tokens,
        in_gain.reshape(width // LANES, LANES),
        w_input,
        w_gate,
        conv_taps,
        w_rate.reshape(channels, channels),
        w_inlet.reshape(channels, channels),
        decay_param.reshape(1, channels),
        decay_bias.reshape(rows // LANES, LANES),
        out_gain.reshape(1, channels),
        w_out,
    )


def solution(mesh):
    return jax.shard_map(
        body,
        mesh=mesh,
        in_specs=(
            P(("grp", "sp"), None),
            P(),
            P(None, "tp"),
            P(None, "tp"),
            P(None, "tp"),
            P("tp", None, None),
            P("tp", None, None),
            P("tp"),
            P("tp", ("grp", "sp")),
            P("tp"),
            P("sp", None),
        ),
        out_specs=P(("grp", "sp", "tp"), None),
        check_vma=False,
    )
```

```python
import functools

import jax
import jax.numpy as jnp
from jax import lax
from jax.experimental import pallas as pl
from jax.experimental.pallas import tpu as pltpu
from jax.sharding import PartitionSpec as P

MESH = pl.DeviceIdType.MESH
F32 = jnp.float32
BF16 = jnp.bfloat16
LANES = 128
SEGS = 8
STEP = 32
PAD = 40


def log1p_small(u):
    series = u * (1.0 - u * (0.5 - u * (1.0 / 3.0 - u * (0.25 - u * (0.2 - u / 6.0)))))
    return jnp.where(u < 0.06, series, jnp.log(1.0 + u))


def softplus(x):
    return jnp.maximum(x, 0.0) + log1p_small(jnp.exp(-jnp.abs(x)))


def gelu(x):
    inner = 0.7978845608028654 * (x + 0.044715 * (x * x * x))
    return 0.5 * x * (1.0 + jnp.tanh(inner))


def kernel(
    tokens_in,
    gain_in,
    w_input_in,
    w_gate_in,
    taps_in,
    w_rate_in,
    w_inlet_in,
    dparam_in,
    bias_in,
    ogain_in,
    w_out_in,
    out,
    tok,
    wi,
    wg,
    wrn,
    gain,
    taps,
    dparam,
    bias,
    ogain,
    wv,
    proj,
    halo,
    biasc,
    invc,
    conv,
    gates,
    sa,
    sb,
    ht,
    pt,
    ge,
    segh,
    segp,
    carry_own,
    state_own,
    carry,
    gout,
    grecv,
    ss_own,
    ss_recv,
    obuf,
    tok_sem,
    in_sem,
    wv_sem,
    out_sem,
    zs,
    zr,
    xr,
    yr,
    xs,
    ys,
    ds_send,
    ds_recv,
    halo_send,
    halo_recv,
    carry_send,
    carry_recv,
    a2a_send,
    a2a_recv,
    ss_send,
    ss_recv_sem,
    know,
):
    grp, z, tp = lax.axis_index("grp"), lax.axis_index("sp"), lax.axis_index("tp")
    spans, peers = lax.axis_size("sp"), lax.axis_size("tp")
    core = lax.rem(tp, 2)
    rows, width = tok.shape
    channels = wi.shape[1]
    lanes2 = channels // LANES
    block = width // spans
    tile = rows // 4
    mine = rows // peers
    first = lax.rem(2 * (tp // 2) + 4 * lax.rem(grp, 2), 8)
    partner = grp + 1 - 2 * lax.rem(grp, 2)
    sibling = tp + 1 - 2 * core

    def column(pos):
        return pl.multiple_of(lax.rem(first + pos, 8) * channels, channels)

    def local(src, dst, sem):
        return pltpu.make_async_copy(src, dst, sem)

    def remote(src, dst, send, recv, where):
        return pltpu.make_async_remote_copy(
            src_ref=src, dst_ref=dst, send_sem=send, recv_sem=recv, device_id=where, device_id_type=MESH
        )

    own_lines = pl.ds(pl.multiple_of(z * block, block), block)
    wv_copies = [
        local(w_out_in.at[:, pl.ds(column(pos), channels)], wv.at[pos, own_lines, :], wv_sem.at[pos])
        for pos in range(8)
    ]
    for pos in range(4):
        wv_copies[pos].start()
    in_copies = [
        local(gain_in, gain, in_sem.at[0]),
        local(w_input_in, wi, in_sem.at[1]),
        local(bias_in, bias, in_sem.at[2]),
        local(taps_in, taps, in_sem.at[3]),
        local(dparam_in, dparam, in_sem.at[4]),
        local(ogain_in, ogain, in_sem.at[5]),
        local(w_rate_in, wrn.at[:, 0:channels], in_sem.at[6]),
        local(w_inlet_in, wrn.at[:, channels : 2 * channels], in_sem.at[7]),
        local(w_gate_in, wg, in_sem.at[8]),
    ]
    for k in (0, 1, 2):
        in_copies[k].start()

    def tok_copy(k):
        part = pl.ds(pl.multiple_of(k * tile, tile), tile)
        return local(tokens_in.at[part, :], tok.at[part, :], tok_sem.at[k])

    for k in (3, 2, 1, 0):
        tok_copy(k).start()
    for k in range(3, 9):
        in_copies[k].start()
    for pos in range(4, 8):
        wv_copies[pos].start()

    last = spans - 1
    barrier = pltpu.get_barrier_semaphore()
    above, below = lax.rem(z + 1, spans), lax.rem(z + last, spans)
    for where in (
        [{"sp": above}, {"sp": below}, {"grp": partner}]
        + [{"tp": lax.rem(tp + k, peers)} for k in range(1, 8)]
    ):
        pl.semaphore_signal(barrier, inc=1, device_id=where, device_id_type=MESH)

    def learn(level):
        pl.when(z < last)(lambda: pl.semaphore_wait(know.at[level], 1))

    def teach(level):
        @pl.when(z > 0)
        def _():
            pl.semaphore_signal(know.at[level], inc=1, device_id={"sp": below}, device_id_type=MESH)

    def blocks_at(span):
        low = jnp.minimum(lax.rem(span + last, spans), 2) + 6 - jnp.where(span > 0, 0, 1)
        return (1 - core) * low + core * (spans - 1 - low)

    count = blocks_at(z)
    onward = lax.rem(z + 1 + core * (spans - 2), spans)
    count_out = blocks_at(onward)
    count_other = spans - 1 - count

    def owner_of(way, t):
        return lax.rem(z + (1 - way) * (spans - t) + way * t, spans)

    def lines_of(owner):
        return pl.ds(pl.multiple_of(owner * block, block), block)

    def z_copy(t, pos, owner):
        part = wv.at[pos, lines_of(owner), :]
        return remote(part, part, zs.at[t, pos], zr.at[t, pos], {"sp": onward})

    def share_copy(k, t):
        lines = lines_of(owner_of(core, t))
        if k < 2:
            where = {"tp": lax.rem(tp + 2 + 4 * k, peers)}
            return remote(
                wv.at[1 + k, lines, :], wv.at[7 - 3 * k, lines, :], xs.at[k, t], xr.at[k, t], where
            )
        return remote(
            wv.at[1:3, lines, :], wv.at[5:7, lines, :], ys.at[t], yr.at[t], {"grp": partner}
        )

    def d_copy(level, way, t):
        part = wv.at[4 * level : 4 * level + 4, lines_of(owner_of(way, t)), :]
        return remote(part, part, ds_send.at[level, t], ds_recv.at[level, t], {"tp": sibling})

    def ring(t, _):
        owner = owner_of(core, t)
        for pos in (1, 2, 0, 3):
            z_copy(t, pos, owner).wait_recv()

            @pl.when(t < count_out)
            def _():
                z_copy(t + 1, pos, owner).start()

        for k in range(3):
            share_copy(k, t).start()
        d_copy(0, core, t).start()
        return 0

    def spread(t, _):
        for k in range(3):
            share_copy(k, t).wait_recv()
        d_copy(1, core, t).start()
        return 0

    def goal(up, down, first_up, first_down):
        up = jnp.where(z > 0, jnp.minimum(up, jnp.maximum(z - 2, 0)), first_up)
        down = jnp.where(z > 0, jnp.where(z == 1, jnp.maximum(down, 3), down), first_down)
        return (1 - core) * up + core * down

    def first_sends():
        for pos in (1, 2, 0, 3):
            z_copy(1, pos, z).start()

    in_copies[0].wait()
    in_copies[1].wait()
    in_copies[2].wait()
    gain_cols = gain[...].T
    bias_cols = bias[...].T
    for j in range(width // LANES):
        part = pl.ds(j * LANES, LANES)
        wi[part, :] = (wi[part, :].astype(F32) * gain_cols[:, j : j + 1]).astype(BF16)
        biasc[part, :] = jnp.broadcast_to(bias_cols[:, j : j + 1], (LANES, LANES))

    def halo_copy():
        return remote(proj.at[pl.ds(rows, 8), :], halo, halo_send, halo_recv, {"sp": above})

    def project(i, _):
        k = 3 - i
        base = pl.multiple_of(k * tile, tile)
        tok_copy(k).wait()

        part = pl.ds(base, tile)
        acc = jnp.dot(tok[part, :], wi[...], preferred_element_type=F32)
        for j in range(tile // 64):
            lines = pl.ds(pl.multiple_of(base + j * 64, 64), 64)
            total = jnp.zeros((64, LANES), F32)
            for c in range(width // LANES):
                x = tok[lines, c * LANES : (c + 1) * LANES].astype(F32)
                total = total + x * x
            mean = jnp.sum(total, axis=1, keepdims=True) * (1.0 / width)
            inv = jnp.broadcast_to(lax.rsqrt(mean + 1e-06), (64, LANES))
            invc[lines, :] = inv
            for c in range(lanes2):
                lane = slice(c * LANES, (c + 1) * LANES)
                scaled = acc[j * 64 : (j + 1) * 64, lane] * inv
                proj[pl.ds(base + 8 + j * 64, 64), lane] = scaled.astype(BF16).astype(F32)

        return 0

    lax.fori_loop(0, 1, project, 0)
    pl.semaphore_wait(barrier, 10)
    pl.when(z < last)(lambda: halo_copy().start())
    teach(0)
    for pos in range(4):
        wv_copies[pos].wait()
    first_sends()
    lax.fori_loop(1, 3, project, 0)
    rp = (1 - core) * jnp.where(z > 0, jnp.clip(z - 2, 0, 1), 0)
    lax.fori_loop(1, rp + 1, ring, 0)
    lax.fori_loop(3, 4, project, 0)
    learn(0)
    teach(1)
    ra = (1 - core) * jnp.where(z > 0, jnp.clip(z - 2, 0, 2), 0)
    lax.fori_loop(rp + 1, ra + 1, ring, 0)

    for k in range(3, 8):
        in_copies[k].wait()
    ahead = jnp.where(z == 1, 3 * core, ra)
    lax.fori_loop(ra + 1, ahead + 1, ring, 0)
    pl.when(z > 0)(lambda: halo_copy().wait_recv())

    @pl.when(z > 0)
    def _():
        proj[0:8, :] = halo[...]

    @pl.when(z == 0)
    def _():
        proj[0:8, :] = jnp.zeros((8, channels), F32)

    scale = -8.0 * softplus(-dparam[...])
    tap = [taps[k : k + 1, :] for k in range(4)]

    def gather_inputs(i):
        for s in range(SEGS):
            base = pl.multiple_of(s * mine + i * STEP, STEP)
            x = proj[pl.ds(base, STEP + 8), :]
            total = pltpu.roll(x, 3, axis=0)[8:] * tap[0]
            total = total + pltpu.roll(x, 2, axis=0)[8:] * tap[1]
            total = total + pltpu.roll(x, 1, axis=0)[8:] * tap[2]
            total = total + x[8:] * tap[3]
            conv[s * STEP : (s + 1) * STEP, :] = total.astype(BF16)

    def scan_tile(i, state):
        gather_inputs(i)
        gates[...] = jnp.dot(conv[...], wrn[...], preferred_element_type=F32)
        for s in range(SEGS):
            base = pl.multiple_of(s * mine + i * STEP, STEP)
            shift = biasc[pl.ds(base, STEP), :]
            part = slice(s * STEP, (s + 1) * STEP)
            for c in range(channels // LANES):
                lane = slice(c * LANES, (c + 1) * LANES)
                rate = jax.nn.sigmoid(gates[part, lane])
                inlet = jax.nn.sigmoid(gates[part, channels + c * LANES : channels + (c + 1) * LANES])
                log_decay = rate * scale[:, lane] + shift
                decay = jnp.exp(log_decay)
                y = -2.0 * log_decay
                series = y * (
                    1.0 - y * (0.5 - y * (1.0 / 6.0 - y * (1.0 / 24.0 - y * (1.0 / 120.0))))
                )
                grown = jnp.where(y < 0.2, series, 1.0 - decay * decay)
                root = grown * lax.rsqrt(jnp.maximum(grown, 1e-37))
                drive = root * inlet * conv[part, lane].astype(F32)
                sa[c, s * PAD : s * PAD + STEP, :] = decay
                sb[c, s * PAD : s * PAD + STEP, :] = drive
        state = list(state)
        for r in range(STEP):
            line = pl.ds(pl.multiple_of((i * STEP + r) * SEGS, SEGS), SEGS)
            for c in range(channels // LANES):
                a = sa[c, pl.ds(r, SEGS, stride=PAD), :]
                b = sb[c, pl.ds(r, SEGS, stride=PAD), :]
                h, p = state[2 * c], state[2 * c + 1]
                h, p = a * h + b, a * p
                ht[c, line, :] = h
                pt[c, line, :] = p
                state[2 * c], state[2 * c + 1] = h, p
        return tuple(state)

    state = (jnp.zeros((SEGS, LANES), F32), jnp.ones((SEGS, LANES), F32)) * lanes2
    state = lax.fori_loop(0, 3, scan_tile, state)
    learn(1)
    teach(2)
    r0 = goal(3, 1, 0, 1)
    lax.fori_loop(ahead + 1, r0 + 1, ring, 0)
    state = lax.fori_loop(3, 6, scan_tile, state)
    r1 = goal(4, 1, 0, 2)
    lax.fori_loop(r0 + 1, r1 + 1, ring, 0)
    state = lax.fori_loop(6, 8, scan_tile, state)

    for c in range(lanes2):
        h_end, p_end = state[2 * c], state[2 * c + 1]
        h, p = jnp.zeros((1, LANES), F32), jnp.ones((1, LANES), F32)
        for s in range(SEGS):
            segh[c, s : s + 1, :] = h
            segp[c, s : s + 1, :] = p
            h = p_end[s : s + 1] * h + h_end[s : s + 1]
            p = p_end[s : s + 1] * p
        carry_own[c : c + 1, :] = p
        carry_own[lanes2 + c : lanes2 + c + 1, :] = h

    learn(2)

    def carry_copy(k):
        return remote(
            carry_own, carry.at[k - 1], carry_send.at[k - 1], carry_recv.at[k - 1],
            {"sp": lax.rem(z + k, spans)},
        )

    for k in (1, 2, 3):
        pl.when(z + k < spans)(lambda: carry_copy(k).start())

    def state_copy():
        return remote(
            state_own, carry.at[3], carry_send.at[3], carry_recv.at[3], {"sp": lax.rem(z + 4, spans)}
        )

    @pl.when(z == 0)
    def _():
        state_own[...] = carry_own[...]
        state_copy().start()

    r2 = goal(5, 2, 1, 3)
    lax.fori_loop(r1 + 1, r2 + 1, ring, 0)

    in_copies[8].wait()
    for j in range(width // LANES):
        part = pl.ds(j * LANES, LANES)
        wg[part, :] = (wg[part, :].astype(F32) * gain_cols[:, j : j + 1]).astype(BF16)

    def gate(i, _):
        part = pl.ds(pl.multiple_of(i * tile, tile), tile)
        acc = jnp.dot(tok[part, :], wg[...], preferred_element_type=F32)
        inv = invc[part, :]
        for c in range(lanes2):
            lane = slice(c * LANES, (c + 1) * LANES)
            ge[part, lane] = gelu((acc[:, lane] * inv).astype(BF16).astype(F32))
        return 0

    lax.fori_loop(0, 2, gate, 0)
    rg = goal(6, 2, 1, 4)
    lax.fori_loop(r2 + 1, rg + 1, ring, 0)
    lax.fori_loop(2, 4, gate, 0)
    r3 = goal(7, 3, 2, 5)
    lax.fori_loop(rg + 1, r3 + 1, ring, 0)
    s0 = goal(4, 1, 0, 2)
    lax.fori_loop(1, s0 + 1, spread, 0)

    r4 = goal(8, 5, 2, 5)
    lax.fori_loop(r3 + 1, r4 + 1, ring, 0)
    s1 = goal(7, 4, 0, 2)
    lax.fori_loop(s0 + 1, s1 + 1, spread, 0)

    def received(copy, slot, k):
        pl.when(z >= k)(lambda: copy.wait_recv())

        @pl.when(z < k)
        def _():
            carry[slot] = jnp.zeros(carry.shape[1:], F32)

    received(state_copy(), 3, 4)
    for k in (1, 2, 3):
        received(carry_copy(k), k - 1, k)
    incoming, out_states = [], []
    for c in range(lanes2):
        h = carry[3, lanes2 + c : lanes2 + c + 1, :]
        for k in (3, 2, 1):
            h = carry[k - 1, c : c + 1, :] * h + carry[k - 1, lanes2 + c : lanes2 + c + 1, :]
        incoming.append(h)
        out_state = carry_own[c : c + 1, :] * h + carry_own[lanes2 + c : lanes2 + c + 1, :]
        out_states.append(out_state)

    @pl.when(jnp.logical_and(z > 0, z + 4 < spans))
    def _():
        for c in range(lanes2):
            state_own[c : c + 1, :] = jnp.zeros((1, LANES), F32)
            state_own[lanes2 + c : lanes2 + c + 1, :] = out_states[c]
        state_copy().start()

    def a2a_copy(other):
        return remote(gout.at[other], grecv.at[tp], a2a_send, a2a_recv.at[tp], {"tp": other})

    def ss_copy(other):
        return remote(ss_own.at[other], ss_recv.at[tp], ss_send, ss_recv_sem, {"tp": other})

    ones = jnp.ones((8, LANES), F32)

    def read_out(i, _):
        s = lax.rem(tp + 4 + i, peers)
        total = jnp.zeros((mine, LANES), F32)
        for c in range(lanes2):
            lane = slice(c * LANES, (c + 1) * LANES)
            enter = segp[c, pl.ds(s, 1), :] * incoming[c] + segh[c, pl.ds(s, 1), :]
            lines = pl.ds(s, mine, stride=SEGS)
            state = ht[c, lines, :] + pt[c, lines, :] * enter
            gated = state * ge[pl.ds(pl.multiple_of(s * mine, mine), mine), lane]
            total = total + gated * gated
            gout[s, :, lane] = (gated * ogain[:, lane]).astype(BF16)
        sums = lax.dot_general(
            ones, total, (((1,), (1,)), ((), ())), preferred_element_type=F32
        )
        ss_own[s] = sums[0:1, :]

        @pl.when(i != 4)
        def _():
            a2a_copy(s).start()
            ss_copy(s).start()

        return 0

    lax.fori_loop(0, 8, read_out, 0)
    grecv[tp] = gout[tp]
    ss_recv[tp] = ss_own[tp]

    lax.fori_loop(r4 + 1, count + 1, ring, 0)
    lax.fori_loop(s1 + 1, count + 1, spread, 0)

    for pos in range(4, 8):
        wv_copies[pos].wait()
    for k in range(1, 8):
        other = lax.rem(tp + k, peers)
        remote(gout.at[other], grecv.at[other], a2a_send, a2a_recv.at[other], {"tp": other}).wait_recv()
    seven = ss_recv.at[pl.ds(0, 7)]
    local(seven, seven, ss_recv_sem).wait()

    def other_half(t, _):
        d_copy(0, 1 - core, t).wait_recv()
        d_copy(1, 1 - core, t).wait_recv()
        return 0

    lax.fori_loop(1, count_other + 1, other_half, 0)

    total = ss_recv[0]
    for k in range(1, 8):
        total = total + ss_recv[k]
    scales = lax.rsqrt(total * (1.0 / width) + 1e-06)
    scales = jnp.broadcast_to(scales, (LANES, mine)).T

    def finish(pos, _):
        acc = jnp.zeros((mine, channels), F32)
        for k in range(8):
            acc = acc + jnp.dot(
                grecv[k], wv[pos, k * channels : (k + 1) * channels, :], preferred_element_type=F32
            )
        for c in range(lanes2):
            lane = slice(c * LANES, (c + 1) * LANES)
            where = pl.ds(pl.multiple_of(column(pos) + c * LANES, LANES), LANES)
            obuf[:, where] = (acc[:, lane] * scales).astype(BF16)
        return 0

    def out_copy(k):
        part = pl.ds(k * (mine // 4), mine // 4)
        return local(obuf.at[part, :], out.at[part, :], out_sem.at[k])

    def passed(t, _):
        for pos in range(4):
            z_copy(t, pos, z).wait_send()
        return 0

    def shared(t, _):
        for k in range(3):
            share_copy(k, t).wait_send()
        d_copy(0, core, t).wait_send()
        d_copy(1, core, t).wait_send()
        return 0

    lax.fori_loop(1, count_out + 1, passed, 0)
    lax.fori_loop(1, count + 1, shared, 0)
    pl.when(z < last)(lambda: halo_copy().wait_send())
    for k in (1, 2, 3):
        pl.when(z + k < spans)(lambda: carry_copy(k).wait_send())
    pl.when(z + 4 < spans)(lambda: state_copy().wait_send())
    sent = gout.at[pl.ds(0, 7)]
    local(sent, sent, a2a_send).wait()
    sent = ss_own.at[pl.ds(0, 7)]
    local(sent, sent, ss_send).wait()
    for pos in range(8):
        finish(pos, 0)
    for k in range(4):
        out_copy(k).start()
    for k in range(4):
        out_copy(k).wait()


def body(
    tokens, in_gain, w_input, w_gate, conv_taps, w_rate, w_inlet, decay_param, decay_bias, out_gain, w_out
):
    rows, width = tokens.shape
    channels = w_input.shape[1]
    lanes2 = channels // LANES
    spans, peers = lax.axis_size("sp"), lax.axis_size("tp")
    mine = rows // peers
    vmem = pltpu.VMEM
    dma = pltpu.SemaphoreType.DMA
    scratch = [
        vmem((rows, width), BF16),
        vmem((width, channels), BF16),
        vmem((width, channels), BF16),
        vmem((channels, 2 * channels), BF16),
        vmem((width // LANES, LANES), F32),
        vmem((4, channels), F32),
        vmem((1, channels), F32),
        vmem((rows // LANES, LANES), F32),
        vmem((1, channels), F32),
        vmem((8, width, channels), BF16),
        vmem((8 + rows, channels), F32),
        vmem((8, channels), F32),
        vmem((rows, LANES), F32),
        vmem((rows, LANES), F32),
        vmem((SEGS * STEP, channels), BF16),
        vmem((SEGS * STEP, 2 * channels), F32),
        vmem((lanes2, SEGS * PAD, LANES), F32),
        vmem((lanes2, SEGS * PAD, LANES), F32),
        vmem((lanes2, rows, LANES), F32),
        vmem((lanes2, rows, LANES), F32),
        vmem((rows, channels), F32),
        vmem((lanes2, SEGS, LANES), F32),
        vmem((lanes2, SEGS, LANES), F32),
        vmem((2 * lanes2, LANES), F32),
        vmem((2 * lanes2, LANES), F32),
        vmem((4, 2 * lanes2, LANES), F32),
        vmem((peers, mine, channels), BF16),
        vmem((peers, mine, channels), BF16),
        vmem((peers, 1, mine), F32),
        vmem((peers, 1, mine), F32),
        vmem((mine, width), BF16),
        dma((4,)),
        dma((9,)),
        dma((8,)),
        dma((8,)),
        dma((11, 4)),
        dma((11, 4)),
        dma((2, 11)),
        dma((11,)),
        dma((2, 11)),
        dma((11,)),
        dma((2, 11)),
        dma((2, 11)),
        dma(()),
        dma(()),
        dma((4,)),
        dma((4,)),
        dma(()),
        dma((8,)),
        dma(()),
        dma(()),
    ]
    scratch += [pltpu.SemaphoreType.REGULAR((3,))]
    spec = pl.BlockSpec(memory_space=pl.ANY)
    return pl.pallas_call(
        kernel,
        out_shape=jax.ShapeDtypeStruct((mine, width), BF16),
        in_specs=[spec] * 11,
        out_specs=spec,
        scratch_shapes=scratch,
        compiler_params=pltpu.CompilerParams(
            collective_id=0, has_side_effects=True, vmem_limit_bytes=60 * 1024 * 1024
        ),
        name="gated_recurrence",
    )(
        tokens,
        in_gain.reshape(width // LANES, LANES),
        w_input,
        w_gate,
        conv_taps,
        w_rate.reshape(channels, channels),
        w_inlet.reshape(channels, channels),
        decay_param.reshape(1, channels),
        decay_bias.reshape(rows // LANES, LANES),
        out_gain.reshape(1, channels),
        w_out,
    )


def solution(mesh):
    return jax.shard_map(
        body,
        mesh=mesh,
        in_specs=(
            P(("grp", "sp"), None),
            P(),
            P(None, "tp"),
            P(None, "tp"),
            P(None, "tp"),
            P("tp", None, None),
            P("tp", None, None),
            P("tp"),
            P("tp", ("grp", "sp")),
            P("tp"),
            P("sp", None),
        ),
        out_specs=P(("grp", "sp", "tp"), None),
        check_vma=False,
    )
```

```python
import functools

import jax
import jax.numpy as jnp
from jax import lax
from jax.experimental import pallas as pl
from jax.experimental.pallas import tpu as pltpu
from jax.sharding import PartitionSpec as P

MESH = pl.DeviceIdType.MESH
F32 = jnp.float32
BF16 = jnp.bfloat16
LANES = 128
SEGS = 8
STEP = 32
PAD = 40


def log1p_small(u):
    series = u * (1.0 - u * (0.5 - u * (1.0 / 3.0 - u * (0.25 - u * (0.2 - u / 6.0)))))
    return jnp.where(u < 0.06, series, jnp.log(1.0 + u))


def softplus(x):
    return jnp.maximum(x, 0.0) + log1p_small(jnp.exp(-jnp.abs(x)))


def gelu(x):
    inner = 0.7978845608028654 * (x + 0.044715 * (x * x * x))
    return 0.5 * x * (1.0 + jnp.tanh(inner))


def kernel(
    tokens_in,
    gain_in,
    w_input_in,
    w_gate_in,
    taps_in,
    w_rate_in,
    w_inlet_in,
    dparam_in,
    bias_in,
    ogain_in,
    w_out_in,
    out,
    tok,
    wi,
    wg,
    wrn,
    gain,
    taps,
    dparam,
    bias,
    ogain,
    wv,
    proj,
    halo,
    biasc,
    invc,
    conv,
    gates,
    sa,
    sb,
    ht,
    pt,
    ge,
    segh,
    segp,
    carry_own,
    state_own,
    carry,
    gout,
    grecv,
    ss_own,
    ss_recv,
    obuf,
    tok_sem,
    in_sem,
    wv_sem,
    out_sem,
    zs,
    zr,
    xr,
    yr,
    xs,
    ys,
    ds_send,
    ds_recv,
    halo_send,
    halo_recv,
    carry_send,
    carry_recv,
    a2a_send,
    a2a_recv,
    ss_send,
    ss_recv_sem,
    know,
):
    grp, z, tp = lax.axis_index("grp"), lax.axis_index("sp"), lax.axis_index("tp")
    spans, peers = lax.axis_size("sp"), lax.axis_size("tp")
    core = lax.rem(tp, 2)
    rows, width = tok.shape
    channels = wi.shape[1]
    lanes2 = channels // LANES
    block = width // spans
    tile = rows // 4
    mine = rows // peers
    first = lax.rem(2 * (tp // 2) + 4 * lax.rem(grp, 2), 8)
    partner = grp + 1 - 2 * lax.rem(grp, 2)
    sibling = tp + 1 - 2 * core

    def column(pos):
        return pl.multiple_of(lax.rem(first + pos, 8) * channels, channels)

    def local(src, dst, sem):
        return pltpu.make_async_copy(src, dst, sem)

    def remote(src, dst, send, recv, where):
        return pltpu.make_async_remote_copy(
            src_ref=src, dst_ref=dst, send_sem=send, recv_sem=recv, device_id=where, device_id_type=MESH
        )

    own_lines = pl.ds(pl.multiple_of(z * block, block), block)
    wv_copies = [
        local(w_out_in.at[:, pl.ds(column(pos), channels)], wv.at[pos, own_lines, :], wv_sem.at[pos])
        for pos in range(8)
    ]
    for pos in range(4):
        wv_copies[pos].start()
    in_copies = [
        local(gain_in, gain, in_sem.at[0]),
        local(w_input_in, wi, in_sem.at[1]),
        local(bias_in, bias, in_sem.at[2]),
        local(taps_in, taps, in_sem.at[3]),
        local(dparam_in, dparam, in_sem.at[4]),
        local(ogain_in, ogain, in_sem.at[5]),
        local(w_rate_in, wrn.at[:, 0:channels], in_sem.at[6]),
        local(w_inlet_in, wrn.at[:, channels : 2 * channels], in_sem.at[7]),
        local(w_gate_in, wg, in_sem.at[8]),
    ]
    for k in (0, 1, 2):
        in_copies[k].start()

    def tok_copy(k):
        part = pl.ds(pl.multiple_of(k * tile, tile), tile)
        return local(tokens_in.at[part, :], tok.at[part, :], tok_sem.at[k])

    for k in (3, 2, 1, 0):
        tok_copy(k).start()
    for k in range(3, 9):
        in_copies[k].start()
    for pos in range(4, 8):
        wv_copies[pos].start()

    last = spans - 1
    barrier = pltpu.get_barrier_semaphore()
    above, below = lax.rem(z + 1, spans), lax.rem(z + last, spans)
    for where in (
        [{"sp": above}, {"sp": below}, {"grp": partner}]
        + [{"tp": lax.rem(tp + k, peers)} for k in range(1, 8)]
    ):
        pl.semaphore_signal(barrier, inc=1, device_id=where, device_id_type=MESH)

    def learn(level):
        pl.when(z < last)(lambda: pl.semaphore_wait(know.at[level], 1))

    def teach(level):
        @pl.when(z > 0)
        def _():
            pl.semaphore_signal(know.at[level], inc=1, device_id={"sp": below}, device_id_type=MESH)

    def blocks_at(span):
        low = jnp.minimum(lax.rem(span + last, spans), 2) + 6 - jnp.where(span > 0, 0, 1)
        return (1 - core) * low + core * (spans - 1 - low)

    count = blocks_at(z)
    onward = lax.rem(z + 1 + core * (spans - 2), spans)
    count_out = blocks_at(onward)
    count_other = spans - 1 - count

    def owner_of(way, t):
        return lax.rem(z + (1 - way) * (spans - t) + way * t, spans)

    def lines_of(owner):
        return pl.ds(pl.multiple_of(owner * block, block), block)

    def z_copy(t, pos, owner):
        part = wv.at[pos, lines_of(owner), :]
        return remote(part, part, zs.at[t, pos], zr.at[t, pos], {"sp": onward})

    def share_copy(k, t):
        lines = lines_of(owner_of(core, t))
        if k < 2:
            where = {"tp": lax.rem(tp + 2 + 4 * k, peers)}
            return remote(
                wv.at[1 + k, lines, :], wv.at[7 - 3 * k, lines, :], xs.at[k, t], xr.at[k, t], where
            )
        return remote(
            wv.at[1:3, lines, :], wv.at[5:7, lines, :], ys.at[t], yr.at[t], {"grp": partner}
        )

    def d_copy(level, way, t):
        part = wv.at[4 * level : 4 * level + 4, lines_of(owner_of(way, t)), :]
        return remote(part, part, ds_send.at[level, t], ds_recv.at[level, t], {"tp": sibling})

    def ring(t, _):
        owner = owner_of(core, t)
        for pos in (1, 2, 0, 3):
            z_copy(t, pos, owner).wait_recv()

            @pl.when(t < count_out)
            def _():
                z_copy(t + 1, pos, owner).start()

        for k in range(3):
            share_copy(k, t).start()
        d_copy(0, core, t).start()
        return 0

    def spread(t, _):
        for k in range(3):
            share_copy(k, t).wait_recv()
        d_copy(1, core, t).start()
        return 0

    def goal(up, down, first_up, first_down):
        up = jnp.where(z > 0, jnp.minimum(up, jnp.maximum(z - 2, 0)), first_up)
        down = jnp.where(z > 0, jnp.where(z == 1, jnp.maximum(down, 3), down), first_down)
        return (1 - core) * up + core * down

    def first_sends():
        for pos in (1, 2, 0, 3):
            z_copy(1, pos, z).start()

    in_copies[0].wait()
    in_copies[1].wait()
    in_copies[2].wait()
    gain_cols = gain[...].T
    bias_cols = bias[...].T
    for j in range(width // LANES):
        part = pl.ds(j * LANES, LANES)
        wi[part, :] = (wi[part, :].astype(F32) * gain_cols[:, j : j + 1]).astype(BF16)
        biasc[part, :] = jnp.broadcast_to(bias_cols[:, j : j + 1], (LANES, LANES))

    def halo_copy():
        return remote(proj.at[pl.ds(rows, 8), :], halo, halo_send, halo_recv, {"sp": above})

    def project(i, _):
        k = 3 - i
        base = pl.multiple_of(k * tile, tile)
        tok_copy(k).wait()

        part = pl.ds(base, tile)
        acc = jnp.dot(tok[part, :], wi[...], preferred_element_type=F32)
        for j in range(tile // 64):
            lines = pl.ds(pl.multiple_of(base + j * 64, 64), 64)
            total = jnp.zeros((64, LANES), F32)
            for c in range(width // LANES):
                x = tok[lines, c * LANES : (c + 1) * LANES].astype(F32)
                total = total + x * x
            mean = jnp.sum(total, axis=1, keepdims=True) * (1.0 / width)
            inv = jnp.broadcast_to(lax.rsqrt(mean + 1e-06), (64, LANES))
            invc[lines, :] = inv
            for c in range(lanes2):
                lane = slice(c * LANES, (c + 1) * LANES)
                scaled = acc[j * 64 : (j + 1) * 64, lane] * inv
                proj[pl.ds(base + 8 + j * 64, 64), lane] = scaled.astype(BF16).astype(F32)

        return 0

    lax.fori_loop(0, 1, project, 0)
    pl.semaphore_wait(barrier, 10)
    pl.when(z < last)(lambda: halo_copy().start())
    teach(0)
    for pos in range(4):
        wv_copies[pos].wait()
    first_sends()
    lax.fori_loop(1, 3, project, 0)
    rp = (1 - core) * jnp.where(z > 0, jnp.clip(z - 2, 0, 1), 0)
    lax.fori_loop(1, rp + 1, ring, 0)
    lax.fori_loop(3, 4, project, 0)
    learn(0)
    teach(1)
    ra = (1 - core) * jnp.where(z > 0, jnp.clip(z - 2, 0, 2), 0)
    lax.fori_loop(rp + 1, ra + 1, ring, 0)

    for k in range(3, 8):
        in_copies[k].wait()
    ahead = jnp.where(z == 1, 3 * core, ra)
    lax.fori_loop(ra + 1, ahead + 1, ring, 0)
    pl.when(z > 0)(lambda: halo_copy().wait_recv())

    @pl.when(z > 0)
    def _():
        proj[0:8, :] = halo[...]

    @pl.when(z == 0)
    def _():
        proj[0:8, :] = jnp.zeros((8, channels), F32)

    scale = -8.0 * softplus(-dparam[...])
    tap = [taps[k : k + 1, :] for k in range(4)]

    def gather_inputs(i):
        for s in range(SEGS):
            base = pl.multiple_of(s * mine + i * STEP, STEP)
            x = proj[pl.ds(base, STEP + 8), :]
            total = pltpu.roll(x, 3, axis=0)[8:] * tap[0]
            total = total + pltpu.roll(x, 2, axis=0)[8:] * tap[1]
            total = total + pltpu.roll(x, 1, axis=0)[8:] * tap[2]
            total = total + x[8:] * tap[3]
            conv[s * STEP : (s + 1) * STEP, :] = total.astype(BF16)

    def scan_tile(i, state):
        gather_inputs(i)
        gates[...] = jnp.dot(conv[...], wrn[...], preferred_element_type=F32)
        for s in range(SEGS):
            base = pl.multiple_of(s * mine + i * STEP, STEP)
            shift = biasc[pl.ds(base, STEP), :]
            part = slice(s * STEP, (s + 1) * STEP)
            for c in range(channels // LANES):
                lane = slice(c * LANES, (c + 1) * LANES)
                rate = jax.nn.sigmoid(gates[part, lane])
                inlet = jax.nn.sigmoid(gates[part, channels + c * LANES : channels + (c + 1) * LANES])
                log_decay = rate * scale[:, lane] + shift
                decay = jnp.exp(log_decay)
                y = -2.0 * log_decay
                series = y * (
                    1.0 - y * (0.5 - y * (1.0 / 6.0 - y * (1.0 / 24.0 - y * (1.0 / 120.0))))
                )
                grown = jnp.where(y < 0.2, series, 1.0 - decay * decay)
                root = grown * lax.rsqrt(jnp.maximum(grown, 1e-37))
                drive = root * inlet * conv[part, lane].astype(F32)
                sa[c, s * PAD : s * PAD + STEP, :] = decay
                sb[c, s * PAD : s * PAD + STEP, :] = drive
        state = list(state)
        for r in range(STEP):
            line = pl.ds(pl.multiple_of((i * STEP + r) * SEGS, SEGS), SEGS)
            for c in range(channels // LANES):
                a = sa[c, pl.ds(r, SEGS, stride=PAD), :]
                b = sb[c, pl.ds(r, SEGS, stride=PAD), :]
                h, p = state[2 * c], state[2 * c + 1]
                h, p = a * h + b, a * p
                ht[c, line, :] = h
                pt[c, line, :] = p
                state[2 * c], state[2 * c + 1] = h, p
        return tuple(state)

    state = (jnp.zeros((SEGS, LANES), F32), jnp.ones((SEGS, LANES), F32)) * lanes2
    state = lax.fori_loop(0, 3, scan_tile, state)
    learn(1)
    teach(2)
    r0 = goal(3, 1, 0, 1)
    lax.fori_loop(ahead + 1, r0 + 1, ring, 0)
    state = lax.fori_loop(3, 6, scan_tile, state)
    r1 = goal(4, 1, 0, 2)
    lax.fori_loop(r0 + 1, r1 + 1, ring, 0)
    state = lax.fori_loop(6, 8, scan_tile, state)

    for c in range(lanes2):
        h_end, p_end = state[2 * c], state[2 * c + 1]
        h, p = jnp.zeros((1, LANES), F32), jnp.ones((1, LANES), F32)
        for s in range(SEGS):
            segh[c, s : s + 1, :] = h
            segp[c, s : s + 1, :] = p
            h = p_end[s : s + 1] * h + h_end[s : s + 1]
            p = p_end[s : s + 1] * p
        carry_own[c : c + 1, :] = p
        carry_own[lanes2 + c : lanes2 + c + 1, :] = h

    learn(2)

    def carry_copy(k):
        return remote(
            carry_own, carry.at[k - 1], carry_send.at[k - 1], carry_recv.at[k - 1],
            {"sp": lax.rem(z + k, spans)},
        )

    for k in (1, 2, 3):
        pl.when(z + k < spans)(lambda: carry_copy(k).start())

    def state_copy():
        return remote(
            state_own, carry.at[3], carry_send.at[3], carry_recv.at[3], {"sp": lax.rem(z + 4, spans)}
        )

    @pl.when(z == 0)
    def _():
        state_own[...] = carry_own[...]
        state_copy().start()

    r2 = goal(5, 2, 1, 3)
    lax.fori_loop(r1 + 1, r2 + 1, ring, 0)

    in_copies[8].wait()
    for j in range(width // LANES):
        part = pl.ds(j * LANES, LANES)
        wg[part, :] = (wg[part, :].astype(F32) * gain_cols[:, j : j + 1]).astype(BF16)

    def gate(i, _):
        part = pl.ds(pl.multiple_of(i * tile, tile), tile)
        acc = jnp.dot(tok[part, :], wg[...], preferred_element_type=F32)
        inv = invc[part, :]
        for c in range(lanes2):
            lane = slice(c * LANES, (c + 1) * LANES)
            ge[part, lane] = gelu((acc[:, lane] * inv).astype(BF16).astype(F32))
        return 0

    lax.fori_loop(0, 2, gate, 0)
    rg = goal(6, 2, 1, 4)
    lax.fori_loop(r2 + 1, rg + 1, ring, 0)
    lax.fori_loop(2, 4, gate, 0)
    r3 = goal(7, 3, 2, 5)
    lax.fori_loop(rg + 1, r3 + 1, ring, 0)
    s0 = goal(4, 1, 0, 2)
    lax.fori_loop(1, s0 + 1, spread, 0)

    r4 = goal(8, 5, 2, 5)
    sooner = jnp.minimum(jnp.maximum(z - 1, 1), 8)
    r4 = jnp.where(z > 0, (1 - core) * sooner + core * r4, r4)
    lax.fori_loop(r3 + 1, r4 + 1, ring, 0)
    s1 = goal(7, 4, 0, 2)
    lax.fori_loop(s0 + 1, s1 + 1, spread, 0)

    def received(copy, slot, k):
        pl.when(z >= k)(lambda: copy.wait_recv())

        @pl.when(z < k)
        def _():
            carry[slot] = jnp.zeros(carry.shape[1:], F32)

    received(state_copy(), 3, 4)
    for k in (1, 2, 3):
        received(carry_copy(k), k - 1, k)
    incoming, out_states = [], []
    for c in range(lanes2):
        h = carry[3, lanes2 + c : lanes2 + c + 1, :]
        for k in (3, 2, 1):
            h = carry[k - 1, c : c + 1, :] * h + carry[k - 1, lanes2 + c : lanes2 + c + 1, :]
        incoming.append(h)
        out_state = carry_own[c : c + 1, :] * h + carry_own[lanes2 + c : lanes2 + c + 1, :]
        out_states.append(out_state)

    @pl.when(jnp.logical_and(z > 0, z + 4 < spans))
    def _():
        for c in range(lanes2):
            state_own[c : c + 1, :] = jnp.zeros((1, LANES), F32)
            state_own[lanes2 + c : lanes2 + c + 1, :] = out_states[c]
        state_copy().start()

    def a2a_copy(other):
        return remote(gout.at[other], grecv.at[tp], a2a_send, a2a_recv.at[tp], {"tp": other})

    def ss_copy(other):
        return remote(ss_own.at[other], ss_recv.at[tp], ss_send, ss_recv_sem, {"tp": other})

    ones = jnp.ones((8, LANES), F32)

    def read_out(i, _):
        s = lax.rem(tp + 4 + i, peers)
        total = jnp.zeros((mine, LANES), F32)
        for c in range(lanes2):
            lane = slice(c * LANES, (c + 1) * LANES)
            enter = segp[c, pl.ds(s, 1), :] * incoming[c] + segh[c, pl.ds(s, 1), :]
            lines = pl.ds(s, mine, stride=SEGS)
            state = ht[c, lines, :] + pt[c, lines, :] * enter
            gated = state * ge[pl.ds(pl.multiple_of(s * mine, mine), mine), lane]
            total = total + gated * gated
            gout[s, :, lane] = (gated * ogain[:, lane]).astype(BF16)
        sums = lax.dot_general(
            ones, total, (((1,), (1,)), ((), ())), preferred_element_type=F32
        )
        ss_own[s] = sums[0:1, :]

        @pl.when(i != 4)
        def _():
            a2a_copy(s).start()
            ss_copy(s).start()

        return 0

    lax.fori_loop(0, 8, read_out, 0)
    grecv[tp] = gout[tp]
    ss_recv[tp] = ss_own[tp]

    lax.fori_loop(r4 + 1, count + 1, ring, 0)
    lax.fori_loop(s1 + 1, count + 1, spread, 0)

    for pos in range(4, 8):
        wv_copies[pos].wait()
    for k in range(1, 8):
        other = lax.rem(tp + k, peers)
        remote(gout.at[other], grecv.at[other], a2a_send, a2a_recv.at[other], {"tp": other}).wait_recv()
    seven = ss_recv.at[pl.ds(0, 7)]
    local(seven, seven, ss_recv_sem).wait()

    def other_half(t, _):
        d_copy(0, 1 - core, t).wait_recv()
        d_copy(1, 1 - core, t).wait_recv()
        return 0

    lax.fori_loop(1, count_other + 1, other_half, 0)

    total = ss_recv[0]
    for k in range(1, 8):
        total = total + ss_recv[k]
    scales = lax.rsqrt(total * (1.0 / width) + 1e-06)
    scales = jnp.broadcast_to(scales, (LANES, mine)).T

    def finish(pos, _):
        acc = jnp.zeros((mine, channels), F32)
        for k in range(8):
            acc = acc + jnp.dot(
                grecv[k], wv[pos, k * channels : (k + 1) * channels, :], preferred_element_type=F32
            )
        for c in range(lanes2):
            lane = slice(c * LANES, (c + 1) * LANES)
            where = pl.ds(pl.multiple_of(column(pos) + c * LANES, LANES), LANES)
            obuf[:, where] = (acc[:, lane] * scales).astype(BF16)
        return 0

    def out_copy(k):
        part = pl.ds(k * (mine // 4), mine // 4)
        return local(obuf.at[part, :], out.at[part, :], out_sem.at[k])

    def passed(t, _):
        for pos in range(4):
            z_copy(t, pos, z).wait_send()
        return 0

    def shared(t, _):
        for k in range(3):
            share_copy(k, t).wait_send()
        d_copy(0, core, t).wait_send()
        d_copy(1, core, t).wait_send()
        return 0

    lax.fori_loop(1, count_out + 1, passed, 0)
    lax.fori_loop(1, count + 1, shared, 0)
    pl.when(z < last)(lambda: halo_copy().wait_send())
    for k in (1, 2, 3):
        pl.when(z + k < spans)(lambda: carry_copy(k).wait_send())
    pl.when(z + 4 < spans)(lambda: state_copy().wait_send())
    sent = gout.at[pl.ds(0, 7)]
    local(sent, sent, a2a_send).wait()
    sent = ss_own.at[pl.ds(0, 7)]
    local(sent, sent, ss_send).wait()
    for pos in range(8):
        finish(pos, 0)
    for k in range(4):
        out_copy(k).start()
    for k in range(4):
        out_copy(k).wait()


def body(
    tokens, in_gain, w_input, w_gate, conv_taps, w_rate, w_inlet, decay_param, decay_bias, out_gain, w_out
):
    rows, width = tokens.shape
    channels = w_input.shape[1]
    lanes2 = channels // LANES
    spans, peers = lax.axis_size("sp"), lax.axis_size("tp")
    mine = rows // peers
    vmem = pltpu.VMEM
    dma = pltpu.SemaphoreType.DMA
    scratch = [
        vmem((rows, width), BF16),
        vmem((width, channels), BF16),
        vmem((width, channels), BF16),
        vmem((channels, 2 * channels), BF16),
        vmem((width // LANES, LANES), F32),
        vmem((4, channels), F32),
        vmem((1, channels), F32),
        vmem((rows // LANES, LANES), F32),
        vmem((1, channels), F32),
        vmem((8, width, channels), BF16),
        vmem((8 + rows, channels), F32),
        vmem((8, channels), F32),
        vmem((rows, LANES), F32),
        vmem((rows, LANES), F32),
        vmem((SEGS * STEP, channels), BF16),
        vmem((SEGS * STEP, 2 * channels), F32),
        vmem((lanes2, SEGS * PAD, LANES), F32),
        vmem((lanes2, SEGS * PAD, LANES), F32),
        vmem((lanes2, rows, LANES), F32),
        vmem((lanes2, rows, LANES), F32),
        vmem((rows, channels), F32),
        vmem((lanes2, SEGS, LANES), F32),
        vmem((lanes2, SEGS, LANES), F32),
        vmem((2 * lanes2, LANES), F32),
        vmem((2 * lanes2, LANES), F32),
        vmem((4, 2 * lanes2, LANES), F32),
        vmem((peers, mine, channels), BF16),
        vmem((peers, mine, channels), BF16),
        vmem((peers, 1, mine), F32),
        vmem((peers, 1, mine), F32),
        vmem((mine, width), BF16),
        dma((4,)),
        dma((9,)),
        dma((8,)),
        dma((8,)),
        dma((11, 4)),
        dma((11, 4)),
        dma((2, 11)),
        dma((11,)),
        dma((2, 11)),
        dma((11,)),
        dma((2, 11)),
        dma((2, 11)),
        dma(()),
        dma(()),
        dma((4,)),
        dma((4,)),
        dma(()),
        dma((8,)),
        dma(()),
        dma(()),
    ]
    scratch += [pltpu.SemaphoreType.REGULAR((3,))]
    spec = pl.BlockSpec(memory_space=pl.ANY)
    return pl.pallas_call(
        kernel,
        out_shape=jax.ShapeDtypeStruct((mine, width), BF16),
        in_specs=[spec] * 11,
        out_specs=spec,
        scratch_shapes=scratch,
        compiler_params=pltpu.CompilerParams(
            collective_id=0, has_side_effects=True, vmem_limit_bytes=60 * 1024 * 1024
        ),
        name="gated_recurrence",
    )(
        tokens,
        in_gain.reshape(width // LANES, LANES),
        w_input,
        w_gate,
        conv_taps,
        w_rate.reshape(channels, channels),
        w_inlet.reshape(channels, channels),
        decay_param.reshape(1, channels),
        decay_bias.reshape(rows // LANES, LANES),
        out_gain.reshape(1, channels),
        w_out,
    )


def solution(mesh):
    return jax.shard_map(
        body,
        mesh=mesh,
        in_specs=(
            P(("grp", "sp"), None),
            P(),
            P(None, "tp"),
            P(None, "tp"),
            P(None, "tp"),
            P("tp", None, None),
            P("tp", None, None),
            P("tp"),
            P("tp", ("grp", "sp")),
            P("tp"),
            P("sp", None),
        ),
        out_specs=P(("grp", "sp", "tp"), None),
        check_vma=False,
    )
```
